32 devices in a mesh: sp: 8 (over z, y), tp: 4 (over x, core).
Axes of the slice: x: 2, y: 2, z: 4, core: 2. Of those that a mesh axis runs over, the one named last changes fastest.
Arguments:
- d_out: bfloat16 [4096, 2048], P('sp'), may hold values from -6 to 6
- route_expert: int32 [4096, 2], P('sp'), may hold values from 0 to 7, all different within a row; in each aligned block of 512 rows (0 to 511, 512 to 1023, ...) at most 144 rows name the same one
- route_weight: float32 [4096, 2], P('sp'), may hold values from 0.2 to 1
- expert_inputs: bfloat16 [8, 1152, 2048], P('sp'), may hold values from -6 to 6
- w_gate: bfloat16 [8, 2048, 2816], P('sp', None, 'tp'), may hold values from -0.125 to 0.125
- w_up: bfloat16 [8, 2048, 2816], P('sp', None, 'tp'), may hold values from -0.125 to 0.125
- w_down: bfloat16 [8, 2816, 2048], P('sp', 'tp'), may hold values from -0.109375 to 0.109375
- w_out: bfloat16 [2048, 1024], P(None, 'tp'), may hold values from -0.1875 to 0.1875
- queries: bfloat16 [4096, 4, 128], P('sp', 'tp'), may hold values from -6 to 6
- keys: bfloat16 [4096, 4, 128], P('sp', 'tp'), may hold values from -2 to 2
- values: bfloat16 [4096, 4, 256], P('sp', 'tp'), may hold values from -6 to 6
- log_decay: float32 [4096, 4, 128], P('sp', 'tp'), may hold values from -1 to 0
Outputs:
- grad_gate: bfloat16 [8, 2048, 2816], P('sp', None, 'tp')
- grad_up: bfloat16 [8, 2048, 2816], P('sp', None, 'tp')
- grad_down: bfloat16 [8, 2816, 2048], P('sp', 'tp')
- grad_proj: float32 [2048, 1024], P('sp', 'tp')
- grad_queries: bfloat16 [4096, 4, 128], P('sp', 'tp')
- grad_keys: bfloat16 [4096, 4, 128], P('sp', 'tp')
- grad_values: bfloat16 [4096, 4, 256], P('sp', 'tp')
- grad_log_decay: float32 [4096, 4, 128], P('sp', 'tp')
The draws below stay inside these ranges and needn't reach their ends.
Inputs may be any that keep to these rules, and one draw needn't show every extreme that they name: `route_expert`: the two experts of a token differ. Among the rows of one device no expert is named more than 144 times, and in every draw some device names some expert exactly 144 times.
All inputs are finite; a program needn't handle non-finite values.
Results may differ from the reference program's by a relative error of at most 0.02.
Values may be sent and summed in bfloat16 or wider, within the bound.
A program may use at most 128 MiB of HBM per device.

```python
import math
import jax
import jax.numpy as jnp
import numpy as np
from jax import lax

D = 2048
FF = 2816
MIXER_HEADS = 4
KEY_CHANNELS = 128
DV = 256
BLK = 64
TOK_DEV = 512
SEQUENCE_TOKENS = 4096
EXPERTS = 8
CAP = 144
N_SP = 8
N_TP = 4


def draw_log_decay(key, part):
    every_head_keys = jax.random.split(jax.random.fold_in(key, 11), 7)
    slow_share = 0.5
    gradual_decay_mask = jax.random.bernoulli(every_head_keys[0], slow_share, (MIXER_HEADS, KEY_CHANNELS))
    slow_rate = jnp.exp(jax.random.uniform(every_head_keys[1], (MIXER_HEADS, KEY_CHANNELS), jnp.float32, jnp.log(0.05), jnp.log(0.5))) / SEQUENCE_TOKENS
    fast_rate = jnp.exp(jax.random.uniform(every_head_keys[2], (MIXER_HEADS, KEY_CHANNELS), jnp.float32, jnp.log(0.01), jnp.log(0.033)))
    base_rate = jnp.where(gradual_decay_mask, slow_rate, fast_rate)
    segment_count = SEQUENCE_TOKENS // TOK_DEV
    device_factor = jnp.exp(jax.random.uniform(every_head_keys[3], (segment_count, 1, 1, 1), jnp.float32, jnp.log(0.5), jnp.log(2.0)))
    device_factor = jnp.broadcast_to(device_factor, (segment_count, TOK_DEV, 1, 1)).reshape(SEQUENCE_TOKENS, 1, 1)
    roughness = jax.random.uniform(every_head_keys[4], (SEQUENCE_TOKENS, MIXER_HEADS, KEY_CHANNELS), jnp.float32, 0.5, 1.5)
    spike_position = jax.random.randint(every_head_keys[5], (4,), 0, SEQUENCE_TOKENS)
    spike_token_rows = jnp.any(jnp.arange(SEQUENCE_TOKENS)[:, None] == spike_position[None, :], axis=1)
    spike_penalty = jnp.log(jax.random.uniform(every_head_keys[6], (SEQUENCE_TOKENS, MIXER_HEADS, KEY_CHANNELS), jnp.float32, 0.5, 0.8))
    channel_decay_logs = -base_rate[None] * device_factor * roughness
    channel_decay_logs = channel_decay_logs + jnp.where(spike_token_rows[:, None, None] & gradual_decay_mask[None], spike_penalty, 0.0)
    return channel_decay_logs.astype(jnp.float32)


def with_spikes(drawn, own_key, source, target, shards_of, factor):
    def block_of(position):
        return (jnp.arange(drawn.shape[position]) // (drawn.shape[position] // shards_of)).reshape((-1,) + (1,) * (drawn.ndim - 1 - position))

    near = jax.random.permutation(own_key, shards_of)[block_of(target)]
    far = (block_of(target) + shards_of // 2) % shards_of
    return jnp.where((block_of(source) == near) | (block_of(source) == far), factor * drawn, drawn)


def levels(rng, dims, shards, least, largest):
    loudness = 1.0
    for dim, shards_of in shards:
        steps = jax.random.uniform(jax.random.fold_in(jax.random.fold_in(rng, 6), dim), (shards_of,), jnp.float32, least / len(shards), largest / len(shards))
        loudness = loudness * jnp.repeat(jnp.exp(steps), dims[dim] // shards_of).reshape((-1,) + (1,) * (len(dims) - 1 - dim))
    return loudness


def assign_block(own_key, own, number, rows, amount, top, reach, skew):
    ranking = jax.random.permutation(own_key, amount)
    crowded, ordinary = load_shares(amount, rows * top, reach, skew, True), load_shares(amount, rows * top, reach, skew, False)
    places = jnp.arange(amount)

    def named(sizes, turn):
        used = int((sizes > 0).sum())
        fixed = max(1, used // 4)
        passed = fixed + (places - fixed + turn * (used - fixed)) % max(1, amount - fixed)
        return jnp.zeros((amount,), jnp.int32).at[ranking[jnp.where(places < fixed, places, passed)]].set(jnp.asarray(sizes, jnp.int32))

    sizes = jnp.where(number % 4 == 0, named(crowded, number // 4), named(ordinary, number - number // 4 - 1))
    mixed = jax.random.permutation(jax.random.fold_in(own, 3), amount)
    giver, receiver = mixed[0:amount // 2 * 2:2], mixed[1:amount // 2 * 2:2]
    slack = jnp.minimum(sizes[giver] - 1, reach - sizes[receiver]) // 2
    slack = jnp.where((giver == ranking[0]) | (receiver == ranking[0]) | (sizes[receiver] == 0), 0, jnp.maximum(slack, 0))
    passed = jax.random.randint(jax.random.fold_in(own, 4), (amount // 2,), 0, 1 << 20) % (slack + 1)
    sizes = sizes.at[giver].add(-passed).at[receiver].add(passed)
    members = jnp.searchsorted(jnp.cumsum(sizes), jnp.arange(rows * top), side="right").astype(jnp.int32)
    grid = members.reshape(top, rows).T
    grid = grid[jax.random.permutation(jax.random.fold_in(own, 1), rows)]
    turn = jax.random.randint(jax.random.fold_in(own, 2), (rows, 1), 0, top)
    return jnp.take_along_axis(grid, (jnp.arange(top)[None, :] + turn) % top, axis=1)


def load_shares(amount, total, reach, lean, full):
    weights = [(1 << 20) // math.isqrt(grade ** lean) + 1 for grade in range(1, amount + 1)]
    largest = reach if full else min(reach, max(-(-total // amount), total * weights[0] // sum(weights)))
    least = 1 if total - largest >= amount - 1 else 0
    given, surplus = [largest] + [least] * (amount - 1), total - largest - least * (amount - 1)
    while surplus > 0:
        movable = [i for i in range(1, amount) if given[i] < largest] or [i for i in range(1, amount) if given[i] < reach]
        mass, budget = sum([weights[i] for i in movable]), surplus
        for i in movable:
            extra = min(reach - given[i], max(1, budget * weights[i] // mass), surplus)
            given[i] = given[i] + extra
            surplus = surplus - extra
    return np.array(given)


def gaussian(stream_key, shape, width, limit, shards=(), kind=jnp.bfloat16):
    loudness = levels(stream_key, shape, shards, -0.22, 0.18) if shards else 1.0
    entries = jax.random.normal(stream_key, shape, jnp.float32) * width * loudness
    return jnp.minimum(jnp.maximum(entries, -limit), limit).astype(kind)


def gaussian_with(rng, dims, scale, bound, cuts, heavy, kind=jnp.bfloat16):
    values = scale * jax.random.normal(rng, dims, jnp.float32)
    if cuts:
        values = values * levels(rng, dims, cuts, -0.22, 0.18)
    return jnp.clip(with_spikes(values, jax.random.fold_in(rng, 3), *heavy), -bound, bound).astype(kind)


def setup_inputs(seed: int = 0) -> dict:
    splits = jax.random.split(jax.random.key(seed), 13)
    d_out = gaussian_with(splits[0], (SEQUENCE_TOKENS, D), 1.0, 6.0, ((0, 8),), (0, 1, 8, 2.0))
    route_expert_keys = jax.random.split(jax.random.fold_in(splits[1], 1), SEQUENCE_TOKENS // TOK_DEV)
    route_expert_turns = jax.random.permutation(jax.random.fold_in(splits[1], 3), SEQUENCE_TOKENS // TOK_DEV)
    route_expert = jax.vmap(lambda own, number: assign_block(jax.random.fold_in(splits[1], 2), own, number, TOK_DEV, EXPERTS, 2, CAP, 0))(route_expert_keys, route_expert_turns).reshape((SEQUENCE_TOKENS, 2))
    route_weight = jnp.clip(0.2 + 0.8 * jax.random.uniform(splits[2], (SEQUENCE_TOKENS, 2), jnp.float32) ** levels(splits[2], (SEQUENCE_TOKENS, 2), ((0, 8),), -0.2, 0.2), 0.2, 1.0)
    expert_inputs = gaussian(splits[3], (EXPERTS, EXPERTS * CAP, D), 1.0, 6.0, ((0, 8),))
    w_gate = gaussian(splits[4], (EXPERTS, D, FF), D ** -0.5, 0.125, ((0, 8), (2, 4)))
    w_up = gaussian(splits[5], (EXPERTS, D, FF), D ** -0.5, 0.125, ((0, 8), (2, 4)))
    w_down = gaussian(splits[6], (EXPERTS, FF, D), FF ** -0.5, 0.109375, ((0, 8), (1, 4)))
    w_out = gaussian(splits[7], (D, MIXER_HEADS * DV), (MIXER_HEADS * DV) ** -0.5, 0.1875, ((1, 4),))
    queries = gaussian(splits[8], (SEQUENCE_TOKENS, MIXER_HEADS, KEY_CHANNELS), 1.0, 6.0, ((0, 8), (1, 4)))
    keys = gaussian(splits[9], (SEQUENCE_TOKENS, MIXER_HEADS, KEY_CHANNELS), (SEQUENCE_TOKENS ** -0.25), 2.0, ((0, 8), (1, 4)))
    values = gaussian(splits[10], (SEQUENCE_TOKENS, MIXER_HEADS, DV), 1.0, 6.0, ((0, 8), (1, 4)))
    log_decay = draw_log_decay(jax.random.fold_in(splits[12], 71), 0)
    return dict(d_out=d_out, route_expert=route_expert, route_weight=route_weight, expert_inputs=expert_inputs, w_gate=w_gate, w_up=w_up, w_down=w_down, w_out=w_out, queries=queries, keys=keys, values=values, log_decay=log_decay)


precise = lax.Precision.HIGHEST

def block_mixer(scaled_queries, keys_in, values_in, decay_in, initial):
    length, head_count, _ = scaled_queries.shape
    value_width = values_in.shape[-1]
    count_blocks = length // BLK

    def to_blocks(tensor):
        return tensor.reshape(count_blocks, BLK, head_count, tensor.shape[-1]).transpose(0, 2, 1, 3)
    causal = jnp.tril(jnp.ones((BLK, BLK), dtype=bool))[:, :, None]

    def advance(carry_state, inputs):
        query_block, key_block, value_block, decay_block = inputs
        cumulative = jnp.cumsum(decay_block, axis=1)
        ending = cumulative[:, -1, :]
        carried = jnp.einsum('hcd,hde->hce', query_block * jnp.exp(cumulative), carry_state, precision=precise)
        within = jnp.where(causal, jnp.exp(cumulative[:, :, None, :] - cumulative[:, None, :, :]), 0.0)
        scores = jnp.einsum('hid,hjd,hijd->hij', query_block, key_block, within, precision=precise)
        inner_part = jnp.einsum('hij,hje->hie', scores, value_block, precision=precise)
        faded_keys = key_block * jnp.exp(ending[:, None, :] - cumulative)
        carry_state = carry_state * jnp.exp(ending)[:, :, None] + jnp.einsum('hcd,hce->hde', faded_keys, value_block, precision=precise)
        return (carry_state, carried + inner_part)
    final_state, blocks_out = lax.scan(jax.checkpoint(advance), initial, (to_blocks(scaled_queries), to_blocks(keys_in), to_blocks(values_in), to_blocks(decay_in)))
    return (blocks_out.transpose(0, 2, 1, 3).reshape(length, head_count, value_width), final_state)

def expert_pass(rows_in, routed_rows, gate_w, up_w, down_w):
    gate_pre = jnp.dot(rows_in, gate_w, preferred_element_type=jnp.float32)
    up_pre = jnp.dot(rows_in, up_w, preferred_element_type=jnp.float32)
    sigmoid_gate = jax.nn.sigmoid(gate_pre)
    active = gate_pre * sigmoid_gate
    hidden = (active * up_pre).astype(jnp.bfloat16)
    d_hidden = lax.dot_general(routed_rows, down_w, (((1,), (1,)), ((), ())), preferred_element_type=jnp.float32)
    d_gate = (d_hidden * up_pre * sigmoid_gate * (1.0 + gate_pre * (1.0 - sigmoid_gate))).astype(jnp.bfloat16)
    d_up = (d_hidden * active).astype(jnp.bfloat16)
    rows_first = (((0,), (0,)), ((), ()))
    grad_gate = lax.dot_general(rows_in, d_gate, rows_first, preferred_element_type=jnp.float32).astype(jnp.bfloat16)
    grad_up = lax.dot_general(rows_in, d_up, rows_first, preferred_element_type=jnp.float32).astype(jnp.bfloat16)
    grad_down = lax.dot_general(hidden, routed_rows, rows_first, preferred_element_type=jnp.float32).astype(jnp.bfloat16)
    return (grad_gate, grad_up, grad_down, d_gate, d_up)

def reference(d_out, route_expert, route_weight, expert_inputs, w_gate, w_up, w_down, w_out, queries, keys, values, log_decay):
    per_block = route_expert.reshape(N_SP, 2 * TOK_DEV).astype(jnp.int32)
    onehot = (per_block[:, :, None] == jnp.arange(EXPERTS, dtype=jnp.int32)[None, None, :]).astype(jnp.int32)
    before = jnp.cumsum(onehot, axis=1) - onehot
    rank_slot = lax.optimization_barrier(jnp.sum(before * onehot, axis=2))
    source_dev = jnp.arange(N_SP, dtype=jnp.int32)[:, None]
    slot_index = (per_block * (N_SP * CAP) + source_dev * CAP + rank_slot).reshape(-1).astype(jnp.int32)
    scaled = (jnp.repeat(d_out, 2, axis=0).astype(jnp.float32) * route_weight.reshape(-1)[:, None]).astype(jnp.bfloat16)
    routed = jnp.zeros((EXPERTS * N_SP * CAP, D), jnp.bfloat16).at[slot_index].set(scaled).reshape(EXPERTS, N_SP * CAP, D)
    part_width = FF // N_TP

    def one_expert(operands):
        rows_in, routed_rows, gate_w, up_w, down_w = operands
        grad_gate, grad_up, grad_down, d_gate, d_up = expert_pass(rows_in, routed_rows, gate_w, up_w, down_w)
        total = jnp.zeros((rows_in.shape[0], D), jnp.float32)
        for piece in range(N_TP):
            lower = piece * part_width
            term = lax.dot_general(d_gate[:, lower:lower + part_width], gate_w[:, lower:lower + part_width], (((1,), (1,)), ((), ())), preferred_element_type=jnp.float32)
            term = term + lax.dot_general(d_up[:, lower:lower + part_width], up_w[:, lower:lower + part_width], (((1,), (1,)), ((), ())), preferred_element_type=jnp.float32)
            total = total + lax.optimization_barrier(term.astype(jnp.bfloat16)).astype(jnp.float32)
        return (grad_gate, grad_up, grad_down, total.astype(jnp.bfloat16))
    grad_gate, grad_up, grad_down, row_grads = lax.map(one_expert, (expert_inputs, routed, w_gate, w_up, w_down))
    picked = row_grads.reshape(-1, D)[slot_index].astype(jnp.float32).reshape(SEQUENCE_TOKENS, 2, D).sum(axis=1)
    mix_grad = (d_out.astype(jnp.float32) + picked).astype(jnp.bfloat16)
    scale_q = KEY_CHANNELS ** (-0.5)
    initial = jnp.zeros((MIXER_HEADS, KEY_CHANNELS, DV), jnp.float32)

    def mixer_map(query_x, key_x, value_x, decay_x):
        return block_mixer(query_x * scale_q, key_x, value_x, decay_x, initial)[0]
    mixer_out, pullback = jax.vjp(mixer_map, queries.astype(jnp.float32), keys.astype(jnp.float32), values.astype(jnp.float32), log_decay)
    mixed = mixer_out.reshape(SEQUENCE_TOKENS, MIXER_HEADS * DV).astype(jnp.bfloat16)
    grad_proj = lax.dot_general(mix_grad, mixed, (((0,), (0,)), ((), ())), preferred_element_type=jnp.float32)
    d_mixed = jnp.dot(mix_grad, w_out, preferred_element_type=jnp.float32).reshape(SEQUENCE_TOKENS, MIXER_HEADS, DV)
    grad_q, grad_k, grad_v, grad_g = pullback(d_mixed)
    return (grad_gate, grad_up, grad_down, grad_proj, grad_q.astype(jnp.bfloat16), grad_k.astype(jnp.bfloat16), grad_v.astype(jnp.bfloat16), grad_g)
```

```python
import functools

import jax
import jax.numpy as jnp
from jax import lax
from jax.experimental import pallas as pl
from jax.experimental.pallas import tpu as pltpu
from jax.sharding import PartitionSpec as P

BLK = 64


precise = lax.Precision.HIGHEST


MESH = pl.DeviceIdType.MESH
NN = (((1,), (0,)), ((), ()))
NT = (((1,), (1,)), ((), ()))
TN = (((0,), (0,)), ((), ()))


def mm(a, b, dims):
    return lax.dot_general(a, b, dims, preferred_element_type=jnp.float32)


def triangle(lower):
    rows = lax.broadcasted_iota(jnp.int32, (BLK, BLK), 0)
    cols = lax.broadcasted_iota(jnp.int32, (BLK, BLK), 1)
    return rows >= cols if lower else rows <= cols


def block_sums(mask, x):
    return lax.dot_general(
        mask.astype(jnp.float32), x, NN, precision=precise, preferred_element_type=jnp.float32
    )


def decays(g_ref, rows):
    cumulative = block_sums(triangle(True), g_ref[rows, :])
    middle = cumulative[BLK // 2 - 1 : BLK // 2, :]
    ending = cumulative[BLK - 1 : BLK, :]
    return cumulative, middle, ending


def greet(n, me, tp=None):
    barrier = pltpu.get_barrier_semaphore()
    others = [{"sp": lax.rem(me + k, n)} for k in range(1, n)]
    if tp is not None:
        others += [{"tp": other} for other in tp]
    for other in others:
        pl.semaphore_signal(barrier, inc=1, device_id=other, device_id_type=MESH)
    return barrier, len(others)


def route_kernel(
    n,
    tp,
    cap,
    d_ref,
    expert_ref,
    weight_ref,
    routed_ref,
    slot_ref,
    outbox,
    ssem,
    rsem,
    lsem,
    tsend,
    trecv,
):
    me = lax.axis_index("sp")
    col = lax.axis_index("tp")
    partner = col + 1 - 2 * lax.rem(col, 2)
    far = [lax.rem(col + 2 * s, tp) for s in range(1, tp // 2)]
    barrier, greeted = greet(n, me, [partner] + far)
    tokens = d_ref.shape[0]
    quarter = outbox.shape[2]
    start = pl.multiple_of(lax.axis_index("tp") * quarter, quarter)
    own = d_ref[:, pl.ds(start, quarter)].astype(jnp.float32)
    kinds = lax.broadcasted_iota(jnp.int32, (n, tokens), 0)
    named = [(kinds == expert_ref[j : j + 1, :]).astype(jnp.float32) for j in range(2)]
    earlier = lax.broadcasted_iota(jnp.int32, (tokens, tokens), 0) < lax.broadcasted_iota(
        jnp.int32, (tokens, tokens), 1
    )
    before = mm((named[0] + named[1]).astype(jnp.bfloat16), earlier.astype(jnp.bfloat16), NN)
    scaled = []
    slots = []
    for j in range(2):
        rank = jnp.sum(before * named[j], axis=0, keepdims=True).astype(jnp.int32)
        slots.append(expert_ref[j : j + 1, :] * cap + rank)
        slot_ref[j : j + 1, :] = slots[j]
        scaled.append((own * weight_ref[:, j : j + 1]).astype(jnp.bfloat16))
    places = lax.broadcasted_iota(jnp.int32, (cap, tokens), 0)
    for e in range(n):
        rows = jnp.zeros((cap, quarter), jnp.float32)
        for j in range(2):
            picks = (slots[j] - e * cap == places).astype(jnp.float32).astype(jnp.bfloat16)
            rows = rows + mm(picks, scaled[j], NN)
        outbox[e] = rows.astype(jnp.bfloat16)
    pl.semaphore_wait(barrier, greeted)

    def place(row, column):
        return routed_ref.at[row, :, pl.ds(pl.multiple_of(column * quarter, quarter), quarter)]

    copies = []
    for k in range(1, n):
        peer = lax.rem(me + k, n)
        copies.append(
            pltpu.make_async_remote_copy(
                src_ref=outbox.at[peer],
                dst_ref=place(me, col),
                send_sem=ssem.at[k - 1],
                recv_sem=rsem.at[k - 1],
                device_id={"sp": peer},
                device_id_type=MESH,
            )
        )
        copies[-1].start()
    stays = pltpu.make_async_copy(outbox.at[me], place(me, col), lsem)
    stays.start()

    def send(k, column, slot, target):
        row = lax.rem(me - k + n, n)
        return pltpu.make_async_remote_copy(
            src_ref=place(row, column),
            dst_ref=place(row, column),
            send_sem=tsend.at[k, slot],
            recv_sem=trecv.at[k, slot],
            device_id={"tp": target},
            device_id_type=MESH,
        )

    across, beside, passed = [], [], []

    def pass_on(k):
        for s in range(len(far)):
            across[k][s].wait_recv()
            column = lax.rem(col - 2 * (s + 1) + tp, tp)
            passed.append(send(k, column, tp // 2 + s, partner))
            passed[-1].start()

    for k in range(n):
        if k == 0:
            stays.wait()
        else:
            copies[k - 1].wait_recv()
        across.append([send(k, col, s + 1, far[s]) for s in range(len(far))])
        for copy in across[k]:
            copy.start()
        beside.append(send(k, col, 0, partner))
        beside[k].start()
        if k > 1:
            pass_on(k - 2)
    for k in range(max(n - 2, 0), n):
        pass_on(k)
    for copy in copies:
        copy.wait_send()
    for row in across:
        for copy in row:
            copy.wait_send()
    for copy in beside + passed:
        copy.wait()


def exchange(n, me, source, target, ssem, rsem, lsem):
    copies = []
    for k in range(1, n):
        peer = lax.rem(me + k, n)
        copies.append(
            pltpu.make_async_remote_copy(
                src_ref=source.at[peer],
                dst_ref=target.at[me],
                send_sem=ssem.at[k - 1],
                recv_sem=rsem.at[k - 1],
                device_id={"sp": peer},
                device_id_type=MESH,
            )
        )
    for copy in copies:
        copy.start()
    stays = pltpu.make_async_copy(source.at[me], target.at[me], lsem)
    stays.start()
    stays.wait()
    for copy in copies:
        copy.wait()


def return_kernel(
    n, tp, cap, sums_ref, slot_ref, d_ref, gathered_ref, back, ssem, rsem, lsem, tsend, trecv
):
    me = lax.axis_index("sp")
    col = lax.axis_index("tp")
    partner = col + 1 - 2 * lax.rem(col, 2)
    far = [lax.rem(col + 2 * s, tp) for s in range(1, tp // 2)]
    barrier, greeted = greet(n, me, [partner] + far)
    pl.semaphore_wait(barrier, greeted)
    exchange(n, me, sums_ref, back, ssem, rsem, lsem)
    tokens = d_ref.shape[0]
    quarter = back.shape[2]
    start = pl.multiple_of(col * quarter, quarter)
    places = lax.broadcasted_iota(jnp.int32, (cap, tokens), 0)
    picked = jnp.zeros((tokens, quarter), jnp.float32)
    for e in range(n):
        here = jnp.zeros((cap, tokens), jnp.float32)
        for j in range(2):
            here = here + (slot_ref[j : j + 1, :] - e * cap == places).astype(jnp.float32)
        picked = picked + mm(here.astype(jnp.bfloat16), back[e], TN)
    own = d_ref[:, pl.ds(start, quarter)].astype(jnp.float32)
    gathered_ref[col] = (own + picked).astype(jnp.bfloat16)

    def send(block, slot, target):
        return pltpu.make_async_remote_copy(
            src_ref=gathered_ref.at[block],
            dst_ref=gathered_ref.at[block],
            send_sem=tsend.at[slot],
            recv_sem=trecv.at[slot],
            device_id={"tp": target},
            device_id_type=MESH,
        )

    across = [send(col, s + 1, far[s]) for s in range(len(far))]
    beside = send(col, 0, partner)
    for copy in across:
        copy.start()
    beside.start()
    passed = []
    for s in range(len(far)):
        across[s].wait_recv()
        block = lax.rem(col - 2 * (s + 1) + tp, tp)
        passed.append(send(block, tp // 2 + s, partner))
        passed[s].start()
    for copy in across:
        copy.wait_send()
    beside.wait()
    for copy in passed:
        copy.wait()


def state_copies(n, me, step, send_ref, recv_ref, send_sem, recv_sem):
    return [
        pltpu.make_async_remote_copy(
            src_ref=send_ref,
            dst_ref=recv_ref.at[k - 1],
            send_sem=send_sem.at[k - 1],
            recv_sem=recv_sem.at[k - 1],
            device_id={"sp": lax.rem(me + step * k + n, n)},
            device_id_type=MESH,
        )
        for k in range(1, n)
    ]


def collect(n, me, step, copies, recv_ref, total, width):
    total[...] = jnp.zeros_like(total)
    for k in range(n - 1, 0, -1):
        copies[k - 1].wait()
        source = me - step * k
        reached = jnp.logical_and(source >= 0, source < n)

        @pl.when(reached)
        def _():
            factor = recv_ref[k - 1, width : width + 1, :].astype(jnp.float32)
            total[...] = total[...] * factor + recv_ref[k - 1, :width, :].astype(jnp.float32)


def forward_kernel(
    n, scale, q_ref, k_ref, v_ref, g_ref, mixed_ref, states_ref, kept, total, send, recv, ssem, rsem
):
    me = lax.axis_index("sp")
    barrier, greeted = greet(n, me)
    length, width = v_ref.shape
    blocks = length // BLK
    causal = triangle(True)
    local = jnp.zeros(total.shape, jnp.float32)
    ahead = jnp.zeros((1, q_ref.shape[1]), jnp.float32)
    befores = []
    for b in range(blocks):
        rows = pl.ds(b * BLK, BLK)
        cumulative, _, ending = decays(g_ref, rows)
        kept[b] = local
        befores.append(ahead)
        faded = (k_ref[rows, :].astype(jnp.float32) * jnp.exp(ending - cumulative)).astype(
            jnp.bfloat16
        )
        local = local * jnp.exp(ending) + mm(v_ref[rows, :], faded, TN)
        ahead = ahead + ending
    send[:width, :] = local.astype(jnp.bfloat16)
    send[width:, :] = jnp.broadcast_to(jnp.exp(ahead), (16, ahead.shape[1])).astype(jnp.bfloat16)
    pl.semaphore_wait(barrier, greeted)
    copies = state_copies(n, me, 1, send, recv, ssem, rsem)
    for copy in copies:
        copy.start()
    inner = []
    scaled = []
    for b in range(blocks):
        rows = pl.ds(b * BLK, BLK)
        cumulative, middle, _ = decays(g_ref, rows)
        query = q_ref[rows, :].astype(jnp.float32) * scale
        key = k_ref[rows, :].astype(jnp.float32)
        lifted_q = (query * jnp.exp(cumulative - middle)).astype(jnp.bfloat16)
        lifted_k = (key * jnp.exp(middle - cumulative)).astype(jnp.bfloat16)
        scores = jnp.where(causal, mm(lifted_q, lifted_k, NT), 0.0).astype(jnp.bfloat16)
        inner.append(mm(scores, v_ref[rows, :], NN))
        scaled.append((query * jnp.exp(cumulative)).astype(jnp.bfloat16))
    collect(n, me, 1, copies, recv, total, width)
    for b in range(blocks):
        rows = pl.ds(b * BLK, BLK)
        state = (kept[b] + total[...] * jnp.exp(befores[b])).astype(jnp.bfloat16)
        states_ref[b] = state
        mixed_ref[rows, :] = (inner[b] + mm(scaled[b], state, NT)).astype(jnp.bfloat16)


def backward_kernel(
    n,
    scale,
    q_ref,
    k_ref,
    v_ref,
    g_ref,
    grad_ref,
    w_ref,
    mixed_ref,
    states_ref,
    gq_ref,
    gk_ref,
    gv_ref,
    gg_ref,
    proj_ref,
    kept,
    total,
    send,
    recv,
    ssem,
    rsem,
    d_ref,
    part,
    pair_in,
    pair,
    parts_in,
    psend,
    precv,
):
    me = lax.axis_index("sp")
    barrier, greeted = greet(n, me)
    length, width = v_ref.shape
    blocks = length // BLK
    causal = triangle(True)
    local = jnp.zeros(total.shape, jnp.float32)
    pieces, _, quarter = grad_ref.shape
    d_mixed = jnp.zeros((length, width), jnp.float32)
    for p in range(pieces):
        d_mixed = d_mixed + mm(grad_ref[p], w_ref[p * quarter : (p + 1) * quarter, :], NN)
    d_ref[...] = d_mixed.astype(jnp.bfloat16)
    after = jnp.zeros((1, q_ref.shape[1]), jnp.float32)
    afters = [None] * blocks
    for b in reversed(range(blocks)):
        rows = pl.ds(b * BLK, BLK)
        cumulative, _, ending = decays(g_ref, rows)
        kept[b] = local
        afters[b] = after
        query = q_ref[rows, :].astype(jnp.float32) * scale
        scaled = (query * jnp.exp(cumulative)).astype(jnp.bfloat16)
        local = local * jnp.exp(ending) + mm(d_ref[rows, :], scaled, TN)
        after = after + ending
    send[:width, :] = local.astype(jnp.bfloat16)
    send[width:, :] = jnp.broadcast_to(jnp.exp(after), (16, after.shape[1])).astype(jnp.bfloat16)
    pl.semaphore_wait(barrier, greeted)
    copies = state_copies(n, me, -1, send, recv, ssem, rsem)
    for copy in copies:
        copy.start()
    half, share = part.shape[1:3]
    per = quarter // share
    for p in range(pieces):
        product = mm(grad_ref[p], mixed_ref[...], TN).astype(jnp.bfloat16)
        for i in range(per):
            at = p * per + i
            part[at % 2, at // 2] = product[i * share : (i + 1) * share, :]
    parity = lax.rem(me, 2)
    mine = me // 2
    pairing = pltpu.make_async_remote_copy(
        src_ref=part.at[1 - parity],
        dst_ref=pair_in,
        send_sem=psend.at[0],
        recv_sem=precv.at[0],
        device_id={"sp": me + 1 - 2 * parity},
        device_id_type=MESH,
    )
    pairing.start()
    change = []
    key_part = []
    for b in range(blocks):
        rows = pl.ds(b * BLK, BLK)
        cumulative, middle, _ = decays(g_ref, rows)
        query = q_ref[rows, :].astype(jnp.float32) * scale
        key = k_ref[rows, :].astype(jnp.float32)
        value = v_ref[rows, :]
        d_out = d_ref[rows, :]
        rise, fall = jnp.exp(cumulative - middle), jnp.exp(middle - cumulative)
        lifted_q = (query * rise).astype(jnp.bfloat16)
        lifted_k = (key * fall).astype(jnp.bfloat16)
        scores = jnp.where(causal, mm(lifted_q, lifted_k, NT), 0.0).astype(jnp.bfloat16)
        d_scores = jnp.where(causal, mm(d_out, value, NT), 0.0).astype(jnp.bfloat16)
        d_lifted_q = mm(d_scores, lifted_k, NN)
        d_lifted_k = mm(d_scores, lifted_q, TN)
        grown = jnp.exp(cumulative)
        d_carried = mm(d_out, states_ref[b], NN) * grown
        gq_ref[rows, :] = ((d_lifted_q * rise + d_carried) * scale).astype(jnp.bfloat16)
        change.append(
            lifted_q.astype(jnp.float32) * d_lifted_q
            - lifted_k.astype(jnp.float32) * d_lifted_k
            + query * d_carried
        )
        key_part.append(d_lifted_k * fall)
        gg_ref[rows, :] = change[b]
        gv_ref[rows, :] = mm(scores, d_out, TN).astype(gv_ref.dtype)
    pairing.wait()
    for i in range(half):
        pair[i] = (part[parity, i].astype(jnp.float32) + pair_in[i].astype(jnp.float32)).astype(
            jnp.bfloat16
        )
    collect(n, me, -1, copies, recv, total, width)
    shares = []
    for s in range(1, half):
        other = lax.rem(mine + s, half)
        shares.append(
            pltpu.make_async_remote_copy(
                src_ref=pair.at[other],
                dst_ref=parts_in.at[s - 1],
                send_sem=psend.at[s],
                recv_sem=precv.at[s],
                device_id={"sp": 2 * other + parity},
                device_id_type=MESH,
            )
        )
        shares[-1].start()
    for b in range(blocks):
        rows = pl.ds(b * BLK, BLK)
        cumulative, _, ending = decays(g_ref, rows)
        d_state = kept[b] + total[...] * jnp.exp(afters[b])
        d_rounded = d_state.astype(jnp.bfloat16)
        key = k_ref[rows, :].astype(jnp.float32)
        fade = jnp.exp(ending - cumulative)
        faded = key * fade
        d_faded = mm(v_ref[rows, :], d_rounded, NN)
        gk_ref[rows, :] = (key_part[b] + d_faded * fade).astype(jnp.bfloat16)
        gv_ref[rows, :] = gv_ref[rows, :] + mm(faded.astype(jnp.bfloat16), d_rounded, NT)
        moved = faded * d_faded
        at_end = jnp.sum(moved, axis=0, keepdims=True) + jnp.exp(ending) * jnp.sum(
            states_ref[b].astype(jnp.float32) * d_state, axis=0, keepdims=True
        )
        gg_ref[rows, :] = block_sums(triangle(False), gg_ref[rows, :] - moved) + at_end
    summed = pair[mine].astype(jnp.float32)
    for s in range(1, half):
        shares[s - 1].wait()
        summed = summed + parts_in[s - 1].astype(jnp.float32)
    proj_ref[...] = summed


def exchange_scratch(n, blocks, width, channels):
    return [
        pltpu.VMEM((blocks, width, channels), jnp.float32),
        pltpu.VMEM((width, channels), jnp.float32),
        pltpu.VMEM((width + 16, channels), jnp.bfloat16),
        pltpu.VMEM((n - 1, width + 16, channels), jnp.bfloat16),
        pltpu.SemaphoreType.DMA((n - 1,)),
        pltpu.SemaphoreType.DMA((n - 1,)),
    ]


def in_vmem(count):
    return [pl.BlockSpec(memory_space=pltpu.VMEM)] * count


def mixer_forward(q, k, v, g, scale):
    n = lax.axis_size("sp")
    length, channels = q.shape
    width = v.shape[1]
    blocks = length // BLK
    return pl.pallas_call(
        functools.partial(forward_kernel, n, scale),
        out_shape=(
            jax.ShapeDtypeStruct((length, width), jnp.bfloat16),
            jax.ShapeDtypeStruct((blocks, width, channels), jnp.bfloat16),
        ),
        in_specs=in_vmem(4),
        out_specs=tuple(in_vmem(2)),
        scratch_shapes=exchange_scratch(n, blocks, width, channels),
        compiler_params=pltpu.CompilerParams(
            collective_id=1, has_side_effects=True, vmem_limit_bytes=16 * 1024 * 1024
        ),
        cost_estimate=pl.CostEstimate(
            flops=4_000_000_000, bytes_accessed=4 * length * width, transcendentals=0
        ),
        name="mixer_forward",
    )(q, k, v, g)


def mixer_backward(q, k, v, g, gathered, w_out, mixed, states, scale):
    n = lax.axis_size("sp")
    length, channels = q.shape
    width = v.shape[1]
    blocks = length // BLK
    share = w_out.shape[0] // n
    return pl.pallas_call(
        functools.partial(backward_kernel, n, scale),
        out_shape=(
            jax.ShapeDtypeStruct((length, channels), jnp.bfloat16),
            jax.ShapeDtypeStruct((length, channels), jnp.bfloat16),
            jax.ShapeDtypeStruct((length, width), jnp.float32),
            jax.ShapeDtypeStruct((length, channels), jnp.float32),
            jax.ShapeDtypeStruct((share, width), jnp.float32),
        ),
        in_specs=in_vmem(8),
        out_specs=tuple(in_vmem(5)),
        scratch_shapes=exchange_scratch(n, blocks, width, channels)
        + [
            pltpu.VMEM((length, width), jnp.bfloat16),
            pltpu.VMEM((2, n // 2, share, width), jnp.bfloat16),
            pltpu.VMEM((n // 2, share, width), jnp.bfloat16),
            pltpu.VMEM((n // 2, share, width), jnp.bfloat16),
            pltpu.VMEM((n // 2 - 1, share, width), jnp.bfloat16),
            pltpu.SemaphoreType.DMA((n // 2,)),
            pltpu.SemaphoreType.DMA((n // 2,)),
        ],
        compiler_params=pltpu.CompilerParams(
            collective_id=2, has_side_effects=True, vmem_limit_bytes=24 * 1024 * 1024
        ),
        cost_estimate=pl.CostEstimate(
            flops=8_000_000_000, bytes_accessed=4 * length * width, transcendentals=0
        ),
        name="mixer_backward",
    )(q, k, v, g, gathered, w_out, mixed, states)


def route_out(d_out, route_expert, route_weight, capacity):
    n, tp = lax.axis_size("sp"), lax.axis_size("tp")
    tokens, model_width = d_out.shape
    quarter = model_width // tp
    return pl.pallas_call(
        functools.partial(route_kernel, n, tp, capacity),
        out_shape=(
            jax.ShapeDtypeStruct((n, capacity, model_width), jnp.bfloat16),
            jax.ShapeDtypeStruct((2, tokens), jnp.int32),
        ),
        in_specs=in_vmem(3),
        out_specs=tuple(in_vmem(2)),
        scratch_shapes=[
            pltpu.VMEM((n, capacity, quarter), jnp.bfloat16),
            pltpu.SemaphoreType.DMA((n - 1,)),
            pltpu.SemaphoreType.DMA((n - 1,)),
            pltpu.SemaphoreType.DMA,
            pltpu.SemaphoreType.DMA((n, tp)),
            pltpu.SemaphoreType.DMA((n, tp)),
        ],
        compiler_params=pltpu.CompilerParams(
            collective_id=3, has_side_effects=True, vmem_limit_bytes=24 * 1024 * 1024
        ),
        cost_estimate=pl.CostEstimate(
            flops=8_000_000_000, bytes_accessed=4 * tokens * quarter, transcendentals=0
        ),
        name="route_out",
    )(d_out, route_expert.T, route_weight)


def route_back(summed, slots, d_out):
    n, tp = lax.axis_size("sp"), lax.axis_size("tp")
    capacity, quarter = summed.shape[1:]
    tokens = d_out.shape[0]
    return pl.pallas_call(
        functools.partial(return_kernel, n, tp, capacity),
        out_shape=jax.ShapeDtypeStruct((tp, tokens, quarter), jnp.bfloat16),
        in_specs=in_vmem(3),
        out_specs=in_vmem(1)[0],
        scratch_shapes=[
            pltpu.VMEM((n, capacity, quarter), jnp.bfloat16),
            pltpu.SemaphoreType.DMA((n - 1,)),
            pltpu.SemaphoreType.DMA((n - 1,)),
            pltpu.SemaphoreType.DMA,
            pltpu.SemaphoreType.DMA((tp,)),
            pltpu.SemaphoreType.DMA((tp,)),
        ],
        compiler_params=pltpu.CompilerParams(
            collective_id=4, has_side_effects=True, vmem_limit_bytes=24 * 1024 * 1024
        ),
        cost_estimate=pl.CostEstimate(
            flops=8_000_000_000, bytes_accessed=4 * tokens * quarter, transcendentals=0
        ),
        name="route_back",
    )(summed, slots, d_out)


def expert_pass(rows_in, routed_rows, gate_w, up_w, down_w):
    gate_pre = jnp.dot(rows_in, gate_w, preferred_element_type=jnp.float32)
    up_pre = jnp.dot(rows_in, up_w, preferred_element_type=jnp.float32)
    sigmoid_gate = jax.nn.sigmoid(gate_pre)
    active = gate_pre * sigmoid_gate
    hidden = (active * up_pre).astype(jnp.bfloat16)
    d_hidden = lax.dot_general(
        routed_rows, down_w, (((1,), (1,)), ((), ())), preferred_element_type=jnp.float32
    )
    d_gate = (d_hidden * up_pre * sigmoid_gate * (1.0 + gate_pre * (1.0 - sigmoid_gate))).astype(
        jnp.bfloat16
    )
    d_up = (d_hidden * active).astype(jnp.bfloat16)
    rows_first = (((0,), (0,)), ((), ()))
    grad_gate = lax.dot_general(
        rows_in, d_gate, rows_first, preferred_element_type=jnp.float32
    ).astype(jnp.bfloat16)
    grad_up = lax.dot_general(rows_in, d_up, rows_first, preferred_element_type=jnp.float32).astype(
        jnp.bfloat16
    )
    grad_down = lax.dot_general(
        hidden, routed_rows, rows_first, preferred_element_type=jnp.float32
    ).astype(jnp.bfloat16)
    return (grad_gate, grad_up, grad_down, d_gate, d_up)


def local(
    d_out,
    route_expert,
    route_weight,
    expert_inputs,
    w_gate,
    w_up,
    w_down,
    w_out,
    queries,
    keys,
    values,
    log_decay,
):
    model_width = d_out.shape[1]
    experts = lax.axis_size("sp")
    capacity = expert_inputs.shape[1] // experts
    quarter = model_width // lax.axis_size("tp")
    routed, slots = route_out(d_out, route_expert, route_weight, capacity)
    routed = routed.reshape(experts * capacity, model_width)
    rows_in = expert_inputs[0]
    gate_w = w_gate[0]
    up_w = w_up[0]
    grad_gate, grad_up, grad_down, d_gate, d_up = expert_pass(
        rows_in, routed, gate_w, up_w, w_down[0]
    )
    partial_terms = lax.dot_general(
        d_gate, gate_w, (((1,), (1,)), ((), ())), preferred_element_type=jnp.float32
    )
    partial_terms = partial_terms + lax.dot_general(
        d_up, up_w, (((1,), (1,)), ((), ())), preferred_element_type=jnp.float32
    )
    rounded = lax.optimization_barrier(partial_terms.astype(jnp.bfloat16)).astype(jnp.float32)
    summed = lax.psum_scatter(rounded.astype(jnp.bfloat16), "tp", scatter_dimension=1, tiled=True)
    scale_q = queries.shape[2] ** (-0.5)
    q, k, v, g = queries[:, 0], keys[:, 0], values[:, 0], log_decay[:, 0]
    mixed, states = mixer_forward(q, k, v, g, scale_q)
    summed, mixed, grad_gate, grad_up, grad_down = lax.optimization_barrier(
        (summed, mixed, grad_gate, grad_up, grad_down)
    )
    gathered = route_back(summed.reshape(experts, capacity, quarter), slots, d_out)
    grad_q, grad_k, grad_v, grad_g, grad_proj = mixer_backward(
        q, k, v, g, gathered, w_out, mixed, states, scale_q
    )
    return (
        grad_gate[None],
        grad_up[None],
        grad_down[None],
        grad_proj,
        grad_q[:, None],
        grad_k[:, None],
        grad_v.astype(jnp.bfloat16)[:, None],
        grad_g[:, None],
    )


def paired(me, offset):
    other = me
    bit = 1
    while bit <= offset:
        if offset & bit:
            other = other + bit - 2 * bit * lax.rem(me // bit, 2)
        bit *= 2
    return other


def prefix_copy(n, me, step, distance, index, send, recv, ssem, rsem):
    return pltpu.make_async_remote_copy(
        src_ref=send.at[index],
        dst_ref=recv.at[index],
        send_sem=ssem.at[index],
        recv_sem=rsem.at[index],
        device_id={"sp": lax.rem(me + step * distance + n, n)},
        device_id_type=MESH,
    )


def prefix_send(n, me, step, distance, index, local, ahead, scan, send, recv, ssem, rsem):
    width = local.shape[0]
    total, reach = scan
    decay = reach[0:1, :] * ahead[0:1, :]
    send[index, :width, :] = (total[...] * ahead[0:1, :] + local[...]).astype(jnp.bfloat16)
    send[index, width:, :] = jnp.broadcast_to(decay, (16, decay.shape[1])).astype(jnp.bfloat16)
    target = me + step * distance

    @pl.when(jnp.logical_and(target >= 0, target < n))
    def _():
        prefix_copy(n, me, step, distance, index, send, recv, ssem, rsem).start()


def prefix_take(n, me, step, distance, index, scan, send, recv, ssem, rsem):
    total, reach = scan
    width = total.shape[0]
    source = me - step * distance
    target = me + step * distance
    copy = prefix_copy(n, me, step, distance, index, send, recv, ssem, rsem)

    @pl.when(jnp.logical_and(target >= 0, target < n))
    def _():
        copy.wait_send()

    @pl.when(jnp.logical_and(source >= 0, source < n))
    def _():
        copy.wait_recv()
        total[...] = total[...] + recv[index, :width, :].astype(jnp.float32) * reach[0:1, :]
        reach[...] = reach[...] * recv[index, width : width + 1, :].astype(jnp.float32)


def distances(n):
    found = []
    step = 1
    while step < n:
        found.append(step)
        step *= 2
    return found


def expert_kernel(
    n,
    cap,
    scale,
    d_hbm,
    expert_ref,
    weight_ref,
    x_hbm,
    wg_hbm,
    wu_hbm,
    wd_hbm,
    q_ref,
    k_ref,
    v_ref,
    g_ref,
    grad_gate,
    grad_up,
    grad_down,
    gathered_ref,
    mixed_ref,
    states_ref,
    d_ref,
    x_ref,
    wg_ref,
    wu_ref,
    wd_ref,
    routed,
    onehot,
    outbox,
    outbox_near,
    slope,
    active,
    hidden,
    d_gate,
    d_up,
    part,
    pair_in,
    far_out,
    far_in,
    sums,
    back,
    picked,
    turned,
    stage,
    cum,
    kept,
    befores,
    inner,
    scaled,
    mix_local,
    mix_ahead,
    mix_total,
    mix_reach,
    mix_send,
    mix_recv,
    lsem,
    osem,
    rs,
    rr,
    fs,
    fr,
    ps,
    pr,
    qs,
    qr,
    ds,
    dr,
    xs,
    xr,
    bs,
    br,
    ms,
    mr,
    gs,
    gr,
):
    me = lax.axis_index("sp")
    col = lax.axis_index("tp")
    core = lax.rem(col, 2)
    side = col // 2
    partner = col + 1 - 2 * core
    far = lax.rem(col + 2, 4)
    chunks = n // 2
    rows2 = 2 * cap
    tokens = d_ref.shape[0]
    model = d_ref.shape[1]
    quarter = model // 4
    half = model // 2

    barrier, greeted = greet(n, me, [partner, far])

    def chunk_rows(z):
        return pl.ds(z * rows2, rows2)

    def block_rows(m):
        return pl.ds(m * cap, cap)

    def columns(q):
        return pl.ds(pl.multiple_of(q * quarter, quarter), quarter)

    order = [0] + list(range(chunks - 1, 0, -1))
    loads = {}

    def load(name, source, target, index):
        loads[name] = pltpu.make_async_copy(source, target, lsem.at[index])
        loads[name].start()

    load("d", d_hbm, d_ref, 0)
    load("wg", wg_hbm, wg_ref, 1)

    def load_rows(z):
        for m in (2 * z, 2 * z + 1):
            first = pl.multiple_of(paired(me, m) * cap, cap)
            load(("x", m), x_hbm.at[pl.ds(first, cap), :], x_ref.at[block_rows(m), :], 4 + m)

    load_rows(0)
    load("wu", wu_hbm, wu_ref, 2)
    load("wd", wd_hbm, wd_ref, 3)
    for z in order[1:]:
        load_rows(z)

    kinds = lax.broadcasted_iota(jnp.int32, (n, tokens), 0)
    named = [(kinds == expert_ref[j : j + 1, :]).astype(jnp.float32) for j in range(2)]
    earlier = lax.broadcasted_iota(jnp.int32, (tokens, tokens), 0) < lax.broadcasted_iota(
        jnp.int32, (tokens, tokens), 1
    )
    before = mm((named[0] + named[1]).astype(jnp.bfloat16), earlier.astype(jnp.bfloat16), NN)
    slots = []
    for j in range(2):
        rank = jnp.sum(before * named[j], axis=0, keepdims=True).astype(jnp.int32)
        slots.append(expert_ref[j : j + 1, :] * cap + rank)
    places = lax.broadcasted_iota(jnp.int32, (cap, tokens), 0)

    def routed_rows(m, chosen):
        first = paired(me, m) * cap
        hits = [(slots[j] - first == places).astype(jnp.float32) for j in range(2)]
        both = (hits[0] + hits[1]).astype(jnp.bfloat16)
        onehot[block_rows(m), :] = both
        weight = jnp.sum(
            hits[0] * weight_ref[0:1, :] + hits[1] * weight_ref[1:2, :], axis=1, keepdims=True
        )
        return (mm(both, chosen, NN) * weight).astype(jnp.bfloat16)

    def route(m):
        if m == 1:
            source = outbox_near
            target = routed.at[block_rows(1), pl.ds(pl.multiple_of(core * half, half), half)]
        else:
            source = outbox.at[block_rows(m), :]
            target = routed.at[block_rows(m), columns(col)]
        return pltpu.make_async_remote_copy(
            src_ref=source,
            dst_ref=target,
            send_sem=rs.at[m],
            recv_sem=rr.at[m],
            device_id={"sp": paired(me, m)},
            device_id_type=MESH,
        )

    def pass_on(m, what, target, send_sem, recv_sem):
        if m == 1:
            piece = routed.at[block_rows(1), pl.ds(pl.multiple_of(what * half, half), half)]
        else:
            piece = routed.at[block_rows(m), columns(what)]
        return pltpu.make_async_remote_copy(
            src_ref=piece,
            dst_ref=piece,
            send_sem=send_sem.at[m],
            recv_sem=recv_sem.at[m],
            device_id={"tp": target},
            device_id_type=MESH,
        )

    sent = []
    loads["d"].wait()
    sends = []
    for z in order[1:]:
        sends += [2 * z, 2 * z + 1]
    sends.insert(1, 1)
    greeting = True
    for m in sends:
        if m == 1:
            outbox_near[...] = routed_rows(
                1, d_ref[:, pl.ds(pl.multiple_of(core * half, half), half)]
            )
        else:
            outbox[block_rows(m), :] = routed_rows(m, d_ref[:, columns(col)])
        if greeting:
            pl.semaphore_wait(barrier, greeted)
            greeting = False
        sent.append(route(m))
        sent[-1].start()
    routed[block_rows(0), :] = routed_rows(0, d_ref[...])

    crossed, beside, relayed = {}, {}, {}

    def arrive(m):
        route(m).wait_recv()
        if m == 1:
            beside[m] = pass_on(1, core, partner, ps, pr)
            beside[m].start()
            return
        crossed[m] = pass_on(m, col, far, fs, fr)
        crossed[m].start()
        beside[m] = pass_on(m, col, partner, ps, pr)
        beside[m].start()

    def relay(m):
        crossed[m].wait_recv()
        relayed[m] = pass_on(m, far, partner, qs, qr)
        relayed[m].start()

    def complete(m):
        beside[m].wait_recv()
        if m > 1:
            relayed[m].wait_recv()

    def gates(z):
        rows = chunk_rows(z)
        loads[("x", 2 * z)].wait()
        loads[("x", 2 * z + 1)].wait()
        if z == 0:
            loads["wg"].wait()
        gate = mm(x_ref[rows, :], wg_ref[...], NT)
        if z == 0:
            loads["wu"].wait()
        up = mm(x_ref[rows, :], wu_ref[...], NT)
        sigmoid = jax.nn.sigmoid(gate)
        silu = gate * sigmoid
        hidden[rows, :] = (silu * up).astype(jnp.bfloat16)
        active[rows, :] = silu
        slope[rows, :] = up * sigmoid * (1.0 + gate * (1.0 - sigmoid))

    halves = {}

    def experts(z):
        rows = chunk_rows(z)
        if z == 0:
            loads["wd"].wait()
        d_hidden = mm(routed[rows, :], wd_ref[...], NT)
        d_gate[rows, :] = (d_hidden * slope[rows, :]).astype(jnp.bfloat16)
        d_up[rows, :] = (d_hidden * active[rows, :]).astype(jnp.bfloat16)
        for whose in (1 - core, core):
            for i in range(2):
                across = 1 - side if i == 0 else side
                cut = columns(2 * across + whose)
                term = mm(d_gate[rows, :], wg_ref[:, cut], NN) + mm(
                    d_up[rows, :], wu_ref[:, cut], NN
                )
                part[rows, cut] = term.astype(jnp.bfloat16)
            if (z, 0) in halves:
                continue
            for i in range(2):
                across = 1 - side if i == 0 else side
                halves[(z, i)] = pltpu.make_async_remote_copy(
                    src_ref=part.at[rows, columns(2 * across + 1 - core)],
                    dst_ref=pair_in.at[i, rows, :],
                    send_sem=ds.at[z, i],
                    recv_sem=dr.at[z, i],
                    device_id={"tp": partner},
                    device_id_type=MESH,
                )
                halves[(z, i)].start()

    over = {}

    def reduce_near(z):
        rows = chunk_rows(z)
        halves[(z, 0)].wait_recv()
        far_out[rows, :] = (
            part[rows, columns(far)].astype(jnp.float32)
            + pair_in[0, rows, :].astype(jnp.float32)
        ).astype(jnp.bfloat16)
        over[z] = pltpu.make_async_remote_copy(
            src_ref=far_out.at[rows, :],
            dst_ref=far_in.at[rows, :],
            send_sem=xs.at[z],
            recv_sem=xr.at[z],
            device_id={"tp": far},
            device_id_type=MESH,
        )
        over[z].start()

    returned = {}

    def reduce_far(z):
        rows = chunk_rows(z)
        halves[(z, 1)].wait_recv()
        over[z].wait_recv()
        sums[rows, :] = (
            part[rows, columns(col)].astype(jnp.float32)
            + pair_in[1, rows, :].astype(jnp.float32)
            + far_in[rows, :].astype(jnp.float32)
        ).astype(jnp.bfloat16)
        for m in (2 * z, 2 * z + 1):
            if m == 0:
                back[block_rows(0), :] = sums[block_rows(0), :]
                continue
            returned[m] = pltpu.make_async_remote_copy(
                src_ref=sums.at[block_rows(m), :],
                dst_ref=back.at[block_rows(m), :],
                send_sem=bs.at[m],
                recv_sem=br.at[m],
                device_id={"sp": paired(me, m)},
                device_id_type=MESH,
            )
            returned[m].start()

    def pick(z):
        rows = chunk_rows(z)
        for m in (2 * z, 2 * z + 1):
            if m > 0:
                returned[m].wait_recv()
        found = mm(onehot[rows, :], back[rows, :], TN)
        picked[...] = found if z == 0 else picked[...] + found

    stored = {}
    used = [0]

    def weight_grad(lhs, rhs, out, name):
        turned[...] = lhs[...].T

        def piece(i):
            slot = used[0] % 2
            if used[0] >= 2:
                stored[used[0] - 2].wait()
            stage[slot] = mm(turned[...], rhs[:, i * quarter : (i + 1) * quarter], NN).astype(
                jnp.bfloat16
            )
            stored[used[0]] = pltpu.make_async_copy(
                stage.at[slot], out.at[:, pl.ds(i * quarter, quarter)], osem.at[slot]
            )
            stored[used[0]].start()
            used[0] += 1

        for i in range(4):
            piece(i)

    blocks = tokens // BLK
    causal = triangle(True)
    width = v_ref.shape[1]
    scan = (mix_total, mix_reach)
    reach = distances(n)

    def mixer_states():
        local = jnp.zeros(mix_total.shape, jnp.float32)
        ahead = jnp.zeros((1, q_ref.shape[1]), jnp.float32)
        for b in range(blocks):
            rows = pl.ds(b * BLK, BLK)
            cumulative, _, ending = decays(g_ref, rows)
            cum[rows, :] = cumulative
            kept[b] = local
            befores[b : b + 1, :] = jnp.exp(ahead)
            faded = (k_ref[rows, :].astype(jnp.float32) * jnp.exp(ending - cumulative)).astype(
                jnp.bfloat16
            )
            local = local * jnp.exp(ending) + mm(v_ref[rows, :], faded, TN)
            ahead = ahead + ending
        mix_local[...] = local
        mix_ahead[...] = jnp.broadcast_to(jnp.exp(ahead), mix_ahead.shape)
        mix_total[...] = jnp.zeros(mix_total.shape, jnp.float32)
        mix_reach[...] = jnp.ones(mix_reach.shape, jnp.float32)

    def mixer_send(index):
        prefix_send(
            n, me, 1, reach[index], index, mix_local, mix_ahead, scan, mix_send, mix_recv, ms, mr
        )

    def mixer_take(index):
        prefix_take(n, me, 1, reach[index], index, scan, mix_send, mix_recv, ms, mr)

    def mixer_inner():
        for b in range(blocks):
            rows = pl.ds(b * BLK, BLK)
            cumulative = cum[rows, :]
            middle = cumulative[BLK // 2 - 1 : BLK // 2, :]
            query = q_ref[rows, :].astype(jnp.float32) * scale
            key = k_ref[rows, :].astype(jnp.float32)
            lifted_q = (query * jnp.exp(cumulative - middle)).astype(jnp.bfloat16)
            lifted_k = (key * jnp.exp(middle - cumulative)).astype(jnp.bfloat16)
            scores = jnp.where(causal, mm(lifted_q, lifted_k, NT), 0.0).astype(jnp.bfloat16)
            inner[rows, :] = mm(scores, v_ref[rows, :], NN)
            scaled[rows, :] = (query * jnp.exp(cumulative)).astype(jnp.bfloat16)

    def mixer_finish():
        for b in range(blocks):
            rows = pl.ds(b * BLK, BLK)
            state = (kept[b] + mix_total[...] * befores[b : b + 1, :]).astype(jnp.bfloat16)
            states_ref[b] = state
            mixed_ref[rows, :] = (inner[rows, :] + mm(scaled[rows, :], state, NT)).astype(
                jnp.bfloat16
            )

    rounds = len(reach)
    taken = [0]

    def mixer_round():
        if taken[0] < rounds:
            mixer_take(taken[0])
            taken[0] += 1
            if taken[0] < rounds:
                mixer_send(taken[0])

    gates(0)
    arrive(1)
    mixer_states()
    mixer_send(0)
    complete(1)
    experts(0)
    waiting = 0
    early = order[1:]
    for i, z in enumerate(early):
        pair = (2 * z, 2 * z + 1)
        for m in pair:
            arrive(m)
        reduce_near(order[i])
        gates(z)
        mixer_round()
        for m in pair:
            relay(m)
        if i == 0:
            mixer_inner()
        for m in pair:
            complete(m)
        reduce_far(order[i])
        experts(z)
    while taken[0] < rounds:
        mixer_round()
    reduce_near(order[-1])
    mixer_finish()
    weight_grad(hidden, routed, grad_down, 0)
    reduce_far(order[-1])
    weight_grad(d_gate, x_ref, grad_gate, 1)
    for z in order[:-2]:
        pick(z)
    weight_grad(d_up, x_ref, grad_up, 2)
    for z in order[-2:]:
        pick(z)
    own = d_ref[:, columns(col)].astype(jnp.float32)
    gathered_ref[col] = (own + picked[...]).astype(jnp.bfloat16)

    def share(block, slot, target):
        return pltpu.make_async_remote_copy(
            src_ref=gathered_ref.at[block],
            dst_ref=gathered_ref.at[block],
            send_sem=gs.at[slot],
            recv_sem=gr.at[slot],
            device_id={"tp": target},
            device_id_type=MESH,
        )

    last = [share(col, 0, far), share(col, 1, partner)]
    for copy in last:
        copy.start()
    for copy in sent:
        copy.wait_send()
    for group in (crossed, beside, relayed, halves, over, returned):
        for copy in group.values():
            copy.wait_send()
    for i in (used[0] - 2, used[0] - 1):
        stored[i].wait()
    last[0].wait_recv()
    last.append(share(far, 2, partner))
    last[2].start()
    last[0].wait_send()
    last[1].wait()
    last[2].wait()


def expert_stage(d_out, route_expert, route_weight, rows_in, gate_t, up_t, down, q, k, v, g, cap, scale):
    n = lax.axis_size("sp")
    tokens, model = d_out.shape
    quarter = model // 4
    units = down.shape[0]
    slots = n * cap
    channels, width = q.shape[1], v.shape[1]
    blocks = tokens // BLK
    rounds = len(distances(n))
    bf16, f32 = jnp.bfloat16, jnp.float32
    weight_shape = jax.ShapeDtypeStruct((units, model), bf16)
    anywhere = pl.BlockSpec(memory_space=pl.ANY)
    local = pl.BlockSpec(memory_space=pltpu.VMEM)
    dma = pltpu.SemaphoreType.DMA
    return pl.pallas_call(
        functools.partial(expert_kernel, n, cap, scale),
        out_shape=(
            weight_shape,
            weight_shape,
            weight_shape,
            jax.ShapeDtypeStruct((4, tokens, quarter), bf16),
            jax.ShapeDtypeStruct((tokens, width), bf16),
            jax.ShapeDtypeStruct((blocks, width, channels), bf16),
        ),
        in_specs=[anywhere, local, local] + [anywhere] * 4 + [local] * 4,
        out_specs=(anywhere, anywhere, anywhere, local, local, local),
        scratch_shapes=[
            pltpu.VMEM((tokens, model), bf16),
            pltpu.VMEM((slots, model), bf16),
            pltpu.VMEM((units, model), bf16),
            pltpu.VMEM((units, model), bf16),
            pltpu.VMEM((units, model), bf16),
            pltpu.VMEM((slots, model), bf16),
            pltpu.VMEM((slots, tokens), bf16),
            pltpu.VMEM((slots, quarter), bf16),
            pltpu.VMEM((cap, model // 2), bf16),
            pltpu.VMEM((slots, units), f32),
            pltpu.VMEM((slots, units), f32),
            pltpu.VMEM((slots, units), bf16),
            pltpu.VMEM((slots, units), bf16),
            pltpu.VMEM((slots, units), bf16),
            pltpu.VMEM((slots, model), bf16),
            pltpu.VMEM((2, slots, quarter), bf16),
            pltpu.VMEM((slots, quarter), bf16),
            pltpu.VMEM((slots, quarter), bf16),
            pltpu.VMEM((slots, quarter), bf16),
            pltpu.VMEM((slots, quarter), bf16),
            pltpu.VMEM((tokens, quarter), f32),
            pltpu.VMEM((units, slots), bf16),
            pltpu.VMEM((2, units, quarter), bf16),
            pltpu.VMEM((tokens, channels), f32),
            pltpu.VMEM((blocks, width, channels), f32),
            pltpu.VMEM((blocks, channels), f32),
            pltpu.VMEM((tokens, width), f32),
            pltpu.VMEM((tokens, channels), bf16),
            pltpu.VMEM((width, channels), f32),
            pltpu.VMEM((8, channels), f32),
            pltpu.VMEM((width, channels), f32),
            pltpu.VMEM((8, channels), f32),
            pltpu.VMEM((rounds, width + 16, channels), bf16),
            pltpu.VMEM((rounds, width + 16, channels), bf16),
            dma((4 + n,)),
            dma((2,)),
            dma((n,)),
            dma((n,)),
            dma((n,)),
            dma((n,)),
            dma((n,)),
            dma((n,)),
            dma((n,)),
            dma((n,)),
            dma((n // 2, 2)),
            dma((n // 2, 2)),
            dma((n // 2,)),
            dma((n // 2,)),
            dma((n,)),
            dma((n,)),
            dma((rounds,)),
            dma((rounds,)),
            dma((3,)),
            dma((3,)),
        ],
        compiler_params=pltpu.CompilerParams(
            collective_id=5, has_side_effects=True, vmem_limit_bytes=60 * 1024 * 1024
        ),
        cost_estimate=pl.CostEstimate(
            flops=60_000_000_000, bytes_accessed=30_000_000, transcendentals=0
        ),
        name="expert_stage",
    )(d_out, route_expert.T, route_weight.T, rows_in, gate_t, up_t, down, q, k, v, g)


def fused_local(
    d_out,
    route_expert,
    route_weight,
    expert_inputs,
    w_gate,
    w_up,
    w_down,
    w_out,
    queries,
    keys,
    values,
    log_decay,
):
    experts = lax.axis_size("sp")
    capacity = expert_inputs.shape[1] // experts
    scale_q = queries.shape[2] ** (-0.5)
    q, k, v, g = queries[:, 0], keys[:, 0], values[:, 0], log_decay[:, 0]
    grad_gate, grad_up, grad_down, gathered, mixed, states = expert_stage(
        d_out,
        route_expert,
        route_weight,
        expert_inputs[0],
        w_gate[0].T,
        w_up[0].T,
        w_down[0],
        q,
        k,
        v,
        g,
        capacity,
        scale_q,
    )
    grad_q, grad_k, grad_v, grad_g, grad_proj = mixer_backward(
        q, k, v, g, gathered, w_out, mixed, states, scale_q
    )
    return (
        grad_gate.T[None],
        grad_up.T[None],
        grad_down[None],
        grad_proj,
        grad_q[:, None],
        grad_k[:, None],
        grad_v.astype(jnp.bfloat16)[:, None],
        grad_g[:, None],
    )


def choose(*arrays):
    n, tp = lax.axis_size("sp"), lax.axis_size("tp")
    tokens, model = arrays[0].shape
    capacity = arrays[3].shape[1] // n
    power = n & (n - 1) == 0 and n > 2
    if tp == 4 and power and capacity % 16 == 0 and n * capacity <= 1536 and model % 512 == 0:
        return fused_local(*arrays)
    return local(*arrays)


def solution(mesh):
    return jax.shard_map(
        choose,
        mesh=mesh,
        in_specs=(
            P("sp", None),
            P("sp", None),
            P("sp", None),
            P("sp", None, None),
            P("sp", None, "tp"),
            P("sp", None, "tp"),
            P("sp", "tp", None),
            P(None, "tp"),
            P("sp", "tp", None),
            P("sp", "tp", None),
            P("sp", "tp", None),
            P("sp", "tp", None),
        ),
        out_specs=(
            P("sp", None, "tp"),
            P("sp", None, "tp"),
            P("sp", "tp", None),
            P("sp", "tp"),
            P("sp", "tp", None),
            P("sp", "tp", None),
            P("sp", "tp", None),
            P("sp", "tp", None),
        ),
        check_vma=False,
    )
```

```python
import functools

import jax
import jax.numpy as jnp
from jax import lax
from jax.experimental import pallas as pl
from jax.experimental.pallas import tpu as pltpu
from jax.sharding import PartitionSpec as P

BLK = 64


precise = lax.Precision.HIGHEST


MESH = pl.DeviceIdType.MESH
NN = (((1,), (0,)), ((), ()))
NT = (((1,), (1,)), ((), ()))
TN = (((0,), (0,)), ((), ()))


def mm(a, b, dims):
    return lax.dot_general(a, b, dims, preferred_element_type=jnp.float32)


def triangle(lower):
    rows = lax.broadcasted_iota(jnp.int32, (BLK, BLK), 0)
    cols = lax.broadcasted_iota(jnp.int32, (BLK, BLK), 1)
    return rows >= cols if lower else rows <= cols


def block_sums(mask, x):
    return lax.dot_general(
        mask.astype(jnp.float32), x, NN, precision=precise, preferred_element_type=jnp.float32
    )


def decays(g_ref, rows):
    cumulative = block_sums(triangle(True), g_ref[rows, :])
    middle = cumulative[BLK // 2 - 1 : BLK // 2, :]
    ending = cumulative[BLK - 1 : BLK, :]
    return cumulative, middle, ending


def greet(n, me, tp=None):
    barrier = pltpu.get_barrier_semaphore()
    others = [{"sp": lax.rem(me + k, n)} for k in range(1, n)]
    if tp is not None:
        others += [{"tp": other} for other in tp]
    for other in others:
        pl.semaphore_signal(barrier, inc=1, device_id=other, device_id_type=MESH)
    return barrier, len(others)


def route_kernel(
    n,
    tp,
    cap,
    d_ref,
    expert_ref,
    weight_ref,
    routed_ref,
    slot_ref,
    outbox,
    ssem,
    rsem,
    lsem,
    tsend,
    trecv,
):
    me = lax.axis_index("sp")
    col = lax.axis_index("tp")
    partner = col + 1 - 2 * lax.rem(col, 2)
    far = [lax.rem(col + 2 * s, tp) for s in range(1, tp // 2)]
    barrier, greeted = greet(n, me, [partner] + far)
    tokens = d_ref.shape[0]
    quarter = outbox.shape[2]
    start = pl.multiple_of(lax.axis_index("tp") * quarter, quarter)
    own = d_ref[:, pl.ds(start, quarter)].astype(jnp.float32)
    kinds = lax.broadcasted_iota(jnp.int32, (n, tokens), 0)
    named = [(kinds == expert_ref[j : j + 1, :]).astype(jnp.float32) for j in range(2)]
    earlier = lax.broadcasted_iota(jnp.int32, (tokens, tokens), 0) < lax.broadcasted_iota(
        jnp.int32, (tokens, tokens), 1
    )
    before = mm((named[0] + named[1]).astype(jnp.bfloat16), earlier.astype(jnp.bfloat16), NN)
    scaled = []
    slots = []
    for j in range(2):
        rank = jnp.sum(before * named[j], axis=0, keepdims=True).astype(jnp.int32)
        slots.append(expert_ref[j : j + 1, :] * cap + rank)
        slot_ref[j : j + 1, :] = slots[j]
        scaled.append((own * weight_ref[:, j : j + 1]).astype(jnp.bfloat16))
    places = lax.broadcasted_iota(jnp.int32, (cap, tokens), 0)
    for e in range(n):
        rows = jnp.zeros((cap, quarter), jnp.float32)
        for j in range(2):
            picks = (slots[j] - e * cap == places).astype(jnp.float32).astype(jnp.bfloat16)
            rows = rows + mm(picks, scaled[j], NN)
        outbox[e] = rows.astype(jnp.bfloat16)
    pl.semaphore_wait(barrier, greeted)

    def place(row, column):
        return routed_ref.at[row, :, pl.ds(pl.multiple_of(column * quarter, quarter), quarter)]

    copies = []
    for k in range(1, n):
        peer = lax.rem(me + k, n)
        copies.append(
            pltpu.make_async_remote_copy(
                src_ref=outbox.at[peer],
                dst_ref=place(me, col),
                send_sem=ssem.at[k - 1],
                recv_sem=rsem.at[k - 1],
                device_id={"sp": peer},
                device_id_type=MESH,
            )
        )
        copies[-1].start()
    stays = pltpu.make_async_copy(outbox.at[me], place(me, col), lsem)
    stays.start()

    def send(k, column, slot, target):
        row = lax.rem(me - k + n, n)
        return pltpu.make_async_remote_copy(
            src_ref=place(row, column),
            dst_ref=place(row, column),
            send_sem=tsend.at[k, slot],
            recv_sem=trecv.at[k, slot],
            device_id={"tp": target},
            device_id_type=MESH,
        )

    across, beside, passed = [], [], []

    def pass_on(k):
        for s in range(len(far)):
            across[k][s].wait_recv()
            column = lax.rem(col - 2 * (s + 1) + tp, tp)
            passed.append(send(k, column, tp // 2 + s, partner))
            passed[-1].start()

    for k in range(n):
        if k == 0:
            stays.wait()
        else:
            copies[k - 1].wait_recv()
        across.append([send(k, col, s + 1, far[s]) for s in range(len(far))])
        for copy in across[k]:
            copy.start()
        beside.append(send(k, col, 0, partner))
        beside[k].start()
        if k > 1:
            pass_on(k - 2)
    for k in range(max(n - 2, 0), n):
        pass_on(k)
    for copy in copies:
        copy.wait_send()
    for row in across:
        for copy in row:
            copy.wait_send()
    for copy in beside + passed:
        copy.wait()


def exchange(n, me, source, target, ssem, rsem, lsem):
    copies = []
    for k in range(1, n):
        peer = lax.rem(me + k, n)
        copies.append(
            pltpu.make_async_remote_copy(
                src_ref=source.at[peer],
                dst_ref=target.at[me],
                send_sem=ssem.at[k - 1],
                recv_sem=rsem.at[k - 1],
                device_id={"sp": peer},
                device_id_type=MESH,
            )
        )
    for copy in copies:
        copy.start()
    stays = pltpu.make_async_copy(source.at[me], target.at[me], lsem)
    stays.start()
    stays.wait()
    for copy in copies:
        copy.wait()


def return_kernel(
    n, tp, cap, sums_ref, slot_ref, d_ref, gathered_ref, back, ssem, rsem, lsem, tsend, trecv
):
    me = lax.axis_index("sp")
    col = lax.axis_index("tp")
    partner = col + 1 - 2 * lax.rem(col, 2)
    far = [lax.rem(col + 2 * s, tp) for s in range(1, tp // 2)]
    barrier, greeted = greet(n, me, [partner] + far)
    pl.semaphore_wait(barrier, greeted)
    exchange(n, me, sums_ref, back, ssem, rsem, lsem)
    tokens = d_ref.shape[0]
    quarter = back.shape[2]
    start = pl.multiple_of(col * quarter, quarter)
    places = lax.broadcasted_iota(jnp.int32, (cap, tokens), 0)
    picked = jnp.zeros((tokens, quarter), jnp.float32)
    for e in range(n):
        here = jnp.zeros((cap, tokens), jnp.float32)
        for j in range(2):
            here = here + (slot_ref[j : j + 1, :] - e * cap == places).astype(jnp.float32)
        picked = picked + mm(here.astype(jnp.bfloat16), back[e], TN)
    own = d_ref[:, pl.ds(start, quarter)].astype(jnp.float32)
    gathered_ref[col] = (own + picked).astype(jnp.bfloat16)

    def send(block, slot, target):
        return pltpu.make_async_remote_copy(
            src_ref=gathered_ref.at[block],
            dst_ref=gathered_ref.at[block],
            send_sem=tsend.at[slot],
            recv_sem=trecv.at[slot],
            device_id={"tp": target},
            device_id_type=MESH,
        )

    across = [send(col, s + 1, far[s]) for s in range(len(far))]
    beside = send(col, 0, partner)
    for copy in across:
        copy.start()
    beside.start()
    passed = []
    for s in range(len(far)):
        across[s].wait_recv()
        block = lax.rem(col - 2 * (s + 1) + tp, tp)
        passed.append(send(block, tp // 2 + s, partner))
        passed[s].start()
    for copy in across:
        copy.wait_send()
    beside.wait()
    for copy in passed:
        copy.wait()


def state_copies(n, me, step, send_ref, recv_ref, send_sem, recv_sem):
    return [
        pltpu.make_async_remote_copy(
            src_ref=send_ref,
            dst_ref=recv_ref.at[k - 1],
            send_sem=send_sem.at[k - 1],
            recv_sem=recv_sem.at[k - 1],
            device_id={"sp": lax.rem(me + step * k + n, n)},
            device_id_type=MESH,
        )
        for k in range(1, n)
    ]


def collect(n, me, step, copies, recv_ref, total, width):
    total[...] = jnp.zeros_like(total)
    for k in range(n - 1, 0, -1):
        copies[k - 1].wait()
        source = me - step * k
        reached = jnp.logical_and(source >= 0, source < n)

        @pl.when(reached)
        def _():
            factor = recv_ref[k - 1, width : width + 1, :].astype(jnp.float32)
            total[...] = total[...] * factor + recv_ref[k - 1, :width, :].astype(jnp.float32)


def forward_kernel(
    n, scale, q_ref, k_ref, v_ref, g_ref, mixed_ref, states_ref, kept, total, send, recv, ssem, rsem
):
    me = lax.axis_index("sp")
    barrier, greeted = greet(n, me)
    length, width = v_ref.shape
    blocks = length // BLK
    causal = triangle(True)
    local = jnp.zeros(total.shape, jnp.float32)
    ahead = jnp.zeros((1, q_ref.shape[1]), jnp.float32)
    befores = []
    for b in range(blocks):
        rows = pl.ds(b * BLK, BLK)
        cumulative, _, ending = decays(g_ref, rows)
        kept[b] = local
        befores.append(ahead)
        faded = (k_ref[rows, :].astype(jnp.float32) * jnp.exp(ending - cumulative)).astype(
            jnp.bfloat16
        )
        local = local * jnp.exp(ending) + mm(v_ref[rows, :], faded, TN)
        ahead = ahead + ending
    send[:width, :] = local.astype(jnp.bfloat16)
    send[width:, :] = jnp.broadcast_to(jnp.exp(ahead), (16, ahead.shape[1])).astype(jnp.bfloat16)
    pl.semaphore_wait(barrier, greeted)
    copies = state_copies(n, me, 1, send, recv, ssem, rsem)
    for copy in copies:
        copy.start()
    inner = []
    scaled = []
    for b in range(blocks):
        rows = pl.ds(b * BLK, BLK)
        cumulative, middle, _ = decays(g_ref, rows)
        query = q_ref[rows, :].astype(jnp.float32) * scale
        key = k_ref[rows, :].astype(jnp.float32)
        lifted_q = (query * jnp.exp(cumulative - middle)).astype(jnp.bfloat16)
        lifted_k = (key * jnp.exp(middle - cumulative)).astype(jnp.bfloat16)
        scores = jnp.where(causal, mm(lifted_q, lifted_k, NT), 0.0).astype(jnp.bfloat16)
        inner.append(mm(scores, v_ref[rows, :], NN))
        scaled.append((query * jnp.exp(cumulative)).astype(jnp.bfloat16))
    collect(n, me, 1, copies, recv, total, width)
    for b in range(blocks):
        rows = pl.ds(b * BLK, BLK)
        state = (kept[b] + total[...] * jnp.exp(befores[b])).astype(jnp.bfloat16)
        states_ref[b] = state
        mixed_ref[rows, :] = (inner[b] + mm(scaled[b], state, NT)).astype(jnp.bfloat16)


def backward_kernel(
    n,
    scale,
    q_ref,
    k_ref,
    v_ref,
    g_ref,
    grad_ref,
    w_ref,
    mixed_ref,
    states_ref,
    gq_ref,
    gk_ref,
    gv_ref,
    gg_ref,
    proj_ref,
    kept,
    total,
    send,
    recv,
    ssem,
    rsem,
    d_ref,
    part,
    pair_in,
    pair,
    parts_in,
    psend,
    precv,
):
    me = lax.axis_index("sp")
    barrier, greeted = greet(n, me)
    length, width = v_ref.shape
    blocks = length // BLK
    causal = triangle(True)
    local = jnp.zeros(total.shape, jnp.float32)
    pieces, _, quarter = grad_ref.shape
    d_mixed = jnp.zeros((length, width), jnp.float32)
    for p in range(pieces):
        d_mixed = d_mixed + mm(grad_ref[p], w_ref[p * quarter : (p + 1) * quarter, :], NN)
    d_ref[...] = d_mixed.astype(jnp.bfloat16)
    after = jnp.zeros((1, q_ref.shape[1]), jnp.float32)
    afters = [None] * blocks
    for b in reversed(range(blocks)):
        rows = pl.ds(b * BLK, BLK)
        cumulative, _, ending = decays(g_ref, rows)
        kept[b] = local
        afters[b] = after
        query = q_ref[rows, :].astype(jnp.float32) * scale
        scaled = (query * jnp.exp(cumulative)).astype(jnp.bfloat16)
        local = local * jnp.exp(ending) + mm(d_ref[rows, :], scaled, TN)
        after = after + ending
    send[:width, :] = local.astype(jnp.bfloat16)
    send[width:, :] = jnp.broadcast_to(jnp.exp(after), (16, after.shape[1])).astype(jnp.bfloat16)
    pl.semaphore_wait(barrier, greeted)
    copies = state_copies(n, me, -1, send, recv, ssem, rsem)
    for copy in copies:
        copy.start()
    half, share = part.shape[1:3]
    per = quarter // share
    for p in range(pieces):
        product = mm(grad_ref[p], mixed_ref[...], TN).astype(jnp.bfloat16)
        for i in range(per):
            at = p * per + i
            part[at % 2, at // 2] = product[i * share : (i + 1) * share, :]
    parity = lax.rem(me, 2)
    mine = me // 2
    pairing = pltpu.make_async_remote_copy(
        src_ref=part.at[1 - parity],
        dst_ref=pair_in,
        send_sem=psend.at[0],
        recv_sem=precv.at[0],
        device_id={"sp": me + 1 - 2 * parity},
        device_id_type=MESH,
    )
    pairing.start()
    change = []
    key_part = []
    for b in range(blocks):
        rows = pl.ds(b * BLK, BLK)
        cumulative, middle, _ = decays(g_ref, rows)
        query = q_ref[rows, :].astype(jnp.float32) * scale
        key = k_ref[rows, :].astype(jnp.float32)
        value = v_ref[rows, :]
        d_out = d_ref[rows, :]
        rise, fall = jnp.exp(cumulative - middle), jnp.exp(middle - cumulative)
        lifted_q = (query * rise).astype(jnp.bfloat16)
        lifted_k = (key * fall).astype(jnp.bfloat16)
        scores = jnp.where(causal, mm(lifted_q, lifted_k, NT), 0.0).astype(jnp.bfloat16)
        d_scores = jnp.where(causal, mm(d_out, value, NT), 0.0).astype(jnp.bfloat16)
        d_lifted_q = mm(d_scores, lifted_k, NN)
        d_lifted_k = mm(d_scores, lifted_q, TN)
        grown = jnp.exp(cumulative)
        d_carried = mm(d_out, states_ref[b], NN) * grown
        gq_ref[rows, :] = ((d_lifted_q * rise + d_carried) * scale).astype(jnp.bfloat16)
        change.append(
            lifted_q.astype(jnp.float32) * d_lifted_q
            - lifted_k.astype(jnp.float32) * d_lifted_k
            + query * d_carried
        )
        key_part.append(d_lifted_k * fall)
        gg_ref[rows, :] = change[b]
        gv_ref[rows, :] = mm(scores, d_out, TN).astype(gv_ref.dtype)
    pairing.wait()
    for i in range(half):
        pair[i] = (part[parity, i].astype(jnp.float32) + pair_in[i].astype(jnp.float32)).astype(
            jnp.bfloat16
        )
    collect(n, me, -1, copies, recv, total, width)
    shares = []
    for s in range(1, half):
        other = lax.rem(mine + s, half)
        shares.append(
            pltpu.make_async_remote_copy(
                src_ref=pair.at[other],
                dst_ref=parts_in.at[s - 1],
                send_sem=psend.at[s],
                recv_sem=precv.at[s],
                device_id={"sp": 2 * other + parity},
                device_id_type=MESH,
            )
        )
        shares[-1].start()
    for b in range(blocks):
        rows = pl.ds(b * BLK, BLK)
        cumulative, _, ending = decays(g_ref, rows)
        d_state = kept[b] + total[...] * jnp.exp(afters[b])
        d_rounded = d_state.astype(jnp.bfloat16)
        key = k_ref[rows, :].astype(jnp.float32)
        fade = jnp.exp(ending - cumulative)
        faded = key * fade
        d_faded = mm(v_ref[rows, :], d_rounded, NN)
        gk_ref[rows, :] = (key_part[b] + d_faded * fade).astype(jnp.bfloat16)
        gv_ref[rows, :] = gv_ref[rows, :] + mm(faded.astype(jnp.bfloat16), d_rounded, NT)
        moved = faded * d_faded
        at_end = jnp.sum(moved, axis=0, keepdims=True) + jnp.exp(ending) * jnp.sum(
            states_ref[b].astype(jnp.float32) * d_state, axis=0, keepdims=True
        )
        gg_ref[rows, :] = block_sums(triangle(False), gg_ref[rows, :] - moved) + at_end
    summed = pair[mine].astype(jnp.float32)
    for s in range(1, half):
        shares[s - 1].wait()
        summed = summed + parts_in[s - 1].astype(jnp.float32)
    proj_ref[...] = summed


def exchange_scratch(n, blocks, width, channels):
    return [
        pltpu.VMEM((blocks, width, channels), jnp.float32),
        pltpu.VMEM((width, channels), jnp.float32),
        pltpu.VMEM((width + 16, channels), jnp.bfloat16),
        pltpu.VMEM((n - 1, width + 16, channels), jnp.bfloat16),
        pltpu.SemaphoreType.DMA((n - 1,)),
        pltpu.SemaphoreType.DMA((n - 1,)),
    ]


def in_vmem(count):
    return [pl.BlockSpec(memory_space=pltpu.VMEM)] * count


def mixer_forward(q, k, v, g, scale):
    n = lax.axis_size("sp")
    length, channels = q.shape
    width = v.shape[1]
    blocks = length // BLK
    return pl.pallas_call(
        functools.partial(forward_kernel, n, scale),
        out_shape=(
            jax.ShapeDtypeStruct((length, width), jnp.bfloat16),
            jax.ShapeDtypeStruct((blocks, width, channels), jnp.bfloat16),
        ),
        in_specs=in_vmem(4),
        out_specs=tuple(in_vmem(2)),
        scratch_shapes=exchange_scratch(n, blocks, width, channels),
        compiler_params=pltpu.CompilerParams(
            collective_id=1, has_side_effects=True, vmem_limit_bytes=16 * 1024 * 1024
        ),
        cost_estimate=pl.CostEstimate(
            flops=4_000_000_000, bytes_accessed=4 * length * width, transcendentals=0
        ),
        name="mixer_forward",
    )(q, k, v, g)


def mixer_backward(q, k, v, g, gathered, w_out, mixed, states, scale):
    n = lax.axis_size("sp")
    length, channels = q.shape
    width = v.shape[1]
    blocks = length // BLK
    share = w_out.shape[0] // n
    return pl.pallas_call(
        functools.partial(backward_kernel, n, scale),
        out_shape=(
            jax.ShapeDtypeStruct((length, channels), jnp.bfloat16),
            jax.ShapeDtypeStruct((length, channels), jnp.bfloat16),
            jax.ShapeDtypeStruct((length, width), jnp.float32),
            jax.ShapeDtypeStruct((length, channels), jnp.float32),
            jax.ShapeDtypeStruct((share, width), jnp.float32),
        ),
        in_specs=in_vmem(8),
        out_specs=tuple(in_vmem(5)),
        scratch_shapes=exchange_scratch(n, blocks, width, channels)
        + [
            pltpu.VMEM((length, width), jnp.bfloat16),
            pltpu.VMEM((2, n // 2, share, width), jnp.bfloat16),
            pltpu.VMEM((n // 2, share, width), jnp.bfloat16),
            pltpu.VMEM((n // 2, share, width), jnp.bfloat16),
            pltpu.VMEM((n // 2 - 1, share, width), jnp.bfloat16),
            pltpu.SemaphoreType.DMA((n // 2,)),
            pltpu.SemaphoreType.DMA((n // 2,)),
        ],
        compiler_params=pltpu.CompilerParams(
            collective_id=2, has_side_effects=True, vmem_limit_bytes=24 * 1024 * 1024
        ),
        cost_estimate=pl.CostEstimate(
            flops=8_000_000_000, bytes_accessed=4 * length * width, transcendentals=0
        ),
        name="mixer_backward",
    )(q, k, v, g, gathered, w_out, mixed, states)


def route_out(d_out, route_expert, route_weight, capacity):
    n, tp = lax.axis_size("sp"), lax.axis_size("tp")
    tokens, model_width = d_out.shape
    quarter = model_width // tp
    return pl.pallas_call(
        functools.partial(route_kernel, n, tp, capacity),
        out_shape=(
            jax.ShapeDtypeStruct((n, capacity, model_width), jnp.bfloat16),
            jax.ShapeDtypeStruct((2, tokens), jnp.int32),
        ),
        in_specs=in_vmem(3),
        out_specs=tuple(in_vmem(2)),
        scratch_shapes=[
            pltpu.VMEM((n, capacity, quarter), jnp.bfloat16),
            pltpu.SemaphoreType.DMA((n - 1,)),
            pltpu.SemaphoreType.DMA((n - 1,)),
            pltpu.SemaphoreType.DMA,
            pltpu.SemaphoreType.DMA((n, tp)),
            pltpu.SemaphoreType.DMA((n, tp)),
        ],
        compiler_params=pltpu.CompilerParams(
            collective_id=3, has_side_effects=True, vmem_limit_bytes=24 * 1024 * 1024
        ),
        cost_estimate=pl.CostEstimate(
            flops=8_000_000_000, bytes_accessed=4 * tokens * quarter, transcendentals=0
        ),
        name="route_out",
    )(d_out, route_expert.T, route_weight)


def route_back(summed, slots, d_out):
    n, tp = lax.axis_size("sp"), lax.axis_size("tp")
    capacity, quarter = summed.shape[1:]
    tokens = d_out.shape[0]
    return pl.pallas_call(
        functools.partial(return_kernel, n, tp, capacity),
        out_shape=jax.ShapeDtypeStruct((tp, tokens, quarter), jnp.bfloat16),
        in_specs=in_vmem(3),
        out_specs=in_vmem(1)[0],
        scratch_shapes=[
            pltpu.VMEM((n, capacity, quarter), jnp.bfloat16),
            pltpu.SemaphoreType.DMA((n - 1,)),
            pltpu.SemaphoreType.DMA((n - 1,)),
            pltpu.SemaphoreType.DMA,
            pltpu.SemaphoreType.DMA((tp,)),
            pltpu.SemaphoreType.DMA((tp,)),
        ],
        compiler_params=pltpu.CompilerParams(
            collective_id=4, has_side_effects=True, vmem_limit_bytes=24 * 1024 * 1024
        ),
        cost_estimate=pl.CostEstimate(
            flops=8_000_000_000, bytes_accessed=4 * tokens * quarter, transcendentals=0
        ),
        name="route_back",
    )(summed, slots, d_out)


def expert_pass(rows_in, routed_rows, gate_w, up_w, down_w):
    gate_pre = jnp.dot(rows_in, gate_w, preferred_element_type=jnp.float32)
    up_pre = jnp.dot(rows_in, up_w, preferred_element_type=jnp.float32)
    sigmoid_gate = jax.nn.sigmoid(gate_pre)
    active = gate_pre * sigmoid_gate
    hidden = (active * up_pre).astype(jnp.bfloat16)
    d_hidden = lax.dot_general(
        routed_rows, down_w, (((1,), (1,)), ((), ())), preferred_element_type=jnp.float32
    )
    d_gate = (d_hidden * up_pre * sigmoid_gate * (1.0 + gate_pre * (1.0 - sigmoid_gate))).astype(
        jnp.bfloat16
    )
    d_up = (d_hidden * active).astype(jnp.bfloat16)
    rows_first = (((0,), (0,)), ((), ()))
    grad_gate = lax.dot_general(
        rows_in, d_gate, rows_first, preferred_element_type=jnp.float32
    ).astype(jnp.bfloat16)
    grad_up = lax.dot_general(rows_in, d_up, rows_first, preferred_element_type=jnp.float32).astype(
        jnp.bfloat16
    )
    grad_down = lax.dot_general(
        hidden, routed_rows, rows_first, preferred_element_type=jnp.float32
    ).astype(jnp.bfloat16)
    return (grad_gate, grad_up, grad_down, d_gate, d_up)


def local(
    d_out,
    route_expert,
    route_weight,
    expert_inputs,
    w_gate,
    w_up,
    w_down,
    w_out,
    queries,
    keys,
    values,
    log_decay,
):
    model_width = d_out.shape[1]
    experts = lax.axis_size("sp")
    capacity = expert_inputs.shape[1] // experts
    quarter = model_width // lax.axis_size("tp")
    routed, slots = route_out(d_out, route_expert, route_weight, capacity)
    routed = routed.reshape(experts * capacity, model_width)
    rows_in = expert_inputs[0]
    gate_w = w_gate[0]
    up_w = w_up[0]
    grad_gate, grad_up, grad_down, d_gate, d_up = expert_pass(
        rows_in, routed, gate_w, up_w, w_down[0]
    )
    partial_terms = lax.dot_general(
        d_gate, gate_w, (((1,), (1,)), ((), ())), preferred_element_type=jnp.float32
    )
    partial_terms = partial_terms + lax.dot_general(
        d_up, up_w, (((1,), (1,)), ((), ())), preferred_element_type=jnp.float32
    )
    rounded = lax.optimization_barrier(partial_terms.astype(jnp.bfloat16)).astype(jnp.float32)
    summed = lax.psum_scatter(rounded.astype(jnp.bfloat16), "tp", scatter_dimension=1, tiled=True)
    scale_q = queries.shape[2] ** (-0.5)
    q, k, v, g = queries[:, 0], keys[:, 0], values[:, 0], log_decay[:, 0]
    mixed, states = mixer_forward(q, k, v, g, scale_q)
    summed, mixed, grad_gate, grad_up, grad_down = lax.optimization_barrier(
        (summed, mixed, grad_gate, grad_up, grad_down)
    )
    gathered = route_back(summed.reshape(experts, capacity, quarter), slots, d_out)
    grad_q, grad_k, grad_v, grad_g, grad_proj = mixer_backward(
        q, k, v, g, gathered, w_out, mixed, states, scale_q
    )
    return (
        grad_gate[None],
        grad_up[None],
        grad_down[None],
        grad_proj,
        grad_q[:, None],
        grad_k[:, None],
        grad_v.astype(jnp.bfloat16)[:, None],
        grad_g[:, None],
    )


def paired(me, offset):
    other = me
    bit = 1
    while bit <= offset:
        if offset & bit:
            other = other + bit - 2 * bit * lax.rem(me // bit, 2)
        bit *= 2
    return other


def prefix_copy(n, me, step, distance, index, send, recv, ssem, rsem):
    return pltpu.make_async_remote_copy(
        src_ref=send.at[index],
        dst_ref=recv.at[index],
        send_sem=ssem.at[index],
        recv_sem=rsem.at[index],
        device_id={"sp": lax.rem(me + step * distance + n, n)},
        device_id_type=MESH,
    )


def prefix_send(n, me, step, distance, index, local, ahead, scan, send, recv, ssem, rsem):
    width = local.shape[0]
    total, reach = scan
    decay = reach[0:1, :] * ahead[0:1, :]
    send[index, :width, :] = (total[...] * ahead[0:1, :] + local[...]).astype(jnp.bfloat16)
    send[index, width:, :] = jnp.broadcast_to(decay, (16, decay.shape[1])).astype(jnp.bfloat16)
    target = me + step * distance

    @pl.when(jnp.logical_and(target >= 0, target < n))
    def _():
        prefix_copy(n, me, step, distance, index, send, recv, ssem, rsem).start()


def prefix_take(n, me, step, distance, index, scan, send, recv, ssem, rsem):
    total, reach = scan
    width = total.shape[0]
    source = me - step * distance
    target = me + step * distance
    copy = prefix_copy(n, me, step, distance, index, send, recv, ssem, rsem)

    @pl.when(jnp.logical_and(target >= 0, target < n))
    def _():
        copy.wait_send()

    @pl.when(jnp.logical_and(source >= 0, source < n))
    def _():
        copy.wait_recv()
        total[...] = total[...] + recv[index, :width, :].astype(jnp.float32) * reach[0:1, :]
        reach[...] = reach[...] * recv[index, width : width + 1, :].astype(jnp.float32)


def distances(n):
    found = []
    step = 1
    while step < n:
        found.append(step)
        step *= 2
    return found


def expert_kernel(
    n,
    cap,
    scale,
    d_hbm,
    expert_ref,
    weight_ref,
    x_hbm,
    wg_hbm,
    wu_hbm,
    wd_hbm,
    q_ref,
    k_ref,
    v_ref,
    g_ref,
    w_hbm,
    grad_gate,
    grad_up,
    grad_down,
    grad_proj,
    grad_q,
    grad_k,
    grad_v,
    grad_g,
    wg_ref,
    wu_ref,
    wd_ref,
    proj_ref,
    gq_ref,
    gk_ref,
    gv_ref,
    gg_ref,
    gathered,
    mixed_ref,
    states_ref,
    d_ref,
    x_ref,
    routed,
    onehot,
    outbox,
    outbox_near,
    slope,
    active,
    hidden,
    d_gate,
    d_up,
    part,
    pair_in,
    far_out,
    far_in,
    sums,
    back,
    picked,
    turned,
    cum,
    kept,
    befores,
    inner,
    scaled,
    lifted_q,
    lifted_k,
    scores_ref,
    d_round,
    key_part,
    proj_out,
    proj_pair,
    proj_mine,
    proj_in,
    w_ref,
    mix_local,
    mix_ahead,
    mix_total,
    mix_reach,
    mix_send,
    mix_recv,
    lsem,
    osem,
    rs,
    rr,
    fs,
    fr,
    ps,
    pr,
    qs,
    qr,
    ds,
    dr,
    xs,
    xr,
    bs,
    br,
    ms,
    mr,
    gs,
    gr,
    ys,
    yr,
    zs,
    zr,
):
    me = lax.axis_index("sp")
    col = lax.axis_index("tp")
    core = lax.rem(col, 2)
    side = col // 2
    partner = col + 1 - 2 * core
    far = lax.rem(col + 2, 4)
    chunks = n // 2
    rows2 = 2 * cap
    tokens = d_ref.shape[0]
    model = d_ref.shape[1]
    quarter = model // 4
    half = model // 2
    near = 3

    barrier, greeted = greet(n, me, [partner, far])

    def chunk_rows(z):
        return pl.ds(z * rows2, rows2)

    def block_rows(m):
        return pl.ds(m * cap, cap)

    def columns(q):
        return pl.ds(pl.multiple_of(q * quarter, quarter), quarter)

    order = [0] + list(range(chunks - 1, 0, -1))
    loads = {}

    def load(name, source, target, index):
        loads[name] = pltpu.make_async_copy(source, target, lsem.at[index])
        loads[name].start()

    load("d", d_hbm, d_ref, 0)
    load("wg", wg_hbm, wg_ref, 1)

    def load_rows(z):
        for m in (2 * z, 2 * z + 1):
            first = pl.multiple_of(paired(me, m) * cap, cap)
            load(("x", m), x_hbm.at[pl.ds(first, cap), :], x_ref.at[block_rows(m), :], 4 + m)

    load_rows(0)
    load("wu", wu_hbm, wu_ref, 2)
    load("wd", wd_hbm, wd_ref, 3)
    for z in order[1:]:
        load_rows(z)
    load("w", w_hbm, w_ref, 4 + n)

    kinds = lax.broadcasted_iota(jnp.int32, (n, tokens), 0)
    named = [(kinds == expert_ref[j : j + 1, :]).astype(jnp.float32) for j in range(2)]
    earlier = lax.broadcasted_iota(jnp.int32, (tokens, tokens), 0) < lax.broadcasted_iota(
        jnp.int32, (tokens, tokens), 1
    )
    before = mm((named[0] + named[1]).astype(jnp.bfloat16), earlier.astype(jnp.bfloat16), NN)
    slots = []
    for j in range(2):
        rank = jnp.sum(before * named[j], axis=0, keepdims=True).astype(jnp.int32)
        slots.append(expert_ref[j : j + 1, :] * cap + rank)
    places = lax.broadcasted_iota(jnp.int32, (cap, tokens), 0)

    def routed_rows(m, chosen):
        first = paired(me, m) * cap
        hits = [(slots[j] - first == places).astype(jnp.float32) for j in range(2)]
        both = (hits[0] + hits[1]).astype(jnp.bfloat16)
        onehot[block_rows(m), :] = both
        weight = jnp.sum(
            hits[0] * weight_ref[0:1, :] + hits[1] * weight_ref[1:2, :], axis=1, keepdims=True
        )
        return (mm(both, chosen, NN) * weight).astype(jnp.bfloat16)

    def route(m):
        if m <= near:
            source = outbox_near.at[block_rows(m - 1), :]
            target = routed.at[block_rows(m), pl.ds(pl.multiple_of(core * half, half), half)]
        else:
            source = outbox.at[block_rows(m - near - 1), :]
            target = routed.at[block_rows(m), columns(col)]
        return pltpu.make_async_remote_copy(
            src_ref=source,
            dst_ref=target,
            send_sem=rs.at[m],
            recv_sem=rr.at[m],
            device_id={"sp": paired(me, m)},
            device_id_type=MESH,
        )

    def pass_on(m, what, target, send_sem, recv_sem):
        if m <= near:
            piece = routed.at[block_rows(m), pl.ds(pl.multiple_of(what * half, half), half)]
        else:
            piece = routed.at[block_rows(m), columns(what)]
        return pltpu.make_async_remote_copy(
            src_ref=piece,
            dst_ref=piece,
            send_sem=send_sem.at[m],
            recv_sem=recv_sem.at[m],
            device_id={"tp": target},
            device_id_type=MESH,
        )

    sent = []
    loads["d"].wait()
    sends = []
    for z in order[1:]:
        sends += [2 * z, 2 * z + 1]
    sends.insert(1, 1)
    greeting = True
    for m in sends:
        if m <= near:
            outbox_near[block_rows(m - 1), :] = routed_rows(
                m, d_ref[:, pl.ds(pl.multiple_of(core * half, half), half)]
            )
        else:
            outbox[block_rows(m - near - 1), :] = routed_rows(m, d_ref[:, columns(col)])
        if greeting:
            pl.semaphore_wait(barrier, greeted)
            greeting = False
        sent.append(route(m))
        sent[-1].start()
    routed[block_rows(0), :] = routed_rows(0, d_ref[...])

    crossed, beside, relayed = {}, {}, {}

    def arrive(m):
        route(m).wait_recv()
        if m <= near:
            beside[m] = pass_on(m, core, partner, ps, pr)
            beside[m].start()
            return
        crossed[m] = pass_on(m, col, far, fs, fr)
        crossed[m].start()
        beside[m] = pass_on(m, col, partner, ps, pr)
        beside[m].start()

    def relay(m):
        if m <= near:
            return
        crossed[m].wait_recv()
        relayed[m] = pass_on(m, far, partner, qs, qr)
        relayed[m].start()

    def complete(m):
        beside[m].wait_recv()
        if m > near:
            relayed[m].wait_recv()

    def gates(z):
        rows = chunk_rows(z)
        held = order.index(z) % 2
        loads[("x", 2 * z)].wait()
        loads[("x", 2 * z + 1)].wait()
        if z == 0:
            loads["wg"].wait()
        gate = mm(x_ref[rows, :], wg_ref[...], NT)
        if z == 0:
            loads["wu"].wait()
        up = mm(x_ref[rows, :], wu_ref[...], NT)
        sigmoid = jax.nn.sigmoid(gate)
        silu = gate * sigmoid
        hidden[rows, :] = (silu * up).astype(jnp.bfloat16)
        active[held] = silu
        slope[held] = up * sigmoid * (1.0 + gate * (1.0 - sigmoid))

    halves = {}

    def experts(z):
        rows = chunk_rows(z)
        if z == 0:
            loads["wd"].wait()
        d_hidden = mm(routed[rows, :], wd_ref[...], NT)
        held = order.index(z) % 2
        d_gate[rows, :] = (d_hidden * slope[held]).astype(jnp.bfloat16)
        d_up[rows, :] = (d_hidden * active[held]).astype(jnp.bfloat16)
        for whose in (1 - core, core):
            for i in range(2):
                across = 1 - side if i == 0 else side
                cut = columns(2 * across + whose)
                term = mm(d_gate[rows, :], wg_ref[:, cut], NN) + mm(
                    d_up[rows, :], wu_ref[:, cut], NN
                )
                part[rows, cut] = term.astype(jnp.bfloat16)
            if (z, 0) in halves:
                continue
            for i in range(2):
                across = 1 - side if i == 0 else side
                halves[(z, i)] = pltpu.make_async_remote_copy(
                    src_ref=part.at[rows, columns(2 * across + 1 - core)],
                    dst_ref=pair_in.at[i, rows, :],
                    send_sem=ds.at[z, i],
                    recv_sem=dr.at[z, i],
                    device_id={"tp": partner},
                    device_id_type=MESH,
                )
                halves[(z, i)].start()

    over = {}

    def reduce_near(z):
        rows = chunk_rows(z)
        halves[(z, 0)].wait_recv()
        far_out[rows, :] = (
            part[rows, columns(far)].astype(jnp.float32)
            + pair_in[0, rows, :].astype(jnp.float32)
        ).astype(jnp.bfloat16)
        over[z] = pltpu.make_async_remote_copy(
            src_ref=far_out.at[rows, :],
            dst_ref=far_in.at[rows, :],
            send_sem=xs.at[z],
            recv_sem=xr.at[z],
            device_id={"tp": far},
            device_id_type=MESH,
        )
        over[z].start()

    returned = {}

    def reduce_far(z):
        rows = chunk_rows(z)
        halves[(z, 1)].wait_recv()
        over[z].wait_recv()
        sums[rows, :] = (
            part[rows, columns(col)].astype(jnp.float32)
            + pair_in[1, rows, :].astype(jnp.float32)
            + far_in[rows, :].astype(jnp.float32)
        ).astype(jnp.bfloat16)
        for m in (2 * z, 2 * z + 1):
            if m == 0:
                back[block_rows(0), :] = sums[block_rows(0), :]
                continue
            returned[m] = pltpu.make_async_remote_copy(
                src_ref=sums.at[block_rows(m), :],
                dst_ref=back.at[block_rows(m), :],
                send_sem=bs.at[m],
                recv_sem=br.at[m],
                device_id={"sp": paired(me, m)},
                device_id_type=MESH,
            )
            returned[m].start()

    def pick(z):
        rows = chunk_rows(z)
        for m in (2 * z, 2 * z + 1):
            if m > 0:
                returned[m].wait_recv()
        found = mm(onehot[rows, :], back[rows, :], TN)
        picked[...] = found if z == 0 else picked[...] + found

    stored = []

    def store(source, target):
        stored.append(pltpu.make_async_copy(source, target, osem.at[len(stored)]))
        stored[-1].start()

    def weight_grad(lhs, rhs, out, target):
        turned[...] = lhs[...].T

        def piece(i, carry):
            cut = columns(i)
            out[:, cut] = mm(turned[...], rhs[:, cut], NN).astype(jnp.bfloat16)
            return carry

        lax.fori_loop(0, 4, piece, 0)
        store(out, target)

    blocks = tokens // BLK
    causal = triangle(True)
    width = v_ref.shape[1]
    scan = (mix_total, mix_reach)
    reach = distances(n)
    rounds = len(reach)

    def scan_from(local, ahead):
        mix_local[...] = local
        mix_ahead[...] = jnp.broadcast_to(jnp.exp(ahead), mix_ahead.shape)
        mix_total[...] = jnp.zeros(mix_total.shape, jnp.float32)
        mix_reach[...] = jnp.ones(mix_reach.shape, jnp.float32)

    def mixer_states():
        local = jnp.zeros(mix_total.shape, jnp.float32)
        ahead = jnp.zeros((1, q_ref.shape[1]), jnp.float32)
        for b in range(blocks):
            rows = pl.ds(b * BLK, BLK)
            cumulative, _, ending = decays(g_ref, rows)
            cum[rows, :] = cumulative
            kept[b] = local
            befores[b : b + 1, :] = jnp.exp(ahead)
            faded = (k_ref[rows, :].astype(jnp.float32) * jnp.exp(ending - cumulative)).astype(
                jnp.bfloat16
            )
            local = local * jnp.exp(ending) + mm(v_ref[rows, :], faded, TN)
            ahead = ahead + ending
        scan_from(local, ahead)

    def mixer_send(step, index):
        at = index if step > 0 else rounds + index
        distance = reach[index]
        prefix_send(
            n, me, step, distance, at, mix_local, mix_ahead, scan, mix_send, mix_recv, ms, mr
        )

    def mixer_take(step, index):
        at = index if step > 0 else rounds + index
        prefix_take(n, me, step, reach[index], at, scan, mix_send, mix_recv, ms, mr)

    def mixer_inner():
        for b in range(blocks):
            rows = pl.ds(b * BLK, BLK)
            cumulative = cum[rows, :]
            middle = cumulative[BLK // 2 - 1 : BLK // 2, :]
            query = q_ref[rows, :].astype(jnp.float32) * scale
            key = k_ref[rows, :].astype(jnp.float32)
            up_q = (query * jnp.exp(cumulative - middle)).astype(jnp.bfloat16)
            up_k = (key * jnp.exp(middle - cumulative)).astype(jnp.bfloat16)
            scores = jnp.where(causal, mm(up_q, up_k, NT), 0.0).astype(jnp.bfloat16)
            lifted_q[rows, :] = up_q
            lifted_k[rows, :] = up_k
            scores_ref[rows, :] = scores
            inner[rows, :] = mm(scores, v_ref[rows, :], NN)
            scaled[rows, :] = (query * jnp.exp(cumulative)).astype(jnp.bfloat16)

    def mixer_finish():
        for b in range(blocks):
            rows = pl.ds(b * BLK, BLK)
            state = (kept[b] + mix_total[...] * befores[b : b + 1, :]).astype(jnp.bfloat16)
            states_ref[b] = state
            mixed_ref[rows, :] = (inner[rows, :] + mm(scaled[rows, :], state, NT)).astype(
                jnp.bfloat16
            )

    taken = [0]

    def mixer_round(step):
        if taken[0] < rounds:
            mixer_take(step, taken[0])
            taken[0] += 1
            if taken[0] < rounds:
                mixer_send(step, taken[0])

    share, turns = proj_out.shape[3], proj_out.shape[1]
    parity = lax.rem(me, 2)
    at_z = me // 2
    paired_off, handed = {}, []

    def project(j):
        q = paired(col, j)
        rows = pl.ds(pl.multiple_of(q * quarter, quarter), quarter)
        grads = gathered[j]
        term = mm(grads, w_ref[rows, :], NN)
        picked[:, :width] = term if j == 0 else picked[:, :width] + term
        product = mm(grads, mixed_ref[...], TN).astype(jnp.bfloat16)
        for i in range(turns):
            for y in range(2):
                at = 2 * i + y
                proj_out[j, i, y] = product[at * share : (at + 1) * share, :]

    def pair_up(j):
        for i in range(turns):
            paired_off[(j, i)] = pltpu.make_async_remote_copy(
                src_ref=proj_out.at[j, i, 1 - parity],
                dst_ref=proj_pair.at[j, i],
                send_sem=ys.at[j, i],
                recv_sem=yr.at[j, i],
                device_id={"sp": me + 1 - 2 * parity},
                device_id_type=MESH,
            )
            paired_off[(j, i)].start()

    def hand_over(j):
        q = paired(col, j)
        for i in range(turns):
            paired_off[(j, i)].wait_recv()
            both_rows = proj_out[j, i, parity].astype(jnp.float32) + proj_pair[j, i].astype(
                jnp.float32
            )
            proj_out[j, i, parity] = both_rows.astype(jnp.bfloat16)
            owner = q * turns + i
            away = jnp.int32(0)
            bit = 1
            while bit < chunks:
                away = away + bit * lax.rem(at_z // bit + owner // bit, 2)
                bit *= 2
            copy = pltpu.make_async_remote_copy(
                src_ref=proj_out.at[j, i, parity],
                dst_ref=proj_in.at[away],
                send_sem=zs.at[j, i],
                recv_sem=zr.at[away],
                device_id={"sp": 2 * owner + parity},
                device_id_type=MESH,
            )
            handed.append((away, copy))

            @pl.when(away == 0)
            def _():
                proj_mine[...] = proj_out[j, i, parity].astype(jnp.float32)

            @pl.when(away != 0)
            def _():
                copy.start()

    def project_sum():
        total = proj_mine[...]
        for z in range(1, chunks):
            pltpu.make_async_remote_copy(
                src_ref=proj_out.at[0, 0, parity],
                dst_ref=proj_in.at[z],
                send_sem=zs.at[0, 0],
                recv_sem=zr.at[z],
                device_id={"sp": paired(me, 2 * z)},
                device_id_type=MESH,
            ).wait_recv()
            total = total + proj_in[z].astype(jnp.float32)
        proj_ref[...] = total

    def back_states():
        d_round[...] = picked[:, :width].astype(jnp.bfloat16)
        local = jnp.zeros(mix_total.shape, jnp.float32)
        after = jnp.zeros((1, q_ref.shape[1]), jnp.float32)
        for b in reversed(range(blocks)):
            rows = pl.ds(b * BLK, BLK)
            ending = cum[b * BLK + BLK - 1 : b * BLK + BLK, :]
            kept[b] = local
            befores[b : b + 1, :] = jnp.exp(after)
            local = local * jnp.exp(ending) + mm(d_round[rows, :], scaled[rows, :], TN)
            after = after + ending
        scan_from(local, after)

    def back_inner():
        for b in range(blocks):
            rows = pl.ds(b * BLK, BLK)
            cumulative = cum[rows, :]
            middle = cumulative[BLK // 2 - 1 : BLK // 2, :]
            query = q_ref[rows, :].astype(jnp.float32) * scale
            d_out = d_round[rows, :]
            up_q, up_k = lifted_q[rows, :], lifted_k[rows, :]
            d_scores = jnp.where(causal, mm(d_out, v_ref[rows, :], NT), 0.0).astype(jnp.bfloat16)
            d_up_q = mm(d_scores, up_k, NN)
            d_up_k = mm(d_scores, up_q, TN)
            d_carried = mm(d_out, states_ref[b], NN) * jnp.exp(cumulative)
            gq_ref[rows, :] = (
                (d_up_q * jnp.exp(cumulative - middle) + d_carried) * scale
            ).astype(jnp.bfloat16)
            gg_ref[rows, :] = (
                up_q.astype(jnp.float32) * d_up_q
                - up_k.astype(jnp.float32) * d_up_k
                + query * d_carried
            )
            key_part[rows, :] = d_up_k * jnp.exp(middle - cumulative)
            inner[rows, :] = mm(scores_ref[rows, :], d_out, TN)

    def back_finish():
        for b in range(blocks):
            rows = pl.ds(b * BLK, BLK)
            cumulative = cum[rows, :]
            ending = cumulative[BLK - 1 : BLK, :]
            d_state = kept[b] + mix_total[...] * befores[b : b + 1, :]
            d_rounded = d_state.astype(jnp.bfloat16)
            fade = jnp.exp(ending - cumulative)
            faded = k_ref[rows, :].astype(jnp.float32) * fade
            d_faded = mm(v_ref[rows, :], d_rounded, NN)
            gk_ref[rows, :] = (key_part[rows, :] + d_faded * fade).astype(jnp.bfloat16)
            gv_ref[rows, :] = (
                inner[rows, :] + mm(faded.astype(jnp.bfloat16), d_rounded, NT)
            ).astype(jnp.bfloat16)
            moved = faded * d_faded
            at_end = jnp.sum(moved, axis=0, keepdims=True) + jnp.exp(ending) * jnp.sum(
                states_ref[b].astype(jnp.float32) * d_state, axis=0, keepdims=True
            )
            gg_ref[rows, :] = block_sums(triangle(False), gg_ref[rows, :] - moved) + at_end

    def both(step, z):
        step(2 * z)
        step(2 * z + 1)

    early = order[1:]
    gates(0)
    mixer_states()
    mixer_send(1, 0)
    arrive(1)
    gates(early[0])
    complete(1)
    experts(0)
    both(arrive, early[0])
    reduce_near(0)
    for i, z in enumerate(early):
        following = early[i + 1] if i + 1 < len(early) else None
        if i == 0:
            mixer_inner()
        if following is not None:
            gates(following)
        both(relay, z)
        both(complete, z)
        experts(z)
        if following is not None:
            both(arrive, following)
        reduce_near(z)
        if following is not None:
            mixer_round(1)
        reduce_far(order[i])
    pick(0)
    reduce_far(order[-1])
    while taken[0] < rounds:
        mixer_round(1)
    mixer_finish()
    weight_grad(hidden, routed, wd_ref, grad_down)
    for z in early:
        pick(z)
    own = d_ref[:, columns(col)].astype(jnp.float32)
    gathered[0] = (own + picked[...]).astype(jnp.bfloat16)

    def give(block, slot, target):
        return pltpu.make_async_remote_copy(
            src_ref=gathered.at[block],
            dst_ref=gathered.at[slot],
            send_sem=gs.at[slot],
            recv_sem=gr.at[slot],
            device_id={"tp": target},
            device_id_type=MESH,
        )

    given = [give(0, 1, partner), give(0, 2, far), give(2, 3, partner)]
    given[1].start()
    given[0].start()
    loads["w"].wait()
    project(0)
    pair_up(0)
    given[0].wait_recv()
    project(1)
    pair_up(1)
    weight_grad(d_gate, x_ref, wg_ref, grad_gate)
    hand_over(0)
    hand_over(1)
    weight_grad(d_up, x_ref, wu_ref, grad_up)
    given[1].wait_recv()
    given[2].start()
    project(2)
    pair_up(2)
    given[2].wait_recv()
    project(3)
    back_states()
    taken[0] = 0
    mixer_send(-1, 0)
    pair_up(3)
    back_inner()
    mixer_round(-1)
    mixer_round(-1)
    hand_over(2)
    hand_over(3)
    mixer_round(-1)
    store(gq_ref, grad_q)
    back_finish()
    store(gk_ref, grad_k)
    store(gv_ref, grad_v)
    store(gg_ref, grad_g)
    project_sum()
    store(proj_ref, grad_proj)
    for copy in stored:
        copy.wait()
    for copy in sent + given:
        copy.wait_send()
    for group in (crossed, beside, relayed, halves, over, returned, paired_off):
        for copy in group.values():
            copy.wait_send()
    for away, copy in handed:

        @pl.when(away != 0)
        def _():
            copy.wait_send()


def expert_stage(
    d_out, route_expert, route_weight, rows_in, gate_t, up_t, down, q, k, v, g, w_out, cap, scale
):
    n = lax.axis_size("sp")
    tokens, model = d_out.shape
    quarter = model // 4
    units = down.shape[0]
    slots = n * cap
    channels, width = q.shape[1], v.shape[1]
    blocks = tokens // BLK
    rounds = len(distances(n))
    share = model // n
    turns = n // 8
    bf16, f32 = jnp.bfloat16, jnp.float32
    weight_shape = jax.ShapeDtypeStruct((units, model), bf16)
    out_shape = (
        weight_shape,
        weight_shape,
        weight_shape,
        jax.ShapeDtypeStruct((share, width), f32),
        jax.ShapeDtypeStruct((tokens, channels), bf16),
        jax.ShapeDtypeStruct((tokens, channels), bf16),
        jax.ShapeDtypeStruct((tokens, width), bf16),
        jax.ShapeDtypeStruct((tokens, channels), f32),
    )
    anywhere = pl.BlockSpec(memory_space=pl.ANY)
    local = pl.BlockSpec(memory_space=pltpu.VMEM)
    dma = pltpu.SemaphoreType.DMA
    return pl.pallas_call(
        functools.partial(expert_kernel, n, cap, scale),
        out_shape=out_shape,
        in_specs=[anywhere, local, local] + [anywhere] * 4 + [local] * 4 + [anywhere],
        out_specs=(anywhere,) * 8,
        scratch_shapes=[pltpu.VMEM(a.shape, a.dtype) for a in out_shape]
        + [
            pltpu.VMEM((4, tokens, quarter), bf16),
            pltpu.VMEM((tokens, width), bf16),
            pltpu.VMEM((blocks, width, channels), bf16),
            pltpu.VMEM((tokens, model), bf16),
            pltpu.VMEM((slots, model), bf16),
            pltpu.VMEM((slots, model), bf16),
            pltpu.VMEM((slots, tokens), bf16),
            pltpu.VMEM((slots - 4 * cap, quarter), bf16),
            pltpu.VMEM((3 * cap, model // 2), bf16),
            pltpu.VMEM((2, 2 * cap, units), f32),
            pltpu.VMEM((2, 2 * cap, units), f32),
            pltpu.VMEM((slots, units), bf16),
            pltpu.VMEM((slots, units), bf16),
            pltpu.VMEM((slots, units), bf16),
            pltpu.VMEM((slots, model), bf16),
            pltpu.VMEM((2, slots, quarter), bf16),
            pltpu.VMEM((slots, quarter), bf16),
            pltpu.VMEM((slots, quarter), bf16),
            pltpu.VMEM((slots, quarter), bf16),
            pltpu.VMEM((slots, quarter), bf16),
            pltpu.VMEM((tokens, quarter), f32),
            pltpu.VMEM((units, slots), bf16),
            pltpu.VMEM((tokens, channels), f32),
            pltpu.VMEM((blocks, width, channels), f32),
            pltpu.VMEM((blocks, channels), f32),
            pltpu.VMEM((tokens, width), f32),
            pltpu.VMEM((tokens, channels), bf16),
            pltpu.VMEM((tokens, channels), bf16),
            pltpu.VMEM((tokens, channels), bf16),
            pltpu.VMEM((tokens, BLK), bf16),
            pltpu.VMEM((tokens, width), bf16),
            pltpu.VMEM((tokens, channels), f32),
            pltpu.VMEM((4, turns, 2, share, width), bf16),
            pltpu.VMEM((4, turns, share, width), bf16),
            pltpu.VMEM((share, width), f32),
            pltpu.VMEM((n // 2, share, width), bf16),
            pltpu.VMEM((model, width), bf16),
            pltpu.VMEM((width, channels), f32),
            pltpu.VMEM((8, channels), f32),
            pltpu.VMEM((width, channels), f32),
            pltpu.VMEM((8, channels), f32),
            pltpu.VMEM((2 * rounds, width + 16, channels), bf16),
            pltpu.VMEM((2 * rounds, width + 16, channels), bf16),
            dma((5 + n,)),
            dma((8,)),
            dma((n,)),
            dma((n,)),
            dma((n,)),
            dma((n,)),
            dma((n,)),
            dma((n,)),
            dma((n,)),
            dma((n,)),
            dma((n // 2, 2)),
            dma((n // 2, 2)),
            dma((n // 2,)),
            dma((n // 2,)),
            dma((n,)),
            dma((n,)),
            dma((2 * rounds,)),
            dma((2 * rounds,)),
            dma((4,)),
            dma((4,)),
            dma((4, turns)),
            dma((4, turns)),
            dma((4, turns)),
            dma((n // 2,)),
        ],
        compiler_params=pltpu.CompilerParams(
            collective_id=5, has_side_effects=True, vmem_limit_bytes=60 * 1024 * 1024
        ),
        cost_estimate=pl.CostEstimate(
            flops=60_000_000_000, bytes_accessed=30_000_000, transcendentals=0
        ),
        name="expert_stage",
    )(d_out, route_expert.T, route_weight.T, rows_in, gate_t, up_t, down, q, k, v, g, w_out)


def store_kernel(pieces, count, *refs):
    sources, targets, held = refs[:count], refs[count : 2 * count], refs[2 * count : 3 * count]
    isem, osem = refs[3 * count :]
    cuts = []
    for i in range(count):
        parts = pieces if i < 3 else 1
        rows = sources[i].shape[0] // parts
        cuts += [(i, pl.ds(p * rows, rows)) for p in range(parts)]
    reads = [
        pltpu.make_async_copy(sources[i].at[cut, :], held[i].at[cut, :], isem.at[at])
        for at, (i, cut) in enumerate(cuts)
    ]
    writes = [
        pltpu.make_async_copy(held[i].at[cut, :], targets[i].at[cut, :], osem.at[at])
        for at, (i, cut) in enumerate(cuts)
    ]
    for read in reads:
        read.start()
    for read, write in zip(reads, writes):
        read.wait()
        write.start()
    for write in writes:
        write.wait()


def store_out(arrays):
    count = len(arrays)
    pieces = 4 if arrays[0].shape[0] % 64 == 0 else 1
    total = 3 * pieces + count - 3
    anywhere = pl.BlockSpec(memory_space=pl.ANY)
    return pl.pallas_call(
        functools.partial(store_kernel, pieces, count),
        out_shape=tuple(jax.ShapeDtypeStruct(a.shape, a.dtype) for a in arrays),
        in_specs=[anywhere] * count,
        out_specs=(anywhere,) * count,
        scratch_shapes=[pltpu.VMEM(a.shape, a.dtype) for a in arrays]
        + [pltpu.SemaphoreType.DMA((total,)), pltpu.SemaphoreType.DMA((total,))],
        compiler_params=pltpu.CompilerParams(vmem_limit_bytes=60 * 1024 * 1024),
        name="store_out",
    )(*arrays)


def fused_local(
    d_out,
    route_expert,
    route_weight,
    expert_inputs,
    w_gate,
    w_up,
    w_down,
    w_out,
    queries,
    keys,
    values,
    log_decay,
):
    experts = lax.axis_size("sp")
    capacity = expert_inputs.shape[1] // experts
    scale_q = queries.shape[2] ** (-0.5)
    q, k, v, g = queries[:, 0], keys[:, 0], values[:, 0], log_decay[:, 0]
    results = expert_stage(
        d_out,
        route_expert,
        route_weight,
        expert_inputs[0],
        w_gate[0].T,
        w_up[0].T,
        w_down[0],
        q,
        k,
        v,
        g,
        w_out,
        capacity,
        scale_q,
    )
    grad_gate, grad_up, grad_down, grad_proj, grad_q, grad_k, grad_v, grad_g = store_out(results)
    return (
        grad_gate.T[None],
        grad_up.T[None],
        grad_down[None],
        grad_proj,
        grad_q[:, None],
        grad_k[:, None],
        grad_v[:, None],
        grad_g[:, None],
    )


def choose(*arrays):
    n, tp = lax.axis_size("sp"), lax.axis_size("tp")
    tokens, model = arrays[0].shape
    capacity = arrays[3].shape[1] // n
    power = n & (n - 1) == 0 and n % 8 == 0
    if tp == 4 and power and capacity % 16 == 0 and n * capacity <= 1536 and model % 512 == 0:
        return fused_local(*arrays)
    return local(*arrays)


def solution(mesh):
    return jax.shard_map(
        choose,
        mesh=mesh,
        in_specs=(
            P("sp", None),
            P("sp", None),
            P("sp", None),
            P("sp", None, None),
            P("sp", None, "tp"),
            P("sp", None, "tp"),
            P("sp", "tp", None),
            P(None, "tp"),
            P("sp", "tp", None),
            P("sp", "tp", None),
            P("sp", "tp", None),
            P("sp", "tp", None),
        ),
        out_specs=(
            P("sp", None, "tp"),
            P("sp", None, "tp"),
            P("sp", "tp", None),
            P("sp", "tp"),
            P("sp", "tp", None),
            P("sp", "tp", None),
            P("sp", "tp", None),
            P("sp", "tp", None),
        ),
        check_vma=False,
    )
```

```python
import functools

import jax
import jax.numpy as jnp
from jax import lax
from jax.experimental import pallas as pl
from jax.experimental.pallas import tpu as pltpu
from jax.sharding import PartitionSpec as P

BLK = 64


precise = lax.Precision.HIGHEST


MESH = pl.DeviceIdType.MESH
NN = (((1,), (0,)), ((), ()))
NT = (((1,), (1,)), ((), ()))
TN = (((0,), (0,)), ((), ()))


def mm(a, b, dims):
    return lax.dot_general(a, b, dims, preferred_element_type=jnp.float32)


def triangle(lower):
    rows = lax.broadcasted_iota(jnp.int32, (BLK, BLK), 0)
    cols = lax.broadcasted_iota(jnp.int32, (BLK, BLK), 1)
    return rows >= cols if lower else rows <= cols


def block_sums(mask, x):
    return lax.dot_general(
        mask.astype(jnp.float32), x, NN, precision=precise, preferred_element_type=jnp.float32
    )


def decays(g_ref, rows):
    cumulative = block_sums(triangle(True), g_ref[rows, :])
    middle = cumulative[BLK // 2 - 1 : BLK // 2, :]
    ending = cumulative[BLK - 1 : BLK, :]
    return cumulative, middle, ending


def greet(n, me, tp=None):
    barrier = pltpu.get_barrier_semaphore()
    others = [{"sp": lax.rem(me + k, n)} for k in range(1, n)]
    if tp is not None:
        others += [{"tp": other} for other in tp]
    for other in others:
        pl.semaphore_signal(barrier, inc=1, device_id=other, device_id_type=MESH)
    return barrier, len(others)


def route_kernel(
    n,
    tp,
    cap,
    d_ref,
    expert_ref,
    weight_ref,
    routed_ref,
    slot_ref,
    outbox,
    ssem,
    rsem,
    lsem,
    tsend,
    trecv,
):
    me = lax.axis_index("sp")
    col = lax.axis_index("tp")
    partner = col + 1 - 2 * lax.rem(col, 2)
    far = [lax.rem(col + 2 * s, tp) for s in range(1, tp // 2)]
    barrier, greeted = greet(n, me, [partner] + far)
    tokens = d_ref.shape[0]
    quarter = outbox.shape[2]
    start = pl.multiple_of(lax.axis_index("tp") * quarter, quarter)
    own = d_ref[:, pl.ds(start, quarter)].astype(jnp.float32)
    kinds = lax.broadcasted_iota(jnp.int32, (n, tokens), 0)
    named = [(kinds == expert_ref[j : j + 1, :]).astype(jnp.float32) for j in range(2)]
    earlier = lax.broadcasted_iota(jnp.int32, (tokens, tokens), 0) < lax.broadcasted_iota(
        jnp.int32, (tokens, tokens), 1
    )
    before = mm((named[0] + named[1]).astype(jnp.bfloat16), earlier.astype(jnp.bfloat16), NN)
    scaled = []
    slots = []
    for j in range(2):
        rank = jnp.sum(before * named[j], axis=0, keepdims=True).astype(jnp.int32)
        slots.append(expert_ref[j : j + 1, :] * cap + rank)
        slot_ref[j : j + 1, :] = slots[j]
        scaled.append((own * weight_ref[:, j : j + 1]).astype(jnp.bfloat16))
    places = lax.broadcasted_iota(jnp.int32, (cap, tokens), 0)
    for e in range(n):
        rows = jnp.zeros((cap, quarter), jnp.float32)
        for j in range(2):
            picks = (slots[j] - e * cap == places).astype(jnp.float32).astype(jnp.bfloat16)
            rows = rows + mm(picks, scaled[j], NN)
        outbox[e] = rows.astype(jnp.bfloat16)
    pl.semaphore_wait(barrier, greeted)

    def place(row, column):
        return routed_ref.at[row, :, pl.ds(pl.multiple_of(column * quarter, quarter), quarter)]

    copies = []
    for k in range(1, n):
        peer = lax.rem(me + k, n)
        copies.append(
            pltpu.make_async_remote_copy(
                src_ref=outbox.at[peer],
                dst_ref=place(me, col),
                send_sem=ssem.at[k - 1],
                recv_sem=rsem.at[k - 1],
                device_id={"sp": peer},
                device_id_type=MESH,
            )
        )
        copies[-1].start()
    stays = pltpu.make_async_copy(outbox.at[me], place(me, col), lsem)
    stays.start()

    def send(k, column, slot, target):
        row = lax.rem(me - k + n, n)
        return pltpu.make_async_remote_copy(
            src_ref=place(row, column),
            dst_ref=place(row, column),
            send_sem=tsend.at[k, slot],
            recv_sem=trecv.at[k, slot],
            device_id={"tp": target},
            device_id_type=MESH,
        )

    across, beside, passed = [], [], []

    def pass_on(k):
        for s in range(len(far)):
            across[k][s].wait_recv()
            column = lax.rem(col - 2 * (s + 1) + tp, tp)
            passed.append(send(k, column, tp // 2 + s, partner))
            passed[-1].start()

    for k in range(n):
        if k == 0:
            stays.wait()
        else:
            copies[k - 1].wait_recv()
        across.append([send(k, col, s + 1, far[s]) for s in range(len(far))])
        for copy in across[k]:
            copy.start()
        beside.append(send(k, col, 0, partner))
        beside[k].start()
        if k > 1:
            pass_on(k - 2)
    for k in range(max(n - 2, 0), n):
        pass_on(k)
    for copy in copies:
        copy.wait_send()
    for row in across:
        for copy in row:
            copy.wait_send()
    for copy in beside + passed:
        copy.wait()


def exchange(n, me, source, target, ssem, rsem, lsem):
    copies = []
    for k in range(1, n):
        peer = lax.rem(me + k, n)
        copies.append(
            pltpu.make_async_remote_copy(
                src_ref=source.at[peer],
                dst_ref=target.at[me],
                send_sem=ssem.at[k - 1],
                recv_sem=rsem.at[k - 1],
                device_id={"sp": peer},
                device_id_type=MESH,
            )
        )
    for copy in copies:
        copy.start()
    stays = pltpu.make_async_copy(source.at[me], target.at[me], lsem)
    stays.start()
    stays.wait()
    for copy in copies:
        copy.wait()


def return_kernel(
    n, tp, cap, sums_ref, slot_ref, d_ref, gathered_ref, back, ssem, rsem, lsem, tsend, trecv
):
    me = lax.axis_index("sp")
    col = lax.axis_index("tp")
    partner = col + 1 - 2 * lax.rem(col, 2)
    far = [lax.rem(col + 2 * s, tp) for s in range(1, tp // 2)]
    barrier, greeted = greet(n, me, [partner] + far)
    pl.semaphore_wait(barrier, greeted)
    exchange(n, me, sums_ref, back, ssem, rsem, lsem)
    tokens = d_ref.shape[0]
    quarter = back.shape[2]
    start = pl.multiple_of(col * quarter, quarter)
    places = lax.broadcasted_iota(jnp.int32, (cap, tokens), 0)
    picked = jnp.zeros((tokens, quarter), jnp.float32)
    for e in range(n):
        here = jnp.zeros((cap, tokens), jnp.float32)
        for j in range(2):
            here = here + (slot_ref[j : j + 1, :] - e * cap == places).astype(jnp.float32)
        picked = picked + mm(here.astype(jnp.bfloat16), back[e], TN)
    own = d_ref[:, pl.ds(start, quarter)].astype(jnp.float32)
    gathered_ref[col] = (own + picked).astype(jnp.bfloat16)

    def send(block, slot, target):
        return pltpu.make_async_remote_copy(
            src_ref=gathered_ref.at[block],
            dst_ref=gathered_ref.at[block],
            send_sem=tsend.at[slot],
            recv_sem=trecv.at[slot],
            device_id={"tp": target},
            device_id_type=MESH,
        )

    across = [send(col, s + 1, far[s]) for s in range(len(far))]
    beside = send(col, 0, partner)
    for copy in across:
        copy.start()
    beside.start()
    passed = []
    for s in range(len(far)):
        across[s].wait_recv()
        block = lax.rem(col - 2 * (s + 1) + tp, tp)
        passed.append(send(block, tp // 2 + s, partner))
        passed[s].start()
    for copy in across:
        copy.wait_send()
    beside.wait()
    for copy in passed:
        copy.wait()


def state_copies(n, me, step, send_ref, recv_ref, send_sem, recv_sem):
    return [
        pltpu.make_async_remote_copy(
            src_ref=send_ref,
            dst_ref=recv_ref.at[k - 1],
            send_sem=send_sem.at[k - 1],
            recv_sem=recv_sem.at[k - 1],
            device_id={"sp": lax.rem(me + step * k + n, n)},
            device_id_type=MESH,
        )
        for k in range(1, n)
    ]


def collect(n, me, step, copies, recv_ref, total, width):
    total[...] = jnp.zeros_like(total)
    for k in range(n - 1, 0, -1):
        copies[k - 1].wait()
        source = me - step * k
        reached = jnp.logical_and(source >= 0, source < n)

        @pl.when(reached)
        def _():
            factor = recv_ref[k - 1, width : width + 1, :].astype(jnp.float32)
            total[...] = total[...] * factor + recv_ref[k - 1, :width, :].astype(jnp.float32)


def forward_kernel(
    n, scale, q_ref, k_ref, v_ref, g_ref, mixed_ref, states_ref, kept, total, send, recv, ssem, rsem
):
    me = lax.axis_index("sp")
    barrier, greeted = greet(n, me)
    length, width = v_ref.shape
    blocks = length // BLK
    causal = triangle(True)
    local = jnp.zeros(total.shape, jnp.float32)
    ahead = jnp.zeros((1, q_ref.shape[1]), jnp.float32)
    befores = []
    for b in range(blocks):
        rows = pl.ds(b * BLK, BLK)
        cumulative, _, ending = decays(g_ref, rows)
        kept[b] = local
        befores.append(ahead)
        faded = (k_ref[rows, :].astype(jnp.float32) * jnp.exp(ending - cumulative)).astype(
            jnp.bfloat16
        )
        local = local * jnp.exp(ending) + mm(v_ref[rows, :], faded, TN)
        ahead = ahead + ending
    send[:width, :] = local.astype(jnp.bfloat16)
    send[width:, :] = jnp.broadcast_to(jnp.exp(ahead), (16, ahead.shape[1])).astype(jnp.bfloat16)
    pl.semaphore_wait(barrier, greeted)
    copies = state_copies(n, me, 1, send, recv, ssem, rsem)
    for copy in copies:
        copy.start()
    inner = []
    scaled = []
    for b in range(blocks):
        rows = pl.ds(b * BLK, BLK)
        cumulative, middle, _ = decays(g_ref, rows)
        query = q_ref[rows, :].astype(jnp.float32) * scale
        key = k_ref[rows, :].astype(jnp.float32)
        lifted_q = (query * jnp.exp(cumulative - middle)).astype(jnp.bfloat16)
        lifted_k = (key * jnp.exp(middle - cumulative)).astype(jnp.bfloat16)
        scores = jnp.where(causal, mm(lifted_q, lifted_k, NT), 0.0).astype(jnp.bfloat16)
        inner.append(mm(scores, v_ref[rows, :], NN))
        scaled.append((query * jnp.exp(cumulative)).astype(jnp.bfloat16))
    collect(n, me, 1, copies, recv, total, width)
    for b in range(blocks):
        rows = pl.ds(b * BLK, BLK)
        state = (kept[b] + total[...] * jnp.exp(befores[b])).astype(jnp.bfloat16)
        states_ref[b] = state
        mixed_ref[rows, :] = (inner[b] + mm(scaled[b], state, NT)).astype(jnp.bfloat16)


def backward_kernel(
    n,
    scale,
    q_ref,
    k_ref,
    v_ref,
    g_ref,
    grad_ref,
    w_ref,
    mixed_ref,
    states_ref,
    gq_ref,
    gk_ref,
    gv_ref,
    gg_ref,
    proj_ref,
    kept,
    total,
    send,
    recv,
    ssem,
    rsem,
    d_ref,
    part,
    pair_in,
    pair,
    parts_in,
    psend,
    precv,
):
    me = lax.axis_index("sp")
    barrier, greeted = greet(n, me)
    length, width = v_ref.shape
    blocks = length // BLK
    causal = triangle(True)
    local = jnp.zeros(total.shape, jnp.float32)
    pieces, _, quarter = grad_ref.shape
    d_mixed = jnp.zeros((length, width), jnp.float32)
    for p in range(pieces):
        d_mixed = d_mixed + mm(grad_ref[p], w_ref[p * quarter : (p + 1) * quarter, :], NN)
    d_ref[...] = d_mixed.astype(jnp.bfloat16)
    after = jnp.zeros((1, q_ref.shape[1]), jnp.float32)
    afters = [None] * blocks
    for b in reversed(range(blocks)):
        rows = pl.ds(b * BLK, BLK)
        cumulative, _, ending = decays(g_ref, rows)
        kept[b] = local
        afters[b] = after
        query = q_ref[rows, :].astype(jnp.float32) * scale
        scaled = (query * jnp.exp(cumulative)).astype(jnp.bfloat16)
        local = local * jnp.exp(ending) + mm(d_ref[rows, :], scaled, TN)
        after = after + ending
    send[:width, :] = local.astype(jnp.bfloat16)
    send[width:, :] = jnp.broadcast_to(jnp.exp(after), (16, after.shape[1])).astype(jnp.bfloat16)
    pl.semaphore_wait(barrier, greeted)
    copies = state_copies(n, me, -1, send, recv, ssem, rsem)
    for copy in copies:
        copy.start()
    half, share = part.shape[1:3]
    per = quarter // share
    for p in range(pieces):
        product = mm(grad_ref[p], mixed_ref[...], TN).astype(jnp.bfloat16)
        for i in range(per):
            at = p * per + i
            part[at % 2, at // 2] = product[i * share : (i + 1) * share, :]
    parity = lax.rem(me, 2)
    mine = me // 2
    pairing = pltpu.make_async_remote_copy(
        src_ref=part.at[1 - parity],
        dst_ref=pair_in,
        send_sem=psend.at[0],
        recv_sem=precv.at[0],
        device_id={"sp": me + 1 - 2 * parity},
        device_id_type=MESH,
    )
    pairing.start()
    change = []
    key_part = []
    for b in range(blocks):
        rows = pl.ds(b * BLK, BLK)
        cumulative, middle, _ = decays(g_ref, rows)
        query = q_ref[rows, :].astype(jnp.float32) * scale
        key = k_ref[rows, :].astype(jnp.float32)
        value = v_ref[rows, :]
        d_out = d_ref[rows, :]
        rise, fall = jnp.exp(cumulative - middle), jnp.exp(middle - cumulative)
        lifted_q = (query * rise).astype(jnp.bfloat16)
        lifted_k = (key * fall).astype(jnp.bfloat16)
        scores = jnp.where(causal, mm(lifted_q, lifted_k, NT), 0.0).astype(jnp.bfloat16)
        d_scores = jnp.where(causal, mm(d_out, value, NT), 0.0).astype(jnp.bfloat16)
        d_lifted_q = mm(d_scores, lifted_k, NN)
        d_lifted_k = mm(d_scores, lifted_q, TN)
        grown = jnp.exp(cumulative)
        d_carried = mm(d_out, states_ref[b], NN) * grown
        gq_ref[rows, :] = ((d_lifted_q * rise + d_carried) * scale).astype(jnp.bfloat16)
        change.append(
            lifted_q.astype(jnp.float32) * d_lifted_q
            - lifted_k.astype(jnp.float32) * d_lifted_k
            + query * d_carried
        )
        key_part.append(d_lifted_k * fall)
        gg_ref[rows, :] = change[b]
        gv_ref[rows, :] = mm(scores, d_out, TN).astype(gv_ref.dtype)
    pairing.wait()
    for i in range(half):
        pair[i] = (part[parity, i].astype(jnp.float32) + pair_in[i].astype(jnp.float32)).astype(
            jnp.bfloat16
        )
    collect(n, me, -1, copies, recv, total, width)
    shares = []
    for s in range(1, half):
        other = lax.rem(mine + s, half)
        shares.append(
            pltpu.make_async_remote_copy(
                src_ref=pair.at[other],
                dst_ref=parts_in.at[s - 1],
                send_sem=psend.at[s],
                recv_sem=precv.at[s],
                device_id={"sp": 2 * other + parity},
                device_id_type=MESH,
            )
        )
        shares[-1].start()
    for b in range(blocks):
        rows = pl.ds(b * BLK, BLK)
        cumulative, _, ending = decays(g_ref, rows)
        d_state = kept[b] + total[...] * jnp.exp(afters[b])
        d_rounded = d_state.astype(jnp.bfloat16)
        key = k_ref[rows, :].astype(jnp.float32)
        fade = jnp.exp(ending - cumulative)
        faded = key * fade
        d_faded = mm(v_ref[rows, :], d_rounded, NN)
        gk_ref[rows, :] = (key_part[b] + d_faded * fade).astype(jnp.bfloat16)
        gv_ref[rows, :] = gv_ref[rows, :] + mm(faded.astype(jnp.bfloat16), d_rounded, NT)
        moved = faded * d_faded
        at_end = jnp.sum(moved, axis=0, keepdims=True) + jnp.exp(ending) * jnp.sum(
            states_ref[b].astype(jnp.float32) * d_state, axis=0, keepdims=True
        )
        gg_ref[rows, :] = block_sums(triangle(False), gg_ref[rows, :] - moved) + at_end
    summed = pair[mine].astype(jnp.float32)
    for s in range(1, half):
        shares[s - 1].wait()
        summed = summed + parts_in[s - 1].astype(jnp.float32)
    proj_ref[...] = summed


def exchange_scratch(n, blocks, width, channels):
    return [
        pltpu.VMEM((blocks, width, channels), jnp.float32),
        pltpu.VMEM((width, channels), jnp.float32),
        pltpu.VMEM((width + 16, channels), jnp.bfloat16),
        pltpu.VMEM((n - 1, width + 16, channels), jnp.bfloat16),
        pltpu.SemaphoreType.DMA((n - 1,)),
        pltpu.SemaphoreType.DMA((n - 1,)),
    ]


def in_vmem(count):
    return [pl.BlockSpec(memory_space=pltpu.VMEM)] * count


def mixer_forward(q, k, v, g, scale):
    n = lax.axis_size("sp")
    length, channels = q.shape
    width = v.shape[1]
    blocks = length // BLK
    return pl.pallas_call(
        functools.partial(forward_kernel, n, scale),
        out_shape=(
            jax.ShapeDtypeStruct((length, width), jnp.bfloat16),
            jax.ShapeDtypeStruct((blocks, width, channels), jnp.bfloat16),
        ),
        in_specs=in_vmem(4),
        out_specs=tuple(in_vmem(2)),
        scratch_shapes=exchange_scratch(n, blocks, width, channels),
        compiler_params=pltpu.CompilerParams(
            collective_id=1, has_side_effects=True, vmem_limit_bytes=16 * 1024 * 1024
        ),
        cost_estimate=pl.CostEstimate(
            flops=4_000_000_000, bytes_accessed=4 * length * width, transcendentals=0
        ),
        name="mixer_forward",
    )(q, k, v, g)


def mixer_backward(q, k, v, g, gathered, w_out, mixed, states, scale):
    n = lax.axis_size("sp")
    length, channels = q.shape
    width = v.shape[1]
    blocks = length // BLK
    share = w_out.shape[0] // n
    return pl.pallas_call(
        functools.partial(backward_kernel, n, scale),
        out_shape=(
            jax.ShapeDtypeStruct((length, channels), jnp.bfloat16),
            jax.ShapeDtypeStruct((length, channels), jnp.bfloat16),
            jax.ShapeDtypeStruct((length, width), jnp.float32),
            jax.ShapeDtypeStruct((length, channels), jnp.float32),
            jax.ShapeDtypeStruct((share, width), jnp.float32),
        ),
        in_specs=in_vmem(8),
        out_specs=tuple(in_vmem(5)),
        scratch_shapes=exchange_scratch(n, blocks, width, channels)
        + [
            pltpu.VMEM((length, width), jnp.bfloat16),
            pltpu.VMEM((2, n // 2, share, width), jnp.bfloat16),
            pltpu.VMEM((n // 2, share, width), jnp.bfloat16),
            pltpu.VMEM((n // 2, share, width), jnp.bfloat16),
            pltpu.VMEM((n // 2 - 1, share, width), jnp.bfloat16),
            pltpu.SemaphoreType.DMA((n // 2,)),
            pltpu.SemaphoreType.DMA((n // 2,)),
        ],
        compiler_params=pltpu.CompilerParams(
            collective_id=2, has_side_effects=True, vmem_limit_bytes=24 * 1024 * 1024
        ),
        cost_estimate=pl.CostEstimate(
            flops=8_000_000_000, bytes_accessed=4 * length * width, transcendentals=0
        ),
        name="mixer_backward",
    )(q, k, v, g, gathered, w_out, mixed, states)


def route_out(d_out, route_expert, route_weight, capacity):
    n, tp = lax.axis_size("sp"), lax.axis_size("tp")
    tokens, model_width = d_out.shape
    quarter = model_width // tp
    return pl.pallas_call(
        functools.partial(route_kernel, n, tp, capacity),
        out_shape=(
            jax.ShapeDtypeStruct((n, capacity, model_width), jnp.bfloat16),
            jax.ShapeDtypeStruct((2, tokens), jnp.int32),
        ),
        in_specs=in_vmem(3),
        out_specs=tuple(in_vmem(2)),
        scratch_shapes=[
            pltpu.VMEM((n, capacity, quarter), jnp.bfloat16),
            pltpu.SemaphoreType.DMA((n - 1,)),
            pltpu.SemaphoreType.DMA((n - 1,)),
            pltpu.SemaphoreType.DMA,
            pltpu.SemaphoreType.DMA((n, tp)),
            pltpu.SemaphoreType.DMA((n, tp)),
        ],
        compiler_params=pltpu.CompilerParams(
            collective_id=3, has_side_effects=True, vmem_limit_bytes=24 * 1024 * 1024
        ),
        cost_estimate=pl.CostEstimate(
            flops=8_000_000_000, bytes_accessed=4 * tokens * quarter, transcendentals=0
        ),
        name="route_out",
    )(d_out, route_expert.T, route_weight)


def route_back(summed, slots, d_out):
    n, tp = lax.axis_size("sp"), lax.axis_size("tp")
    capacity, quarter = summed.shape[1:]
    tokens = d_out.shape[0]
    return pl.pallas_call(
        functools.partial(return_kernel, n, tp, capacity),
        out_shape=jax.ShapeDtypeStruct((tp, tokens, quarter), jnp.bfloat16),
        in_specs=in_vmem(3),
        out_specs=in_vmem(1)[0],
        scratch_shapes=[
            pltpu.VMEM((n, capacity, quarter), jnp.bfloat16),
            pltpu.SemaphoreType.DMA((n - 1,)),
            pltpu.SemaphoreType.DMA((n - 1,)),
            pltpu.SemaphoreType.DMA,
            pltpu.SemaphoreType.DMA((tp,)),
            pltpu.SemaphoreType.DMA((tp,)),
        ],
        compiler_params=pltpu.CompilerParams(
            collective_id=4, has_side_effects=True, vmem_limit_bytes=24 * 1024 * 1024
        ),
        cost_estimate=pl.CostEstimate(
            flops=8_000_000_000, bytes_accessed=4 * tokens * quarter, transcendentals=0
        ),
        name="route_back",
    )(summed, slots, d_out)


def expert_pass(rows_in, routed_rows, gate_w, up_w, down_w):
    gate_pre = jnp.dot(rows_in, gate_w, preferred_element_type=jnp.float32)
    up_pre = jnp.dot(rows_in, up_w, preferred_element_type=jnp.float32)
    sigmoid_gate = jax.nn.sigmoid(gate_pre)
    active = gate_pre * sigmoid_gate
    hidden = (active * up_pre).astype(jnp.bfloat16)
    d_hidden = lax.dot_general(
        routed_rows, down_w, (((1,), (1,)), ((), ())), preferred_element_type=jnp.float32
    )
    d_gate = (d_hidden * up_pre * sigmoid_gate * (1.0 + gate_pre * (1.0 - sigmoid_gate))).astype(
        jnp.bfloat16
    )
    d_up = (d_hidden * active).astype(jnp.bfloat16)
    rows_first = (((0,), (0,)), ((), ()))
    grad_gate = lax.dot_general(
        rows_in, d_gate, rows_first, preferred_element_type=jnp.float32
    ).astype(jnp.bfloat16)
    grad_up = lax.dot_general(rows_in, d_up, rows_first, preferred_element_type=jnp.float32).astype(
        jnp.bfloat16
    )
    grad_down = lax.dot_general(
        hidden, routed_rows, rows_first, preferred_element_type=jnp.float32
    ).astype(jnp.bfloat16)
    return (grad_gate, grad_up, grad_down, d_gate, d_up)


def local(
    d_out,
    route_expert,
    route_weight,
    expert_inputs,
    w_gate,
    w_up,
    w_down,
    w_out,
    queries,
    keys,
    values,
    log_decay,
):
    model_width = d_out.shape[1]
    experts = lax.axis_size("sp")
    capacity = expert_inputs.shape[1] // experts
    quarter = model_width // lax.axis_size("tp")
    routed, slots = route_out(d_out, route_expert, route_weight, capacity)
    routed = routed.reshape(experts * capacity, model_width)
    rows_in = expert_inputs[0]
    gate_w = w_gate[0]
    up_w = w_up[0]
    grad_gate, grad_up, grad_down, d_gate, d_up = expert_pass(
        rows_in, routed, gate_w, up_w, w_down[0]
    )
    partial_terms = lax.dot_general(
        d_gate, gate_w, (((1,), (1,)), ((), ())), preferred_element_type=jnp.float32
    )
    partial_terms = partial_terms + lax.dot_general(
        d_up, up_w, (((1,), (1,)), ((), ())), preferred_element_type=jnp.float32
    )
    rounded = lax.optimization_barrier(partial_terms.astype(jnp.bfloat16)).astype(jnp.float32)
    summed = lax.psum_scatter(rounded.astype(jnp.bfloat16), "tp", scatter_dimension=1, tiled=True)
    scale_q = queries.shape[2] ** (-0.5)
    q, k, v, g = queries[:, 0], keys[:, 0], values[:, 0], log_decay[:, 0]
    mixed, states = mixer_forward(q, k, v, g, scale_q)
    summed, mixed, grad_gate, grad_up, grad_down = lax.optimization_barrier(
        (summed, mixed, grad_gate, grad_up, grad_down)
    )
    gathered = route_back(summed.reshape(experts, capacity, quarter), slots, d_out)
    grad_q, grad_k, grad_v, grad_g, grad_proj = mixer_backward(
        q, k, v, g, gathered, w_out, mixed, states, scale_q
    )
    return (
        grad_gate[None],
        grad_up[None],
        grad_down[None],
        grad_proj,
        grad_q[:, None],
        grad_k[:, None],
        grad_v.astype(jnp.bfloat16)[:, None],
        grad_g[:, None],
    )


def paired(me, offset):
    other = me
    bit = 1
    while bit <= offset:
        if offset & bit:
            other = other + bit - 2 * bit * lax.rem(me // bit, 2)
        bit *= 2
    return other


def prefix_copy(n, me, step, distance, index, send, recv, ssem, rsem):
    return pltpu.make_async_remote_copy(
        src_ref=send.at[index],
        dst_ref=recv.at[index],
        send_sem=ssem.at[index],
        recv_sem=rsem.at[index],
        device_id={"sp": lax.rem(me + step * distance + n, n)},
        device_id_type=MESH,
    )


def prefix_send(n, me, step, distance, index, local, ahead, scan, send, recv, ssem, rsem):
    width = local.shape[0]
    total, reach = scan
    decay = reach[0:1, :] * ahead[0:1, :]
    send[index, :width, :] = (total[...] * ahead[0:1, :] + local[...]).astype(jnp.bfloat16)
    send[index, width:, :] = jnp.broadcast_to(decay, (16, decay.shape[1])).astype(jnp.bfloat16)
    target = me + step * distance

    @pl.when(jnp.logical_and(target >= 0, target < n))
    def _():
        prefix_copy(n, me, step, distance, index, send, recv, ssem, rsem).start()


def prefix_take(n, me, step, distance, index, scan, send, recv, ssem, rsem):
    total, reach = scan
    width = total.shape[0]
    source = me - step * distance
    target = me + step * distance
    copy = prefix_copy(n, me, step, distance, index, send, recv, ssem, rsem)

    @pl.when(jnp.logical_and(target >= 0, target < n))
    def _():
        copy.wait_send()

    @pl.when(jnp.logical_and(source >= 0, source < n))
    def _():
        copy.wait_recv()
        total[...] = total[...] + recv[index, :width, :].astype(jnp.float32) * reach[0:1, :]
        reach[...] = reach[...] * recv[index, width : width + 1, :].astype(jnp.float32)


def distances(n):
    found = []
    step = 1
    while step < n:
        found.append(step)
        step *= 2
    return found


def expert_kernel(
    n,
    cap,
    scale,
    d_hbm,
    expert_ref,
    weight_ref,
    x_hbm,
    wg_hbm,
    wu_hbm,
    wd_hbm,
    q_ref,
    k_ref,
    v_ref,
    g_ref,
    w_hbm,
    grad_gate,
    grad_up,
    grad_down,
    grad_proj,
    grad_q,
    grad_k,
    grad_v,
    grad_g,
    wg_ref,
    wu_ref,
    wd_ref,
    proj_ref,
    gq_ref,
    gk_ref,
    gv_ref,
    gg_ref,
    gathered,
    mixed_ref,
    states_ref,
    d_ref,
    x_ref,
    routed,
    onehot,
    outbox,
    outbox_near,
    slope,
    active,
    hidden,
    d_gate,
    d_up,
    part,
    pair_in,
    far_out,
    far_in,
    sums,
    back,
    picked,
    turned,
    cum,
    kept,
    befores,
    inner,
    scaled,
    lifted_q,
    lifted_k,
    scores_ref,
    d_mixed,
    d_round,
    key_part,
    proj_out,
    proj_pair,
    proj_mine,
    proj_in,
    w_ref,
    mix_local,
    mix_ahead,
    mix_total,
    mix_reach,
    mix_send,
    mix_recv,
    lsem,
    osem,
    rs,
    rr,
    fs,
    fr,
    ps,
    pr,
    qs,
    qr,
    ds,
    dr,
    xs,
    xr,
    bs,
    br,
    ms,
    mr,
    gs,
    gr,
    ys,
    yr,
    zs,
    zr,
):
    me = lax.axis_index("sp")
    col = lax.axis_index("tp")
    core = lax.rem(col, 2)
    side = col // 2
    partner = col + 1 - 2 * core
    far = lax.rem(col + 2, 4)
    chunks = n // 2
    rows2 = 2 * cap
    tokens = d_ref.shape[0]
    model = d_ref.shape[1]
    quarter = model // 4
    half = model // 2
    near = 3
    cuts = [pl.ds(0, quarter // 2), pl.ds(quarter // 2, quarter // 2)]

    barrier, greeted = greet(n, me, [partner, far])

    def chunk_rows(z):
        return pl.ds(z * rows2, rows2)

    def block_rows(m):
        return pl.ds(m * cap, cap)

    def columns(q):
        return pl.ds(pl.multiple_of(q * quarter, quarter), quarter)

    order = [0, chunks - 1, 1] + list(range(chunks - 2, 1, -1))
    loads = {}

    def load(name, source, target, index):
        loads[name] = pltpu.make_async_copy(source, target, lsem.at[index])
        loads[name].start()

    load("d", d_hbm, d_ref, 0)
    load("wg", wg_hbm, wg_ref, 1)

    def load_rows(z):
        for m in (2 * z, 2 * z + 1):
            first = pl.multiple_of(paired(me, m) * cap, cap)
            load(("x", m), x_hbm.at[pl.ds(first, cap), :], x_ref.at[block_rows(m), :], 4 + m)

    load_rows(0)
    load("wu", wu_hbm, wu_ref, 2)
    load("wd", wd_hbm, wd_ref, 3)
    for z in order[1:]:
        load_rows(z)
    load("w", w_hbm, w_ref, 4 + n)

    kinds = lax.broadcasted_iota(jnp.int32, (n, tokens), 0)
    named = [(kinds == expert_ref[j : j + 1, :]).astype(jnp.float32) for j in range(2)]
    earlier = lax.broadcasted_iota(jnp.int32, (tokens, tokens), 0) < lax.broadcasted_iota(
        jnp.int32, (tokens, tokens), 1
    )
    before = mm((named[0] + named[1]).astype(jnp.bfloat16), earlier.astype(jnp.bfloat16), NN)
    slots = []
    for j in range(2):
        rank = jnp.sum(before * named[j], axis=0, keepdims=True).astype(jnp.int32)
        slots.append(expert_ref[j : j + 1, :] * cap + rank)
    places = lax.broadcasted_iota(jnp.int32, (cap, tokens), 0)

    def routed_rows(m, chosen):
        first = paired(me, m) * cap
        hits = [(slots[j] - first == places).astype(jnp.float32) for j in range(2)]
        both = (hits[0] + hits[1]).astype(jnp.bfloat16)
        onehot[block_rows(m), :] = both
        weight = jnp.sum(
            hits[0] * weight_ref[0:1, :] + hits[1] * weight_ref[1:2, :], axis=1, keepdims=True
        )
        return (mm(both, chosen, NN) * weight).astype(jnp.bfloat16)

    def route(m):
        if m <= near:
            source = outbox_near.at[block_rows(m - 1), :]
            target = routed.at[block_rows(m), pl.ds(pl.multiple_of(core * half, half), half)]
        else:
            source = outbox.at[block_rows(m - near - 1), :]
            target = routed.at[block_rows(m), columns(col)]
        return pltpu.make_async_remote_copy(
            src_ref=source,
            dst_ref=target,
            send_sem=rs.at[m],
            recv_sem=rr.at[m],
            device_id={"sp": paired(me, m)},
            device_id_type=MESH,
        )

    def pass_on(m, what, target, send_sem, recv_sem):
        if m <= near:
            piece = routed.at[block_rows(m), pl.ds(pl.multiple_of(what * half, half), half)]
        else:
            piece = routed.at[block_rows(m), columns(what)]
        return pltpu.make_async_remote_copy(
            src_ref=piece,
            dst_ref=piece,
            send_sem=send_sem.at[m],
            recv_sem=recv_sem.at[m],
            device_id={"tp": target},
            device_id_type=MESH,
        )

    sent = []
    loads["d"].wait()
    sends = []
    for z in range(chunks - 1, 0, -1):
        sends += [2 * z, 2 * z + 1]
    sends.insert(1, 1)
    greeting = True
    for m in sends:
        if m <= near:
            outbox_near[block_rows(m - 1), :] = routed_rows(
                m, d_ref[:, pl.ds(pl.multiple_of(core * half, half), half)]
            )
        else:
            outbox[block_rows(m - near - 1), :] = routed_rows(m, d_ref[:, columns(col)])
        if greeting:
            pl.semaphore_wait(barrier, greeted)
            greeting = False
        sent.append(route(m))
        sent[-1].start()
    routed[block_rows(0), :] = routed_rows(0, d_ref[...])

    crossed, beside, relayed = {}, {}, {}

    def arrive(m):
        route(m).wait_recv()
        if m <= near:
            beside[m] = pass_on(m, core, partner, ps, pr)
            beside[m].start()
            return
        crossed[m] = pass_on(m, col, far, fs, fr)
        crossed[m].start()
        beside[m] = pass_on(m, col, partner, ps, pr)
        beside[m].start()

    def relay(m):
        if m <= near:
            return
        crossed[m].wait_recv()
        relayed[m] = pass_on(m, far, partner, qs, qr)
        relayed[m].start()

    def complete(m):
        beside[m].wait_recv()
        if m > near:
            relayed[m].wait_recv()

    def gates(z):
        rows = chunk_rows(z)
        held = order.index(z) % 2
        loads[("x", 2 * z)].wait()
        loads[("x", 2 * z + 1)].wait()
        if z == 0:
            loads["wg"].wait()
        gate = mm(x_ref[rows, :], wg_ref[...], NT)
        if z == 0:
            loads["wu"].wait()
        up = mm(x_ref[rows, :], wu_ref[...], NT)
        sigmoid = jax.nn.sigmoid(gate)
        silu = gate * sigmoid
        hidden[rows, :] = (silu * up).astype(jnp.bfloat16)
        active[held] = silu
        slope[held] = up * sigmoid * (1.0 + gate * (1.0 - sigmoid))

    halves = {}

    def experts(z):
        rows = chunk_rows(z)
        if z == 0:
            loads["wd"].wait()
        d_hidden = mm(routed[rows, :], wd_ref[...], NT)
        held = order.index(z) % 2
        d_gate[rows, :] = (d_hidden * slope[held]).astype(jnp.bfloat16)
        d_up[rows, :] = (d_hidden * active[held]).astype(jnp.bfloat16)
        for whose in (1 - core, core):
            for i in range(2):
                across = 1 - side if i == 0 else side
                cut = columns(2 * across + whose)
                term = mm(d_gate[rows, :], wg_ref[:, cut], NN) + mm(
                    d_up[rows, :], wu_ref[:, cut], NN
                )
                part[rows, cut] = term.astype(jnp.bfloat16)
            if (z, 0) in halves:
                continue
            for i in range(2):
                across = 1 - side if i == 0 else side
                halves[(z, i)] = pltpu.make_async_remote_copy(
                    src_ref=part.at[rows, columns(2 * across + 1 - core)],
                    dst_ref=pair_in.at[i, rows, :],
                    send_sem=ds.at[z, i],
                    recv_sem=dr.at[z, i],
                    device_id={"tp": partner},
                    device_id_type=MESH,
                )
                halves[(z, i)].start()

    over = {}

    def half_of(q, h):
        first = q * quarter + h * (quarter // 2)
        return pl.ds(pl.multiple_of(first, quarter // 2), quarter // 2)

    def reduce_near(z):
        rows = chunk_rows(z)
        halves[(z, 0)].wait_recv()
        for h in range(2):
            far_out[rows, cuts[h]] = (
                part[rows, half_of(far, h)].astype(jnp.float32)
                + pair_in[0, rows, cuts[h]].astype(jnp.float32)
            ).astype(jnp.bfloat16)
            over[(z, h)] = pltpu.make_async_remote_copy(
                src_ref=far_out.at[rows, cuts[h]],
                dst_ref=far_in.at[rows, cuts[h]],
                send_sem=xs.at[z, h],
                recv_sem=xr.at[z, h],
                device_id={"tp": far},
                device_id_type=MESH,
            )
            over[(z, h)].start()

    returned = {}

    def reduce_far(z):
        halves[(z, 1)].wait_recv()
        for h in range(2):
            reduce_half(z, h)

    def reduce_half(z, h):
        rows = chunk_rows(z)
        over[(z, h)].wait_recv()
        sums[rows, cuts[h]] = (
            part[rows, half_of(col, h)].astype(jnp.float32)
            + pair_in[1, rows, cuts[h]].astype(jnp.float32)
            + far_in[rows, cuts[h]].astype(jnp.float32)
        ).astype(jnp.bfloat16)
        for m in (2 * z, 2 * z + 1):
            if m == 0:
                back[block_rows(0), cuts[h]] = sums[block_rows(0), cuts[h]]
                continue
            returned[(m, h)] = pltpu.make_async_remote_copy(
                src_ref=sums.at[block_rows(m), cuts[h]],
                dst_ref=back.at[block_rows(m), cuts[h]],
                send_sem=bs.at[m, h],
                recv_sem=br.at[m, h],
                device_id={"sp": paired(me, m)},
                device_id_type=MESH,
            )
            returned[(m, h)].start()

    def pick(z, h):
        rows = chunk_rows(z)
        for m in (2 * z, 2 * z + 1):
            if m > 0:
                returned[(m, h)].wait_recv()
        found = mm(onehot[rows, :], back[rows, cuts[h]], TN)
        picked[:, cuts[h]] = found if z == 0 else picked[:, cuts[h]] + found

    stored = []

    def store(source, target):
        stored.append(pltpu.make_async_copy(source, target, osem.at[len(stored)]))
        stored[-1].start()

    def weight_grad(lhs, rhs, out, target):
        turned[...] = lhs[...].T

        def piece(i, carry):
            cut = columns(i)
            out[:, cut] = mm(turned[...], rhs[:, cut], NN).astype(jnp.bfloat16)
            return carry

        lax.fori_loop(0, 4, piece, 0)
        store(out, target)

    blocks = tokens // BLK
    causal = triangle(True)
    width = v_ref.shape[1]
    scan = (mix_total, mix_reach)
    reach = distances(n)
    rounds = len(reach)

    def scan_from(local, ahead):
        mix_local[...] = local
        mix_ahead[...] = jnp.broadcast_to(jnp.exp(ahead), mix_ahead.shape)
        mix_total[...] = jnp.zeros(mix_total.shape, jnp.float32)
        mix_reach[...] = jnp.ones(mix_reach.shape, jnp.float32)

    def mixer_states():
        local = jnp.zeros(mix_total.shape, jnp.float32)
        ahead = jnp.zeros((1, q_ref.shape[1]), jnp.float32)
        for b in range(blocks):
            rows = pl.ds(b * BLK, BLK)
            cumulative, _, ending = decays(g_ref, rows)
            cum[rows, :] = cumulative
            kept[b] = local
            befores[b : b + 1, :] = jnp.exp(ahead)
            faded = (k_ref[rows, :].astype(jnp.float32) * jnp.exp(ending - cumulative)).astype(
                jnp.bfloat16
            )
            local = local * jnp.exp(ending) + mm(v_ref[rows, :], faded, TN)
            ahead = ahead + ending
        scan_from(local, ahead)

    def mixer_send(step, index):
        at = index if step > 0 else rounds + index
        distance = reach[index]
        prefix_send(
            n, me, step, distance, at, mix_local, mix_ahead, scan, mix_send, mix_recv, ms, mr
        )

    def mixer_take(step, index):
        at = index if step > 0 else rounds + index
        prefix_take(n, me, step, reach[index], at, scan, mix_send, mix_recv, ms, mr)

    def mixer_inner():
        for b in range(blocks):
            rows = pl.ds(b * BLK, BLK)
            cumulative = cum[rows, :]
            middle = cumulative[BLK // 2 - 1 : BLK // 2, :]
            query = q_ref[rows, :].astype(jnp.float32) * scale
            key = k_ref[rows, :].astype(jnp.float32)
            up_q = (query * jnp.exp(cumulative - middle)).astype(jnp.bfloat16)
            up_k = (key * jnp.exp(middle - cumulative)).astype(jnp.bfloat16)
            scores = jnp.where(causal, mm(up_q, up_k, NT), 0.0).astype(jnp.bfloat16)
            lifted_q[rows, :] = up_q
            lifted_k[rows, :] = up_k
            scores_ref[rows, :] = scores
            inner[rows, :] = mm(scores, v_ref[rows, :], NN)
            scaled[rows, :] = (query * jnp.exp(cumulative)).astype(jnp.bfloat16)

    def mixer_finish():
        for b in range(blocks):
            rows = pl.ds(b * BLK, BLK)
            state = (kept[b] + mix_total[...] * befores[b : b + 1, :]).astype(jnp.bfloat16)
            states_ref[b] = state
            mixed_ref[rows, :] = (inner[rows, :] + mm(scaled[rows, :], state, NT)).astype(
                jnp.bfloat16
            )

    taken = [0]

    def mixer_round(step):
        if taken[0] < rounds:
            mixer_take(step, taken[0])
            taken[0] += 1
            if taken[0] < rounds:
                mixer_send(step, taken[0])

    share, turns = proj_out.shape[3], proj_out.shape[1]
    parity = lax.rem(me, 2)
    at_z = me // 2
    paired_off, handed = {}, []

    def project(j, h):
        first = paired(col, j) * quarter + h * (quarter // 2)
        rows = pl.ds(pl.multiple_of(first, quarter // 2), quarter // 2)
        grads = gathered[j, :, cuts[h]]
        term = mm(grads, w_ref[rows, :], NN)
        d_mixed[...] = term if j + h == 0 else d_mixed[...] + term
        product = mm(grads, mixed_ref[...], TN).astype(jnp.bfloat16)
        for t in range(turns):
            at = h * turns + t
            proj_out[j, at // 2, at % 2] = product[t * share : (t + 1) * share, :]

    def pair_up(j):
        for i in range(turns):
            paired_off[(j, i)] = pltpu.make_async_remote_copy(
                src_ref=proj_out.at[j, i, 1 - parity],
                dst_ref=proj_pair.at[j, i],
                send_sem=ys.at[j, i],
                recv_sem=yr.at[j, i],
                device_id={"sp": me + 1 - 2 * parity},
                device_id_type=MESH,
            )
            paired_off[(j, i)].start()

    def hand_over(j):
        q = paired(col, j)
        for i in range(turns):
            paired_off[(j, i)].wait_recv()
            both_rows = proj_out[j, i, parity].astype(jnp.float32) + proj_pair[j, i].astype(
                jnp.float32
            )
            proj_out[j, i, parity] = both_rows.astype(jnp.bfloat16)
            owner = q * turns + i
            away = jnp.int32(0)
            bit = 1
            while bit < chunks:
                away = away + bit * lax.rem(at_z // bit + owner // bit, 2)
                bit *= 2
            copy = pltpu.make_async_remote_copy(
                src_ref=proj_out.at[j, i, parity],
                dst_ref=proj_in.at[away],
                send_sem=zs.at[j, i],
                recv_sem=zr.at[away],
                device_id={"sp": 2 * owner + parity},
                device_id_type=MESH,
            )
            handed.append((away, copy))

            @pl.when(away == 0)
            def _():
                proj_mine[...] = proj_out[j, i, parity].astype(jnp.float32)

            @pl.when(away != 0)
            def _():
                copy.start()

    def project_sum():
        total = proj_mine[...]
        for z in range(1, chunks):
            pltpu.make_async_remote_copy(
                src_ref=proj_out.at[0, 0, parity],
                dst_ref=proj_in.at[z],
                send_sem=zs.at[0, 0],
                recv_sem=zr.at[z],
                device_id={"sp": paired(me, 2 * z)},
                device_id_type=MESH,
            ).wait_recv()
            total = total + proj_in[z].astype(jnp.float32)
        proj_ref[...] = total

    def back_states():
        d_round[...] = d_mixed[...].astype(jnp.bfloat16)
        local = jnp.zeros(mix_total.shape, jnp.float32)
        after = jnp.zeros((1, q_ref.shape[1]), jnp.float32)
        for b in reversed(range(blocks)):
            rows = pl.ds(b * BLK, BLK)
            ending = cum[b * BLK + BLK - 1 : b * BLK + BLK, :]
            kept[b] = local
            befores[b : b + 1, :] = jnp.exp(after)
            local = local * jnp.exp(ending) + mm(d_round[rows, :], scaled[rows, :], TN)
            after = after + ending
        scan_from(local, after)

    def back_inner():
        for b in range(blocks):
            rows = pl.ds(b * BLK, BLK)
            cumulative = cum[rows, :]
            middle = cumulative[BLK // 2 - 1 : BLK // 2, :]
            query = q_ref[rows, :].astype(jnp.float32) * scale
            d_out = d_round[rows, :]
            up_q, up_k = lifted_q[rows, :], lifted_k[rows, :]
            d_scores = jnp.where(causal, mm(d_out, v_ref[rows, :], NT), 0.0).astype(jnp.bfloat16)
            d_up_q = mm(d_scores, up_k, NN)
            d_up_k = mm(d_scores, up_q, TN)
            d_carried = mm(d_out, states_ref[b], NN) * jnp.exp(cumulative)
            gq_ref[rows, :] = (
                (d_up_q * jnp.exp(cumulative - middle) + d_carried) * scale
            ).astype(jnp.bfloat16)
            gg_ref[rows, :] = (
                up_q.astype(jnp.float32) * d_up_q
                - up_k.astype(jnp.float32) * d_up_k
                + query * d_carried
            )
            key_part[rows, :] = d_up_k * jnp.exp(middle - cumulative)
            inner[rows, :] = mm(scores_ref[rows, :], d_out, TN)

    def back_finish():
        for b in range(blocks):
            rows = pl.ds(b * BLK, BLK)
            cumulative = cum[rows, :]
            ending = cumulative[BLK - 1 : BLK, :]
            d_state = kept[b] + mix_total[...] * befores[b : b + 1, :]
            d_rounded = d_state.astype(jnp.bfloat16)
            fade = jnp.exp(ending - cumulative)
            faded = k_ref[rows, :].astype(jnp.float32) * fade
            d_faded = mm(v_ref[rows, :], d_rounded, NN)
            gk_ref[rows, :] = (key_part[rows, :] + d_faded * fade).astype(jnp.bfloat16)
            gv_ref[rows, :] = (
                inner[rows, :] + mm(faded.astype(jnp.bfloat16), d_rounded, NT)
            ).astype(jnp.bfloat16)
            moved = faded * d_faded
            at_end = jnp.sum(moved, axis=0, keepdims=True) + jnp.exp(ending) * jnp.sum(
                states_ref[b].astype(jnp.float32) * d_state, axis=0, keepdims=True
            )
            gg_ref[rows, :] = block_sums(triangle(False), gg_ref[rows, :] - moved) + at_end

    def both(step, z):
        step(2 * z)
        step(2 * z + 1)

    def give(block, slot, target, h):
        return pltpu.make_async_remote_copy(
            src_ref=gathered.at[block, :, cuts[h]],
            dst_ref=gathered.at[slot, :, cuts[h]],
            send_sem=gs.at[slot, h],
            recv_sem=gr.at[slot, h],
            device_id={"tp": target},
            device_id_type=MESH,
        )

    def share_out(h):
        first = pl.multiple_of(col * quarter + h * (quarter // 2), quarter // 2)
        own = d_ref[:, pl.ds(first, quarter // 2)].astype(jnp.float32)
        gathered[0, :, cuts[h]] = (own + picked[:, cuts[h]]).astype(jnp.bfloat16)
        given[(2, h)] = give(0, 2, far, h)
        given[(1, h)] = give(0, 1, partner, h)
        given[(2, h)].start()
        given[(1, h)].start()

    def share_on(h):
        given[(2, h)].wait_recv()
        given[(3, h)] = give(2, 3, partner, h)
        given[(3, h)].start()

    def settle(slot, h):
        given[(slot, h)].wait_recv()

    given = {}
    early = order[1:]
    gates(0)
    mixer_states()
    mixer_send(1, 0)
    gates(early[0])
    arrive(1)
    mixer_inner()
    arrive(2 * early[0])
    complete(1)
    experts(0)
    arrive(2 * early[0] + 1)
    reduce_near(0)
    gates(early[1])
    both(relay, early[0])
    both(complete, early[0])
    experts(early[0])
    for z in early[2:]:
        both(arrive, z)
    mixer_round(1)
    reduce_near(early[0])
    reduce_far(0)
    both(arrive, early[1])
    pending = [early[0]]
    for i, z in enumerate(early[1:]):
        following = early[i + 2] if i + 2 < len(early) else None
        both(relay, z)
        both(complete, z)
        experts(z)
        mixer_round(1)
        if following is not None:
            gates(following)
        if i > 0:
            reduce_far(pending.pop(0))
        reduce_near(z)
        pending.append(z)
    weight_grad(hidden, routed, wd_ref, grad_down)
    reduce_far(pending.pop(0))
    pick(0, 0)
    pick(0, 1)
    reduce_far(pending.pop(0))
    weight_grad(d_gate, x_ref, wg_ref, grad_gate)
    while taken[0] < rounds:
        mixer_round(1)
    mixer_finish()
    weight_grad(d_up, x_ref, wu_ref, grad_up)
    loads["w"].wait()
    for z in early:
        pick(z, 0)
    share_out(0)
    project(0, 0)
    for z in early:
        pick(z, 1)
    share_out(1)
    project(0, 1)
    pair_up(0)
    settle(1, 0)
    project(1, 0)
    settle(1, 1)
    project(1, 1)
    pair_up(1)
    share_on(0)
    project(2, 0)
    hand_over(0)
    hand_over(1)
    share_on(1)
    project(2, 1)
    pair_up(2)
    settle(3, 0)
    project(3, 0)
    settle(3, 1)
    project(3, 1)
    back_states()
    taken[0] = 0
    mixer_send(-1, 0)
    pair_up(3)
    back_inner()
    mixer_round(-1)
    mixer_round(-1)
    hand_over(2)
    hand_over(3)
    mixer_round(-1)
    store(gq_ref, grad_q)
    back_finish()
    store(gk_ref, grad_k)
    store(gv_ref, grad_v)
    store(gg_ref, grad_g)
    project_sum()
    store(proj_ref, grad_proj)
    for copy in stored:
        copy.wait()
    for copy in sent:
        copy.wait_send()
    for group in (given, crossed, beside, relayed, halves, over, returned, paired_off):
        for copy in group.values():
            copy.wait_send()
    for away, copy in handed:

        @pl.when(away != 0)
        def _():
            copy.wait_send()


def expert_stage(
    d_out, route_expert, route_weight, rows_in, gate_t, up_t, down, q, k, v, g, w_out, cap, scale
):
    n = lax.axis_size("sp")
    tokens, model = d_out.shape
    quarter = model // 4
    units = down.shape[0]
    slots = n * cap
    channels, width = q.shape[1], v.shape[1]
    blocks = tokens // BLK
    rounds = len(distances(n))
    share = model // n
    turns = n // 8
    bf16, f32 = jnp.bfloat16, jnp.float32
    weight_shape = jax.ShapeDtypeStruct((units, model), bf16)
    out_shape = (
        weight_shape,
        weight_shape,
        weight_shape,
        jax.ShapeDtypeStruct((share, width), f32),
        jax.ShapeDtypeStruct((tokens, channels), bf16),
        jax.ShapeDtypeStruct((tokens, channels), bf16),
        jax.ShapeDtypeStruct((tokens, width), bf16),
        jax.ShapeDtypeStruct((tokens, channels), f32),
    )
    anywhere = pl.BlockSpec(memory_space=pl.ANY)
    local = pl.BlockSpec(memory_space=pltpu.VMEM)
    dma = pltpu.SemaphoreType.DMA
    return pl.pallas_call(
        functools.partial(expert_kernel, n, cap, scale),
        out_shape=out_shape,
        in_specs=[anywhere, local, local] + [anywhere] * 4 + [local] * 4 + [anywhere],
        out_specs=(anywhere,) * 8,
        scratch_shapes=[pltpu.VMEM(a.shape, a.dtype) for a in out_shape]
        + [
            pltpu.VMEM((4, tokens, quarter), bf16),
            pltpu.VMEM((tokens, width), bf16),
            pltpu.VMEM((blocks, width, channels), bf16),
            pltpu.VMEM((tokens, model), bf16),
            pltpu.VMEM((slots, model), bf16),
            pltpu.VMEM((slots, model), bf16),
            pltpu.VMEM((slots, tokens), bf16),
            pltpu.VMEM((slots - 4 * cap, quarter), bf16),
            pltpu.VMEM((3 * cap, model // 2), bf16),
            pltpu.VMEM((2, 2 * cap, units), f32),
            pltpu.VMEM((2, 2 * cap, units), f32),
            pltpu.VMEM((slots, units), bf16),
            pltpu.VMEM((slots, units), bf16),
            pltpu.VMEM((slots, units), bf16),
            pltpu.VMEM((slots, model), bf16),
            pltpu.VMEM((2, slots, quarter), bf16),
            pltpu.VMEM((slots, quarter), bf16),
            pltpu.VMEM((slots, quarter), bf16),
            pltpu.VMEM((slots, quarter), bf16),
            pltpu.VMEM((slots, quarter), bf16),
            pltpu.VMEM((tokens, quarter), f32),
            pltpu.VMEM((units, slots), bf16),
            pltpu.VMEM((tokens, channels), f32),
            pltpu.VMEM((blocks, width, channels), f32),
            pltpu.VMEM((blocks, channels), f32),
            pltpu.VMEM((tokens, width), f32),
            pltpu.VMEM((tokens, channels), bf16),
            pltpu.VMEM((tokens, channels), bf16),
            pltpu.VMEM((tokens, channels), bf16),
            pltpu.VMEM((tokens, BLK), bf16),
            pltpu.VMEM((tokens, width), f32),
            pltpu.VMEM((tokens, width), bf16),
            pltpu.VMEM((tokens, channels), f32),
            pltpu.VMEM((4, turns, 2, share, width), bf16),
            pltpu.VMEM((4, turns, share, width), bf16),
            pltpu.VMEM((share, width), f32),
            pltpu.VMEM((n // 2, share, width), bf16),
            pltpu.VMEM((model, width), bf16),
            pltpu.VMEM((width, channels), f32),
            pltpu.VMEM((8, channels), f32),
            pltpu.VMEM((width, channels), f32),
            pltpu.VMEM((8, channels), f32),
            pltpu.VMEM((2 * rounds, width + 16, channels), bf16),
            pltpu.VMEM((2 * rounds, width + 16, channels), bf16),
            dma((5 + n,)),
            dma((8,)),
            dma((n,)),
            dma((n,)),
            dma((n,)),
            dma((n,)),
            dma((n,)),
            dma((n,)),
            dma((n,)),
            dma((n,)),
            dma((n // 2, 2)),
            dma((n // 2, 2)),
            dma((n // 2, 2)),
            dma((n // 2, 2)),
            dma((n, 2)),
            dma((n, 2)),
            dma((2 * rounds,)),
            dma((2 * rounds,)),
            dma((4, 2)),
            dma((4, 2)),
            dma((4, turns)),
            dma((4, turns)),
            dma((4, turns)),
            dma((n // 2,)),
        ],
        compiler_params=pltpu.CompilerParams(
            collective_id=5, has_side_effects=True, vmem_limit_bytes=60 * 1024 * 1024
        ),
        cost_estimate=pl.CostEstimate(
            flops=60_000_000_000, bytes_accessed=30_000_000, transcendentals=0
        ),
        name="expert_stage",
    )(d_out, route_expert.T, route_weight.T, rows_in, gate_t, up_t, down, q, k, v, g, w_out)


def store_kernel(pieces, count, *refs):
    sources, targets, held = refs[:count], refs[count : 2 * count], refs[2 * count : 3 * count]
    isem, osem = refs[3 * count :]
    cuts = []
    for i in range(count):
        parts = pieces if i < 3 else 1
        rows = sources[i].shape[0] // parts
        cuts += [(i, pl.ds(p * rows, rows)) for p in range(parts)]
    reads = [
        pltpu.make_async_copy(sources[i].at[cut, :], held[i].at[cut, :], isem.at[at])
        for at, (i, cut) in enumerate(cuts)
    ]
    writes = [
        pltpu.make_async_copy(held[i].at[cut, :], targets[i].at[cut, :], osem.at[at])
        for at, (i, cut) in enumerate(cuts)
    ]
    for read in reads:
        read.start()
    for read, write in zip(reads, writes):
        read.wait()
        write.start()
    for write in writes:
        write.wait()


def store_out(arrays):
    count = len(arrays)
    pieces = 4 if arrays[0].shape[0] % 64 == 0 else 1
    total = 3 * pieces + count - 3
    anywhere = pl.BlockSpec(memory_space=pl.ANY)
    return pl.pallas_call(
        functools.partial(store_kernel, pieces, count),
        out_shape=tuple(jax.ShapeDtypeStruct(a.shape, a.dtype) for a in arrays),
        in_specs=[anywhere] * count,
        out_specs=(anywhere,) * count,
        scratch_shapes=[pltpu.VMEM(a.shape, a.dtype) for a in arrays]
        + [pltpu.SemaphoreType.DMA((total,)), pltpu.SemaphoreType.DMA((total,))],
        compiler_params=pltpu.CompilerParams(vmem_limit_bytes=60 * 1024 * 1024),
        name="store_out",
    )(*arrays)


def fused_local(
    d_out,
    route_expert,
    route_weight,
    expert_inputs,
    w_gate,
    w_up,
    w_down,
    w_out,
    queries,
    keys,
    values,
    log_decay,
):
    experts = lax.axis_size("sp")
    capacity = expert_inputs.shape[1] // experts
    scale_q = queries.shape[2] ** (-0.5)
    q, k, v, g = queries[:, 0], keys[:, 0], values[:, 0], log_decay[:, 0]
    results = expert_stage(
        d_out,
        route_expert,
        route_weight,
        expert_inputs[0],
        w_gate[0].T,
        w_up[0].T,
        w_down[0],
        q,
        k,
        v,
        g,
        w_out,
        capacity,
        scale_q,
    )
    grad_gate, grad_up, grad_down, grad_proj, grad_q, grad_k, grad_v, grad_g = store_out(results)
    return (
        grad_gate.T[None],
        grad_up.T[None],
        grad_down[None],
        grad_proj,
        grad_q[:, None],
        grad_k[:, None],
        grad_v[:, None],
        grad_g[:, None],
    )


def choose(*arrays):
    n, tp = lax.axis_size("sp"), lax.axis_size("tp")
    tokens, model = arrays[0].shape
    capacity = arrays[3].shape[1] // n
    power = n & (n - 1) == 0 and n % 8 == 0
    if tp == 4 and power and capacity % 16 == 0 and n * capacity <= 1536 and model % 512 == 0:
        return fused_local(*arrays)
    return local(*arrays)


def solution(mesh):
    return jax.shard_map(
        choose,
        mesh=mesh,
        in_specs=(
            P("sp", None),
            P("sp", None),
            P("sp", None),
            P("sp", None, None),
            P("sp", None, "tp"),
            P("sp", None, "tp"),
            P("sp", "tp", None),
            P(None, "tp"),
            P("sp", "tp", None),
            P("sp", "tp", None),
            P("sp", "tp", None),
            P("sp", "tp", None),
        ),
        out_specs=(
            P("sp", None, "tp"),
            P("sp", None, "tp"),
            P("sp", "tp", None),
            P("sp", "tp"),
            P("sp", "tp", None),
            P("sp", "tp", None),
            P("sp", "tp", None),
            P("sp", "tp", None),
        ),
        check_vma=False,
    )
```

```python
import functools

import jax
import jax.numpy as jnp
from jax import lax
from jax.experimental import pallas as pl
from jax.experimental.pallas import tpu as pltpu
from jax.sharding import PartitionSpec as P

BLK = 64


precise = lax.Precision.HIGHEST


MESH = pl.DeviceIdType.MESH
NN = (((1,), (0,)), ((), ()))
NT = (((1,), (1,)), ((), ()))
TN = (((0,), (0,)), ((), ()))


def mm(a, b, dims):
    return lax.dot_general(a, b, dims, preferred_element_type=jnp.float32)


def triangle(lower):
    rows = lax.broadcasted_iota(jnp.int32, (BLK, BLK), 0)
    cols = lax.broadcasted_iota(jnp.int32, (BLK, BLK), 1)
    return rows >= cols if lower else rows <= cols


def block_sums(mask, x):
    return lax.dot_general(
        mask.astype(jnp.float32), x, NN, precision=precise, preferred_element_type=jnp.float32
    )


def decays(g_ref, rows):
    cumulative = block_sums(triangle(True), g_ref[rows, :])
    middle = cumulative[BLK // 2 - 1 : BLK // 2, :]
    ending = cumulative[BLK - 1 : BLK, :]
    return cumulative, middle, ending


def greet(n, me, tp=None):
    barrier = pltpu.get_barrier_semaphore()
    others = [{"sp": lax.rem(me + k, n)} for k in range(1, n)]
    if tp is not None:
        others += [{"tp": other} for other in tp]
    for other in others:
        pl.semaphore_signal(barrier, inc=1, device_id=other, device_id_type=MESH)
    return barrier, len(others)


def route_kernel(
    n,
    tp,
    cap,
    d_ref,
    expert_ref,
    weight_ref,
    routed_ref,
    slot_ref,
    outbox,
    ssem,
    rsem,
    lsem,
    tsend,
    trecv,
):
    me = lax.axis_index("sp")
    col = lax.axis_index("tp")
    partner = col + 1 - 2 * lax.rem(col, 2)
    far = [lax.rem(col + 2 * s, tp) for s in range(1, tp // 2)]
    barrier, greeted = greet(n, me, [partner] + far)
    tokens = d_ref.shape[0]
    quarter = outbox.shape[2]
    start = pl.multiple_of(lax.axis_index("tp") * quarter, quarter)
    own = d_ref[:, pl.ds(start, quarter)].astype(jnp.float32)
    kinds = lax.broadcasted_iota(jnp.int32, (n, tokens), 0)
    named = [(kinds == expert_ref[j : j + 1, :]).astype(jnp.float32) for j in range(2)]
    earlier = lax.broadcasted_iota(jnp.int32, (tokens, tokens), 0) < lax.broadcasted_iota(
        jnp.int32, (tokens, tokens), 1
    )
    before = mm((named[0] + named[1]).astype(jnp.bfloat16), earlier.astype(jnp.bfloat16), NN)
    scaled = []
    slots = []
    for j in range(2):
        rank = jnp.sum(before * named[j], axis=0, keepdims=True).astype(jnp.int32)
        slots.append(expert_ref[j : j + 1, :] * cap + rank)
        slot_ref[j : j + 1, :] = slots[j]
        scaled.append((own * weight_ref[:, j : j + 1]).astype(jnp.bfloat16))
    places = lax.broadcasted_iota(jnp.int32, (cap, tokens), 0)
    for e in range(n):
        rows = jnp.zeros((cap, quarter), jnp.float32)
        for j in range(2):
            picks = (slots[j] - e * cap == places).astype(jnp.float32).astype(jnp.bfloat16)
            rows = rows + mm(picks, scaled[j], NN)
        outbox[e] = rows.astype(jnp.bfloat16)
    pl.semaphore_wait(barrier, greeted)

    def place(row, column):
        return routed_ref.at[row, :, pl.ds(pl.multiple_of(column * quarter, quarter), quarter)]

    copies = []
    for k in range(1, n):
        peer = lax.rem(me + k, n)
        copies.append(
            pltpu.make_async_remote_copy(
                src_ref=outbox.at[peer],
                dst_ref=place(me, col),
                send_sem=ssem.at[k - 1],
                recv_sem=rsem.at[k - 1],
                device_id={"sp": peer},
                device_id_type=MESH,
            )
        )
        copies[-1].start()
    stays = pltpu.make_async_copy(outbox.at[me], place(me, col), lsem)
    stays.start()

    def send(k, column, slot, target):
        row = lax.rem(me - k + n, n)
        return pltpu.make_async_remote_copy(
            src_ref=place(row, column),
            dst_ref=place(row, column),
            send_sem=tsend.at[k, slot],
            recv_sem=trecv.at[k, slot],
            device_id={"tp": target},
            device_id_type=MESH,
        )

    across, beside, passed = [], [], []

    def pass_on(k):
        for s in range(len(far)):
            across[k][s].wait_recv()
            column = lax.rem(col - 2 * (s + 1) + tp, tp)
            passed.append(send(k, column, tp // 2 + s, partner))
            passed[-1].start()

    for k in range(n):
        if k == 0:
            stays.wait()
        else:
            copies[k - 1].wait_recv()
        across.append([send(k, col, s + 1, far[s]) for s in range(len(far))])
        for copy in across[k]:
            copy.start()
        beside.append(send(k, col, 0, partner))
        beside[k].start()
        if k > 1:
            pass_on(k - 2)
    for k in range(max(n - 2, 0), n):
        pass_on(k)
    for copy in copies:
        copy.wait_send()
    for row in across:
        for copy in row:
            copy.wait_send()
    for copy in beside + passed:
        copy.wait()


def exchange(n, me, source, target, ssem, rsem, lsem):
    copies = []
    for k in range(1, n):
        peer = lax.rem(me + k, n)
        copies.append(
            pltpu.make_async_remote_copy(
                src_ref=source.at[peer],
                dst_ref=target.at[me],
                send_sem=ssem.at[k - 1],
                recv_sem=rsem.at[k - 1],
                device_id={"sp": peer},
                device_id_type=MESH,
            )
        )
    for copy in copies:
        copy.start()
    stays = pltpu.make_async_copy(source.at[me], target.at[me], lsem)
    stays.start()
    stays.wait()
    for copy in copies:
        copy.wait()


def return_kernel(
    n, tp, cap, sums_ref, slot_ref, d_ref, gathered_ref, back, ssem, rsem, lsem, tsend, trecv
):
    me = lax.axis_index("sp")
    col = lax.axis_index("tp")
    partner = col + 1 - 2 * lax.rem(col, 2)
    far = [lax.rem(col + 2 * s, tp) for s in range(1, tp // 2)]
    barrier, greeted = greet(n, me, [partner] + far)
    pl.semaphore_wait(barrier, greeted)
    exchange(n, me, sums_ref, back, ssem, rsem, lsem)
    tokens = d_ref.shape[0]
    quarter = back.shape[2]
    start = pl.multiple_of(col * quarter, quarter)
    places = lax.broadcasted_iota(jnp.int32, (cap, tokens), 0)
    picked = jnp.zeros((tokens, quarter), jnp.float32)
    for e in range(n):
        here = jnp.zeros((cap, tokens), jnp.float32)
        for j in range(2):
            here = here + (slot_ref[j : j + 1, :] - e * cap == places).astype(jnp.float32)
        picked = picked + mm(here.astype(jnp.bfloat16), back[e], TN)
    own = d_ref[:, pl.ds(start, quarter)].astype(jnp.float32)
    gathered_ref[col] = (own + picked).astype(jnp.bfloat16)

    def send(block, slot, target):
        return pltpu.make_async_remote_copy(
            src_ref=gathered_ref.at[block],
            dst_ref=gathered_ref.at[block],
            send_sem=tsend.at[slot],
            recv_sem=trecv.at[slot],
            device_id={"tp": target},
            device_id_type=MESH,
        )

    across = [send(col, s + 1, far[s]) for s in range(len(far))]
    beside = send(col, 0, partner)
    for copy in across:
        copy.start()
    beside.start()
    passed = []
    for s in range(len(far)):
        across[s].wait_recv()
        block = lax.rem(col - 2 * (s + 1) + tp, tp)
        passed.append(send(block, tp // 2 + s, partner))
        passed[s].start()
    for copy in across:
        copy.wait_send()
    beside.wait()
    for copy in passed:
        copy.wait()


def state_copies(n, me, step, send_ref, recv_ref, send_sem, recv_sem):
    return [
        pltpu.make_async_remote_copy(
            src_ref=send_ref,
            dst_ref=recv_ref.at[k - 1],
            send_sem=send_sem.at[k - 1],
            recv_sem=recv_sem.at[k - 1],
            device_id={"sp": lax.rem(me + step * k + n, n)},
            device_id_type=MESH,
        )
        for k in range(1, n)
    ]


def collect(n, me, step, copies, recv_ref, total, width):
    total[...] = jnp.zeros_like(total)
    for k in range(n - 1, 0, -1):
        copies[k - 1].wait()
        source = me - step * k
        reached = jnp.logical_and(source >= 0, source < n)

        @pl.when(reached)
        def _():
            factor = recv_ref[k - 1, width : width + 1, :].astype(jnp.float32)
            total[...] = total[...] * factor + recv_ref[k - 1, :width, :].astype(jnp.float32)


def forward_kernel(
    n, scale, q_ref, k_ref, v_ref, g_ref, mixed_ref, states_ref, kept, total, send, recv, ssem, rsem
):
    me = lax.axis_index("sp")
    barrier, greeted = greet(n, me)
    length, width = v_ref.shape
    blocks = length // BLK
    causal = triangle(True)
    local = jnp.zeros(total.shape, jnp.float32)
    ahead = jnp.zeros((1, q_ref.shape[1]), jnp.float32)
    befores = []
    for b in range(blocks):
        rows = pl.ds(b * BLK, BLK)
        cumulative, _, ending = decays(g_ref, rows)
        kept[b] = local
        befores.append(ahead)
        faded = (k_ref[rows, :].astype(jnp.float32) * jnp.exp(ending - cumulative)).astype(
            jnp.bfloat16
        )
        local = local * jnp.exp(ending) + mm(v_ref[rows, :], faded, TN)
        ahead = ahead + ending
    send[:width, :] = local.astype(jnp.bfloat16)
    send[width:, :] = jnp.broadcast_to(jnp.exp(ahead), (16, ahead.shape[1])).astype(jnp.bfloat16)
    pl.semaphore_wait(barrier, greeted)
    copies = state_copies(n, me, 1, send, recv, ssem, rsem)
    for copy in copies:
        copy.start()
    inner = []
    scaled = []
    for b in range(blocks):
        rows = pl.ds(b * BLK, BLK)
        cumulative, middle, _ = decays(g_ref, rows)
        query = q_ref[rows, :].astype(jnp.float32) * scale
        key = k_ref[rows, :].astype(jnp.float32)
        lifted_q = (query * jnp.exp(cumulative - middle)).astype(jnp.bfloat16)
        lifted_k = (key * jnp.exp(middle - cumulative)).astype(jnp.bfloat16)
        scores = jnp.where(causal, mm(lifted_q, lifted_k, NT), 0.0).astype(jnp.bfloat16)
        inner.append(mm(scores, v_ref[rows, :], NN))
        scaled.append((query * jnp.exp(cumulative)).astype(jnp.bfloat16))
    collect(n, me, 1, copies, recv, total, width)
    for b in range(blocks):
        rows = pl.ds(b * BLK, BLK)
        state = (kept[b] + total[...] * jnp.exp(befores[b])).astype(jnp.bfloat16)
        states_ref[b] = state
        mixed_ref[rows, :] = (inner[b] + mm(scaled[b], state, NT)).astype(jnp.bfloat16)


def backward_kernel(
    n,
    scale,
    q_ref,
    k_ref,
    v_ref,
    g_ref,
    grad_ref,
    w_ref,
    mixed_ref,
    states_ref,
    gq_ref,
    gk_ref,
    gv_ref,
    gg_ref,
    proj_ref,
    kept,
    total,
    send,
    recv,
    ssem,
    rsem,
    d_ref,
    part,
    pair_in,
    pair,
    parts_in,
    psend,
    precv,
):
    me = lax.axis_index("sp")
    barrier, greeted = greet(n, me)
    length, width = v_ref.shape
    blocks = length // BLK
    causal = triangle(True)
    local = jnp.zeros(total.shape, jnp.float32)
    pieces, _, quarter = grad_ref.shape
    d_mixed = jnp.zeros((length, width), jnp.float32)
    for p in range(pieces):
        d_mixed = d_mixed + mm(grad_ref[p], w_ref[p * quarter : (p + 1) * quarter, :], NN)
    d_ref[...] = d_mixed.astype(jnp.bfloat16)
    after = jnp.zeros((1, q_ref.shape[1]), jnp.float32)
    afters = [None] * blocks
    for b in reversed(range(blocks)):
        rows = pl.ds(b * BLK, BLK)
        cumulative, _, ending = decays(g_ref, rows)
        kept[b] = local
        afters[b] = after
        query = q_ref[rows, :].astype(jnp.float32) * scale
        scaled = (query * jnp.exp(cumulative)).astype(jnp.bfloat16)
        local = local * jnp.exp(ending) + mm(d_ref[rows, :], scaled, TN)
        after = after + ending
    send[:width, :] = local.astype(jnp.bfloat16)
    send[width:, :] = jnp.broadcast_to(jnp.exp(after), (16, after.shape[1])).astype(jnp.bfloat16)
    pl.semaphore_wait(barrier, greeted)
    copies = state_copies(n, me, -1, send, recv, ssem, rsem)
    for copy in copies:
        copy.start()
    half, share = part.shape[1:3]
    per = quarter // share
    for p in range(pieces):
        product = mm(grad_ref[p], mixed_ref[...], TN).astype(jnp.bfloat16)
        for i in range(per):
            at = p * per + i
            part[at % 2, at // 2] = product[i * share : (i + 1) * share, :]
    parity = lax.rem(me, 2)
    mine = me // 2
    pairing = pltpu.make_async_remote_copy(
        src_ref=part.at[1 - parity],
        dst_ref=pair_in,
        send_sem=psend.at[0],
        recv_sem=precv.at[0],
        device_id={"sp": me + 1 - 2 * parity},
        device_id_type=MESH,
    )
    pairing.start()
    change = []
    key_part = []
    for b in range(blocks):
        rows = pl.ds(b * BLK, BLK)
        cumulative, middle, _ = decays(g_ref, rows)
        query = q_ref[rows, :].astype(jnp.float32) * scale
        key = k_ref[rows, :].astype(jnp.float32)
        value = v_ref[rows, :]
        d_out = d_ref[rows, :]
        rise, fall = jnp.exp(cumulative - middle), jnp.exp(middle - cumulative)
        lifted_q = (query * rise).astype(jnp.bfloat16)
        lifted_k = (key * fall).astype(jnp.bfloat16)
        scores = jnp.where(causal, mm(lifted_q, lifted_k, NT), 0.0).astype(jnp.bfloat16)
        d_scores = jnp.where(causal, mm(d_out, value, NT), 0.0).astype(jnp.bfloat16)
        d_lifted_q = mm(d_scores, lifted_k, NN)
        d_lifted_k = mm(d_scores, lifted_q, TN)
        grown = jnp.exp(cumulative)
        d_carried = mm(d_out, states_ref[b], NN) * grown
        gq_ref[rows, :] = ((d_lifted_q * rise + d_carried) * scale).astype(jnp.bfloat16)
        change.append(
            lifted_q.astype(jnp.float32) * d_lifted_q
            - lifted_k.astype(jnp.float32) * d_lifted_k
            + query * d_carried
        )
        key_part.append(d_lifted_k * fall)
        gg_ref[rows, :] = change[b]
        gv_ref[rows, :] = mm(scores, d_out, TN).astype(gv_ref.dtype)
    pairing.wait()
    for i in range(half):
        pair[i] = (part[parity, i].astype(jnp.float32) + pair_in[i].astype(jnp.float32)).astype(
            jnp.bfloat16
        )
    collect(n, me, -1, copies, recv, total, width)
    shares = []
    for s in range(1, half):
        other = lax.rem(mine + s, half)
        shares.append(
            pltpu.make_async_remote_copy(
                src_ref=pair.at[other],
                dst_ref=parts_in.at[s - 1],
                send_sem=psend.at[s],
                recv_sem=precv.at[s],
                device_id={"sp": 2 * other + parity},
                device_id_type=MESH,
            )
        )
        shares[-1].start()
    for b in range(blocks):
        rows = pl.ds(b * BLK, BLK)
        cumulative, _, ending = decays(g_ref, rows)
        d_state = kept[b] + total[...] * jnp.exp(afters[b])
        d_rounded = d_state.astype(jnp.bfloat16)
        key = k_ref[rows, :].astype(jnp.float32)
        fade = jnp.exp(ending - cumulative)
        faded = key * fade
        d_faded = mm(v_ref[rows, :], d_rounded, NN)
        gk_ref[rows, :] = (key_part[b] + d_faded * fade).astype(jnp.bfloat16)
        gv_ref[rows, :] = gv_ref[rows, :] + mm(faded.astype(jnp.bfloat16), d_rounded, NT)
        moved = faded * d_faded
        at_end = jnp.sum(moved, axis=0, keepdims=True) + jnp.exp(ending) * jnp.sum(
            states_ref[b].astype(jnp.float32) * d_state, axis=0, keepdims=True
        )
        gg_ref[rows, :] = block_sums(triangle(False), gg_ref[rows, :] - moved) + at_end
    summed = pair[mine].astype(jnp.float32)
    for s in range(1, half):
        shares[s - 1].wait()
        summed = summed + parts_in[s - 1].astype(jnp.float32)
    proj_ref[...] = summed


def exchange_scratch(n, blocks, width, channels):
    return [
        pltpu.VMEM((blocks, width, channels), jnp.float32),
        pltpu.VMEM((width, channels), jnp.float32),
        pltpu.VMEM((width + 16, channels), jnp.bfloat16),
        pltpu.VMEM((n - 1, width + 16, channels), jnp.bfloat16),
        pltpu.SemaphoreType.DMA((n - 1,)),
        pltpu.SemaphoreType.DMA((n - 1,)),
    ]


def in_vmem(count):
    return [pl.BlockSpec(memory_space=pltpu.VMEM)] * count


def mixer_forward(q, k, v, g, scale):
    n = lax.axis_size("sp")
    length, channels = q.shape
    width = v.shape[1]
    blocks = length // BLK
    return pl.pallas_call(
        functools.partial(forward_kernel, n, scale),
        out_shape=(
            jax.ShapeDtypeStruct((length, width), jnp.bfloat16),
            jax.ShapeDtypeStruct((blocks, width, channels), jnp.bfloat16),
        ),
        in_specs=in_vmem(4),
        out_specs=tuple(in_vmem(2)),
        scratch_shapes=exchange_scratch(n, blocks, width, channels),
        compiler_params=pltpu.CompilerParams(
            collective_id=1, has_side_effects=True, vmem_limit_bytes=16 * 1024 * 1024
        ),
        cost_estimate=pl.CostEstimate(
            flops=4_000_000_000, bytes_accessed=4 * length * width, transcendentals=0
        ),
        name="mixer_forward",
    )(q, k, v, g)


def mixer_backward(q, k, v, g, gathered, w_out, mixed, states, scale):
    n = lax.axis_size("sp")
    length, channels = q.shape
    width = v.shape[1]
    blocks = length // BLK
    share = w_out.shape[0] // n
    return pl.pallas_call(
        functools.partial(backward_kernel, n, scale),
        out_shape=(
            jax.ShapeDtypeStruct((length, channels), jnp.bfloat16),
            jax.ShapeDtypeStruct((length, channels), jnp.bfloat16),
            jax.ShapeDtypeStruct((length, width), jnp.float32),
            jax.ShapeDtypeStruct((length, channels), jnp.float32),
            jax.ShapeDtypeStruct((share, width), jnp.float32),
        ),
        in_specs=in_vmem(8),
        out_specs=tuple(in_vmem(5)),
        scratch_shapes=exchange_scratch(n, blocks, width, channels)
        + [
            pltpu.VMEM((length, width), jnp.bfloat16),
            pltpu.VMEM((2, n // 2, share, width), jnp.bfloat16),
            pltpu.VMEM((n // 2, share, width), jnp.bfloat16),
            pltpu.VMEM((n // 2, share, width), jnp.bfloat16),
            pltpu.VMEM((n // 2 - 1, share, width), jnp.bfloat16),
            pltpu.SemaphoreType.DMA((n // 2,)),
            pltpu.SemaphoreType.DMA((n // 2,)),
        ],
        compiler_params=pltpu.CompilerParams(
            collective_id=2, has_side_effects=True, vmem_limit_bytes=24 * 1024 * 1024
        ),
        cost_estimate=pl.CostEstimate(
            flops=8_000_000_000, bytes_accessed=4 * length * width, transcendentals=0
        ),
        name="mixer_backward",
    )(q, k, v, g, gathered, w_out, mixed, states)


def route_out(d_out, route_expert, route_weight, capacity):
    n, tp = lax.axis_size("sp"), lax.axis_size("tp")
    tokens, model_width = d_out.shape
    quarter = model_width // tp
    return pl.pallas_call(
        functools.partial(route_kernel, n, tp, capacity),
        out_shape=(
            jax.ShapeDtypeStruct((n, capacity, model_width), jnp.bfloat16),
            jax.ShapeDtypeStruct((2, tokens), jnp.int32),
        ),
        in_specs=in_vmem(3),
        out_specs=tuple(in_vmem(2)),
        scratch_shapes=[
            pltpu.VMEM((n, capacity, quarter), jnp.bfloat16),
            pltpu.SemaphoreType.DMA((n - 1,)),
            pltpu.SemaphoreType.DMA((n - 1,)),
            pltpu.SemaphoreType.DMA,
            pltpu.SemaphoreType.DMA((n, tp)),
            pltpu.SemaphoreType.DMA((n, tp)),
        ],
        compiler_params=pltpu.CompilerParams(
            collective_id=3, has_side_effects=True, vmem_limit_bytes=24 * 1024 * 1024
        ),
        cost_estimate=pl.CostEstimate(
            flops=8_000_000_000, bytes_accessed=4 * tokens * quarter, transcendentals=0
        ),
        name="route_out",
    )(d_out, route_expert.T, route_weight)


def route_back(summed, slots, d_out):
    n, tp = lax.axis_size("sp"), lax.axis_size("tp")
    capacity, quarter = summed.shape[1:]
    tokens = d_out.shape[0]
    return pl.pallas_call(
        functools.partial(return_kernel, n, tp, capacity),
        out_shape=jax.ShapeDtypeStruct((tp, tokens, quarter), jnp.bfloat16),
        in_specs=in_vmem(3),
        out_specs=in_vmem(1)[0],
        scratch_shapes=[
            pltpu.VMEM((n, capacity, quarter), jnp.bfloat16),
            pltpu.SemaphoreType.DMA((n - 1,)),
            pltpu.SemaphoreType.DMA((n - 1,)),
            pltpu.SemaphoreType.DMA,
            pltpu.SemaphoreType.DMA((tp,)),
            pltpu.SemaphoreType.DMA((tp,)),
        ],
        compiler_params=pltpu.CompilerParams(
            collective_id=4, has_side_effects=True, vmem_limit_bytes=24 * 1024 * 1024
        ),
        cost_estimate=pl.CostEstimate(
            flops=8_000_000_000, bytes_accessed=4 * tokens * quarter, transcendentals=0
        ),
        name="route_back",
    )(summed, slots, d_out)


def expert_pass(rows_in, routed_rows, gate_w, up_w, down_w):
    gate_pre = jnp.dot(rows_in, gate_w, preferred_element_type=jnp.float32)
    up_pre = jnp.dot(rows_in, up_w, preferred_element_type=jnp.float32)
    sigmoid_gate = jax.nn.sigmoid(gate_pre)
    active = gate_pre * sigmoid_gate
    hidden = (active * up_pre).astype(jnp.bfloat16)
    d_hidden = lax.dot_general(
        routed_rows, down_w, (((1,), (1,)), ((), ())), preferred_element_type=jnp.float32
    )
    d_gate = (d_hidden * up_pre * sigmoid_gate * (1.0 + gate_pre * (1.0 - sigmoid_gate))).astype(
        jnp.bfloat16
    )
    d_up = (d_hidden * active).astype(jnp.bfloat16)
    rows_first = (((0,), (0,)), ((), ()))
    grad_gate = lax.dot_general(
        rows_in, d_gate, rows_first, preferred_element_type=jnp.float32
    ).astype(jnp.bfloat16)
    grad_up = lax.dot_general(rows_in, d_up, rows_first, preferred_element_type=jnp.float32).astype(
        jnp.bfloat16
    )
    grad_down = lax.dot_general(
        hidden, routed_rows, rows_first, preferred_element_type=jnp.float32
    ).astype(jnp.bfloat16)
    return (grad_gate, grad_up, grad_down, d_gate, d_up)


def local(
    d_out,
    route_expert,
    route_weight,
    expert_inputs,
    w_gate,
    w_up,
    w_down,
    w_out,
    queries,
    keys,
    values,
    log_decay,
):
    model_width = d_out.shape[1]
    experts = lax.axis_size("sp")
    capacity = expert_inputs.shape[1] // experts
    quarter = model_width // lax.axis_size("tp")
    routed, slots = route_out(d_out, route_expert, route_weight, capacity)
    routed = routed.reshape(experts * capacity, model_width)
    rows_in = expert_inputs[0]
    gate_w = w_gate[0]
    up_w = w_up[0]
    grad_gate, grad_up, grad_down, d_gate, d_up = expert_pass(
        rows_in, routed, gate_w, up_w, w_down[0]
    )
    partial_terms = lax.dot_general(
        d_gate, gate_w, (((1,), (1,)), ((), ())), preferred_element_type=jnp.float32
    )
    partial_terms = partial_terms + lax.dot_general(
        d_up, up_w, (((1,), (1,)), ((), ())), preferred_element_type=jnp.float32
    )
    rounded = lax.optimization_barrier(partial_terms.astype(jnp.bfloat16)).astype(jnp.float32)
    summed = lax.psum_scatter(rounded.astype(jnp.bfloat16), "tp", scatter_dimension=1, tiled=True)
    scale_q = queries.shape[2] ** (-0.5)
    q, k, v, g = queries[:, 0], keys[:, 0], values[:, 0], log_decay[:, 0]
    mixed, states = mixer_forward(q, k, v, g, scale_q)
    summed, mixed, grad_gate, grad_up, grad_down = lax.optimization_barrier(
        (summed, mixed, grad_gate, grad_up, grad_down)
    )
    gathered = route_back(summed.reshape(experts, capacity, quarter), slots, d_out)
    grad_q, grad_k, grad_v, grad_g, grad_proj = mixer_backward(
        q, k, v, g, gathered, w_out, mixed, states, scale_q
    )
    return (
        grad_gate[None],
        grad_up[None],
        grad_down[None],
        grad_proj,
        grad_q[:, None],
        grad_k[:, None],
        grad_v.astype(jnp.bfloat16)[:, None],
        grad_g[:, None],
    )


def paired(me, offset):
    other = me
    bit = 1
    while bit <= offset:
        if offset & bit:
            other = other + bit - 2 * bit * lax.rem(me // bit, 2)
        bit *= 2
    return other


def prefix_copy(n, me, step, distance, index, send, recv, ssem, rsem):
    return pltpu.make_async_remote_copy(
        src_ref=send.at[index],
        dst_ref=recv.at[index],
        send_sem=ssem.at[index],
        recv_sem=rsem.at[index],
        device_id={"sp": lax.rem(me + step * distance + n, n)},
        device_id_type=MESH,
    )


def prefix_send(n, me, step, distance, index, local, ahead, scan, send, recv, ssem, rsem):
    width = local.shape[0]
    total, reach = scan
    decay = reach[0:1, :] * ahead[0:1, :]
    send[index, :width, :] = (total[...] * ahead[0:1, :] + local[...]).astype(jnp.bfloat16)
    send[index, width:, :] = jnp.broadcast_to(decay, (16, decay.shape[1])).astype(jnp.bfloat16)
    target = me + step * distance

    @pl.when(jnp.logical_and(target >= 0, target < n))
    def _():
        prefix_copy(n, me, step, distance, index, send, recv, ssem, rsem).start()


def prefix_take(n, me, step, distance, index, scan, send, recv, ssem, rsem):
    total, reach = scan
    width = total.shape[0]
    source = me - step * distance
    target = me + step * distance
    copy = prefix_copy(n, me, step, distance, index, send, recv, ssem, rsem)

    @pl.when(jnp.logical_and(target >= 0, target < n))
    def _():
        copy.wait_send()

    @pl.when(jnp.logical_and(source >= 0, source < n))
    def _():
        copy.wait_recv()
        total[...] = total[...] + recv[index, :width, :].astype(jnp.float32) * reach[0:1, :]
        reach[...] = reach[...] * recv[index, width : width + 1, :].astype(jnp.float32)


def distances(n):
    found = []
    step = 1
    while step < n:
        found.append(step)
        step *= 2
    return found


def expert_kernel(
    n,
    cap,
    scale,
    d_hbm,
    expert_ref,
    weight_ref,
    x_hbm,
    wg_hbm,
    wu_hbm,
    wd_hbm,
    q_ref,
    k_ref,
    v_ref,
    g_ref,
    w_hbm,
    grad_gate,
    grad_up,
    grad_down,
    grad_proj,
    grad_q,
    grad_k,
    grad_v,
    grad_g,
    wg_ref,
    wu_ref,
    wd_ref,
    proj_ref,
    gq_ref,
    gk_ref,
    gv_ref,
    gg_ref,
    gathered,
    mixed_ref,
    states_ref,
    d_ref,
    x_ref,
    routed,
    onehot,
    outbox,
    outbox_near,
    slope,
    active,
    hidden,
    d_gate,
    d_up,
    part,
    pair_in,
    far_out,
    far_in,
    sums,
    back,
    picked,
    turned,
    cum,
    kept,
    befores,
    inner,
    scaled,
    lifted_q,
    lifted_k,
    scores_ref,
    d_mixed,
    d_round,
    key_part,
    proj_out,
    proj_pair,
    proj_mine,
    proj_in,
    w_ref,
    mix_local,
    mix_ahead,
    mix_total,
    mix_reach,
    mix_send,
    mix_recv,
    lsem,
    osem,
    rs,
    rr,
    fs,
    fr,
    ps,
    pr,
    qs,
    qr,
    ds,
    dr,
    xs,
    xr,
    bs,
    br,
    ms,
    mr,
    gs,
    gr,
    ys,
    yr,
    zs,
    zr,
):
    me = lax.axis_index("sp")
    col = lax.axis_index("tp")
    core = lax.rem(col, 2)
    side = col // 2
    partner = col + 1 - 2 * core
    far = lax.rem(col + 2, 4)
    chunks = n // 2
    rows2 = 2 * cap
    tokens = d_ref.shape[0]
    model = d_ref.shape[1]
    quarter = model // 4
    half = model // 2
    near = 3
    cuts = [pl.ds(0, quarter // 2), pl.ds(quarter // 2, quarter // 2)]

    barrier, greeted = greet(n, me, [partner, far])

    def chunk_rows(z):
        return pl.ds(z * rows2, rows2)

    def block_rows(m):
        return pl.ds(m * cap, cap)

    def columns(q):
        return pl.ds(pl.multiple_of(q * quarter, quarter), quarter)

    order = [0, chunks - 1, 1] + list(range(chunks - 2, 1, -1))
    loads = {}

    def load(name, source, target, index):
        loads[name] = pltpu.make_async_copy(source, target, lsem.at[index])
        loads[name].start()

    load("d", d_hbm, d_ref, 0)
    load("wg", wg_hbm, wg_ref, 1)

    def load_rows(z):
        for m in (2 * z, 2 * z + 1):
            first = pl.multiple_of(paired(me, m) * cap, cap)
            load(("x", m), x_hbm.at[pl.ds(first, cap), :], x_ref.at[block_rows(m), :], 4 + m)

    load_rows(0)
    load("wu", wu_hbm, wu_ref, 2)
    load("wd", wd_hbm, wd_ref, 3)
    for z in order[1:]:
        load_rows(z)
    load("w", w_hbm, w_ref, 4 + n)

    kinds = lax.broadcasted_iota(jnp.int32, (n, tokens), 0)
    named = [(kinds == expert_ref[j : j + 1, :]).astype(jnp.float32) for j in range(2)]
    earlier = lax.broadcasted_iota(jnp.int32, (tokens, tokens), 0) < lax.broadcasted_iota(
        jnp.int32, (tokens, tokens), 1
    )
    before = mm((named[0] + named[1]).astype(jnp.bfloat16), earlier.astype(jnp.bfloat16), NN)
    slots = []
    for j in range(2):
        rank = jnp.sum(before * named[j], axis=0, keepdims=True).astype(jnp.int32)
        slots.append(expert_ref[j : j + 1, :] * cap + rank)
    places = lax.broadcasted_iota(jnp.int32, (cap, tokens), 0)

    def routed_rows(m, chosen):
        first = paired(me, m) * cap
        hits = [(slots[j] - first == places).astype(jnp.float32) for j in range(2)]
        both = (hits[0] + hits[1]).astype(jnp.bfloat16)
        onehot[block_rows(m), :] = both
        weight = jnp.sum(
            hits[0] * weight_ref[0:1, :] + hits[1] * weight_ref[1:2, :], axis=1, keepdims=True
        )
        return (mm(both, chosen, NN) * weight).astype(jnp.bfloat16)

    def route(m):
        if m <= near:
            source = outbox_near.at[block_rows(m - 1), :]
            target = routed.at[block_rows(m), pl.ds(pl.multiple_of(core * half, half), half)]
        else:
            source = outbox.at[block_rows(m - near - 1), :]
            target = routed.at[block_rows(m), columns(col)]
        return pltpu.make_async_remote_copy(
            src_ref=source,
            dst_ref=target,
            send_sem=rs.at[m],
            recv_sem=rr.at[m],
            device_id={"sp": paired(me, m)},
            device_id_type=MESH,
        )

    def pass_on(m, what, target, send_sem, recv_sem):
        if m <= near:
            piece = routed.at[block_rows(m), pl.ds(pl.multiple_of(what * half, half), half)]
        else:
            piece = routed.at[block_rows(m), columns(what)]
        return pltpu.make_async_remote_copy(
            src_ref=piece,
            dst_ref=piece,
            send_sem=send_sem.at[m],
            recv_sem=recv_sem.at[m],
            device_id={"tp": target},
            device_id_type=MESH,
        )

    sent = []
    loads["d"].wait()
    sends = []
    for z in range(chunks - 1, 0, -1):
        sends += [2 * z, 2 * z + 1]
    sends.insert(1, 1)
    greeting = True
    for m in sends:
        if m <= near:
            outbox_near[block_rows(m - 1), :] = routed_rows(
                m, d_ref[:, pl.ds(pl.multiple_of(core * half, half), half)]
            )
        else:
            outbox[block_rows(m - near - 1), :] = routed_rows(m, d_ref[:, columns(col)])
        if greeting:
            pl.semaphore_wait(barrier, greeted)
            greeting = False
        sent.append(route(m))
        sent[-1].start()
    routed[block_rows(0), :] = routed_rows(0, d_ref[...])

    crossed, beside, relayed = {}, {}, {}

    def arrive(m):
        route(m).wait_recv()
        if m <= near:
            beside[m] = pass_on(m, core, partner, ps, pr)
            beside[m].start()
            return
        crossed[m] = pass_on(m, col, far, fs, fr)
        crossed[m].start()
        beside[m] = pass_on(m, col, partner, ps, pr)
        beside[m].start()

    def relay(m):
        if m <= near:
            return
        crossed[m].wait_recv()
        relayed[m] = pass_on(m, far, partner, qs, qr)
        relayed[m].start()

    def complete(m):
        beside[m].wait_recv()
        if m > near:
            relayed[m].wait_recv()

    def gates(z):
        rows = chunk_rows(z)
        held = order.index(z) % 2
        loads[("x", 2 * z)].wait()
        loads[("x", 2 * z + 1)].wait()
        if z == 0:
            loads["wg"].wait()
        gate = mm(x_ref[rows, :], wg_ref[...], NT)
        if z == 0:
            loads["wu"].wait()
        up = mm(x_ref[rows, :], wu_ref[...], NT)
        sigmoid = jax.nn.sigmoid(gate)
        silu = gate * sigmoid
        hidden[rows, :] = (silu * up).astype(jnp.bfloat16)
        active[held] = silu
        slope[held] = up * sigmoid * (1.0 + gate * (1.0 - sigmoid))

    halves = {}

    def experts(z):
        rows = chunk_rows(z)
        if z == 0:
            loads["wd"].wait()
        d_hidden = mm(routed[rows, :], wd_ref[...], NT)
        held = order.index(z) % 2
        d_gate[rows, :] = (d_hidden * slope[held]).astype(jnp.bfloat16)
        d_up[rows, :] = (d_hidden * active[held]).astype(jnp.bfloat16)
        for whose in (1 - core, core):
            for i in range(2):
                across = 1 - side if i == 0 else side
                cut = columns(2 * across + whose)
                term = mm(d_gate[rows, :], wg_ref[:, cut], NN) + mm(
                    d_up[rows, :], wu_ref[:, cut], NN
                )
                part[rows, cut] = term.astype(jnp.bfloat16)
            if (z, 0) in halves:
                continue
            for i in range(2):
                across = 1 - side if i == 0 else side
                halves[(z, i)] = pltpu.make_async_remote_copy(
                    src_ref=part.at[rows, columns(2 * across + 1 - core)],
                    dst_ref=pair_in.at[i, rows, :],
                    send_sem=ds.at[z, i],
                    recv_sem=dr.at[z, i],
                    device_id={"tp": partner},
                    device_id_type=MESH,
                )
                halves[(z, i)].start()

    over = {}

    def half_of(q, h):
        first = q * quarter + h * (quarter // 2)
        return pl.ds(pl.multiple_of(first, quarter // 2), quarter // 2)

    def reduce_near(z):
        rows = chunk_rows(z)
        halves[(z, 0)].wait_recv()
        for h in range(2):
            far_out[rows, cuts[h]] = (
                part[rows, half_of(far, h)].astype(jnp.float32)
                + pair_in[0, rows, cuts[h]].astype(jnp.float32)
            ).astype(jnp.bfloat16)
            over[(z, h)] = pltpu.make_async_remote_copy(
                src_ref=far_out.at[rows, cuts[h]],
                dst_ref=far_in.at[rows, cuts[h]],
                send_sem=xs.at[z, h],
                recv_sem=xr.at[z, h],
                device_id={"tp": far},
                device_id_type=MESH,
            )
            over[(z, h)].start()

    returned = {}

    def reduce_far(z):
        halves[(z, 1)].wait_recv()
        for h in range(2):
            reduce_half(z, h)

    def reduce_half(z, h):
        rows = chunk_rows(z)
        over[(z, h)].wait_recv()
        sums[rows, cuts[h]] = (
            part[rows, half_of(col, h)].astype(jnp.float32)
            + pair_in[1, rows, cuts[h]].astype(jnp.float32)
            + far_in[rows, cuts[h]].astype(jnp.float32)
        ).astype(jnp.bfloat16)
        for m in (2 * z, 2 * z + 1):
            if m == 0:
                back[block_rows(0), cuts[h]] = sums[block_rows(0), cuts[h]]
                continue
            returned[(m, h)] = pltpu.make_async_remote_copy(
                src_ref=sums.at[block_rows(m), cuts[h]],
                dst_ref=back.at[block_rows(m), cuts[h]],
                send_sem=bs.at[m, h],
                recv_sem=br.at[m, h],
                device_id={"sp": paired(me, m)},
                device_id_type=MESH,
            )
            returned[(m, h)].start()

    def pick(z, h):
        rows = chunk_rows(z)
        for m in (2 * z, 2 * z + 1):
            if m > 0:
                returned[(m, h)].wait_recv()
        found = mm(onehot[rows, :], back[rows, cuts[h]], TN)
        picked[:, cuts[h]] = found if z == 0 else picked[:, cuts[h]] + found

    stored = []

    def store(source, target):
        stored.append(pltpu.make_async_copy(source, target, osem.at[len(stored)]))
        stored[-1].start()

    def weight_grad(lhs, rhs, out, target):
        turned[...] = lhs[...].T

        def piece(i, carry):
            cut = columns(i)
            out[:, cut] = mm(turned[...], rhs[:, cut], NN).astype(jnp.bfloat16)
            return carry

        lax.fori_loop(0, 4, piece, 0)
        store(out, target)

    blocks = tokens // BLK
    causal = triangle(True)
    width = v_ref.shape[1]
    scan = (mix_total, mix_reach)
    reach = distances(n)
    rounds = len(reach)

    def scan_from(local, ahead):
        mix_local[...] = local
        mix_ahead[...] = jnp.broadcast_to(jnp.exp(ahead), mix_ahead.shape)
        mix_total[...] = jnp.zeros(mix_total.shape, jnp.float32)
        mix_reach[...] = jnp.ones(mix_reach.shape, jnp.float32)

    def mixer_states():
        local = jnp.zeros(mix_total.shape, jnp.float32)
        ahead = jnp.zeros((1, q_ref.shape[1]), jnp.float32)
        for b in range(blocks):
            rows = pl.ds(b * BLK, BLK)
            cumulative, _, ending = decays(g_ref, rows)
            cum[rows, :] = cumulative
            kept[b] = local
            befores[b : b + 1, :] = jnp.exp(ahead)
            faded = (k_ref[rows, :].astype(jnp.float32) * jnp.exp(ending - cumulative)).astype(
                jnp.bfloat16
            )
            local = local * jnp.exp(ending) + mm(v_ref[rows, :], faded, TN)
            ahead = ahead + ending
        scan_from(local, ahead)

    def mixer_send(step, index):
        at = index if step > 0 else rounds + index
        distance = reach[index]
        prefix_send(
            n, me, step, distance, at, mix_local, mix_ahead, scan, mix_send, mix_recv, ms, mr
        )

    def mixer_take(step, index):
        at = index if step > 0 else rounds + index
        prefix_take(n, me, step, reach[index], at, scan, mix_send, mix_recv, ms, mr)

    def mixer_inner():
        for b in range(blocks):
            rows = pl.ds(b * BLK, BLK)
            cumulative = cum[rows, :]
            middle = cumulative[BLK // 2 - 1 : BLK // 2, :]
            query = q_ref[rows, :].astype(jnp.float32) * scale
            key = k_ref[rows, :].astype(jnp.float32)
            up_q = (query * jnp.exp(cumulative - middle)).astype(jnp.bfloat16)
            up_k = (key * jnp.exp(middle - cumulative)).astype(jnp.bfloat16)
            scores = jnp.where(causal, mm(up_q, up_k, NT), 0.0).astype(jnp.bfloat16)
            lifted_q[rows, :] = up_q
            lifted_k[rows, :] = up_k
            scores_ref[rows, :] = scores
            inner[rows, :] = mm(scores, v_ref[rows, :], NN)
            scaled[rows, :] = (query * jnp.exp(cumulative)).astype(jnp.bfloat16)

    def mixer_finish():
        for b in range(blocks):
            rows = pl.ds(b * BLK, BLK)
            state = (kept[b] + mix_total[...] * befores[b : b + 1, :]).astype(jnp.bfloat16)
            states_ref[b] = state
            mixed_ref[rows, :] = (inner[rows, :] + mm(scaled[rows, :], state, NT)).astype(
                jnp.bfloat16
            )

    taken = [0]

    def mixer_round(step):
        if taken[0] < rounds:
            mixer_take(step, taken[0])
            taken[0] += 1
            if taken[0] < rounds:
                mixer_send(step, taken[0])

    share, turns = proj_out.shape[3], proj_out.shape[1]
    parity = lax.rem(me, 2)
    at_z = me // 2
    paired_off, handed = {}, []

    def project(j, h):
        first = paired(col, j) * quarter + h * (quarter // 2)
        rows = pl.ds(pl.multiple_of(first, quarter // 2), quarter // 2)
        grads = gathered[j, :, cuts[h]]
        term = mm(grads, w_ref[rows, :], NN)
        d_mixed[...] = term if j + h == 0 else d_mixed[...] + term
        product = mm(grads, mixed_ref[...], TN).astype(jnp.bfloat16)
        for t in range(turns):
            at = h * turns + t
            proj_out[j, at // 2, at % 2] = product[t * share : (t + 1) * share, :]

    def pair_up(j):
        for i in range(turns):
            paired_off[(j, i)] = pltpu.make_async_remote_copy(
                src_ref=proj_out.at[j, i, 1 - parity],
                dst_ref=proj_pair.at[j, i],
                send_sem=ys.at[j, i],
                recv_sem=yr.at[j, i],
                device_id={"sp": me + 1 - 2 * parity},
                device_id_type=MESH,
            )
            paired_off[(j, i)].start()

    def hand_over(j):
        q = paired(col, j)
        for i in range(turns):
            paired_off[(j, i)].wait_recv()
            both_rows = proj_out[j, i, parity].astype(jnp.float32) + proj_pair[j, i].astype(
                jnp.float32
            )
            proj_out[j, i, parity] = both_rows.astype(jnp.bfloat16)
            owner = q * turns + i
            away = jnp.int32(0)
            bit = 1
            while bit < chunks:
                away = away + bit * lax.rem(at_z // bit + owner // bit, 2)
                bit *= 2
            copy = pltpu.make_async_remote_copy(
                src_ref=proj_out.at[j, i, parity],
                dst_ref=proj_in.at[away],
                send_sem=zs.at[j, i],
                recv_sem=zr.at[away],
                device_id={"sp": 2 * owner + parity},
                device_id_type=MESH,
            )
            handed.append((away, copy))

            @pl.when(away == 0)
            def _():
                proj_mine[...] = proj_out[j, i, parity].astype(jnp.float32)

            @pl.when(away != 0)
            def _():
                copy.start()

    def project_sum():
        total = proj_mine[...]
        for z in range(1, chunks):
            pltpu.make_async_remote_copy(
                src_ref=proj_out.at[0, 0, parity],
                dst_ref=proj_in.at[z],
                send_sem=zs.at[0, 0],
                recv_sem=zr.at[z],
                device_id={"sp": paired(me, 2 * z)},
                device_id_type=MESH,
            ).wait_recv()
            total = total + proj_in[z].astype(jnp.float32)
        proj_ref[...] = total

    def back_states():
        d_round[...] = d_mixed[...].astype(jnp.bfloat16)
        local = jnp.zeros(mix_total.shape, jnp.float32)
        after = jnp.zeros((1, q_ref.shape[1]), jnp.float32)
        for b in reversed(range(blocks)):
            rows = pl.ds(b * BLK, BLK)
            ending = cum[b * BLK + BLK - 1 : b * BLK + BLK, :]
            kept[b] = local
            befores[b : b + 1, :] = jnp.exp(after)
            local = local * jnp.exp(ending) + mm(d_round[rows, :], scaled[rows, :], TN)
            after = after + ending
        scan_from(local, after)

    def back_inner():
        for b in range(blocks):
            rows = pl.ds(b * BLK, BLK)
            cumulative = cum[rows, :]
            middle = cumulative[BLK // 2 - 1 : BLK // 2, :]
            query = q_ref[rows, :].astype(jnp.float32) * scale
            d_out = d_round[rows, :]
            up_q, up_k = lifted_q[rows, :], lifted_k[rows, :]
            d_scores = jnp.where(causal, mm(d_out, v_ref[rows, :], NT), 0.0).astype(jnp.bfloat16)
            d_up_q = mm(d_scores, up_k, NN)
            d_up_k = mm(d_scores, up_q, TN)
            d_carried = mm(d_out, states_ref[b], NN) * jnp.exp(cumulative)
            gq_ref[rows, :] = (
                (d_up_q * jnp.exp(cumulative - middle) + d_carried) * scale
            ).astype(jnp.bfloat16)
            gg_ref[rows, :] = (
                up_q.astype(jnp.float32) * d_up_q
                - up_k.astype(jnp.float32) * d_up_k
                + query * d_carried
            )
            key_part[rows, :] = d_up_k * jnp.exp(middle - cumulative)
            inner[rows, :] = mm(scores_ref[rows, :], d_out, TN)

    def back_finish():
        for b in range(blocks):
            rows = pl.ds(b * BLK, BLK)
            cumulative = cum[rows, :]
            ending = cumulative[BLK - 1 : BLK, :]
            d_state = kept[b] + mix_total[...] * befores[b : b + 1, :]
            d_rounded = d_state.astype(jnp.bfloat16)
            fade = jnp.exp(ending - cumulative)
            faded = k_ref[rows, :].astype(jnp.float32) * fade
            d_faded = mm(v_ref[rows, :], d_rounded, NN)
            gk_ref[rows, :] = (key_part[rows, :] + d_faded * fade).astype(jnp.bfloat16)
            gv_ref[rows, :] = (
                inner[rows, :] + mm(faded.astype(jnp.bfloat16), d_rounded, NT)
            ).astype(jnp.bfloat16)
            moved = faded * d_faded
            at_end = jnp.sum(moved, axis=0, keepdims=True) + jnp.exp(ending) * jnp.sum(
                states_ref[b].astype(jnp.float32) * d_state, axis=0, keepdims=True
            )
            gg_ref[rows, :] = block_sums(triangle(False), gg_ref[rows, :] - moved) + at_end

    def both(step, z):
        step(2 * z)
        step(2 * z + 1)

    def give(block, slot, target, h):
        return pltpu.make_async_remote_copy(
            src_ref=gathered.at[block, :, cuts[h]],
            dst_ref=gathered.at[slot, :, cuts[h]],
            send_sem=gs.at[slot, h],
            recv_sem=gr.at[slot, h],
            device_id={"tp": target},
            device_id_type=MESH,
        )

    def share_out(h):
        first = pl.multiple_of(col * quarter + h * (quarter // 2), quarter // 2)
        own = d_ref[:, pl.ds(first, quarter // 2)].astype(jnp.float32)
        gathered[0, :, cuts[h]] = (own + picked[:, cuts[h]]).astype(jnp.bfloat16)
        given[(2, h)] = give(0, 2, far, h)
        given[(1, h)] = give(0, 1, partner, h)
        given[(2, h)].start()
        given[(1, h)].start()

    def share_on(h):
        given[(2, h)].wait_recv()
        given[(3, h)] = give(2, 3, partner, h)
        given[(3, h)].start()

    def settle(slot, h):
        given[(slot, h)].wait_recv()

    given = {}
    early = order[1:]
    gates(0)
    mixer_states()
    mixer_send(1, 0)
    gates(early[0])
    arrive(1)
    mixer_inner()
    arrive(2 * early[0])
    complete(1)
    experts(0)
    arrive(2 * early[0] + 1)
    reduce_near(0)
    gates(early[1])
    both(relay, early[0])
    both(complete, early[0])
    experts(early[0])
    reduce_near(early[0])
    for z in early[2:]:
        both(arrive, z)
    mixer_round(1)
    reduce_far(0)
    both(arrive, early[1])
    pending = [early[0]]
    for i, z in enumerate(early[1:]):
        following = early[i + 2] if i + 2 < len(early) else None
        both(relay, z)
        both(complete, z)
        experts(z)
        mixer_round(1)
        if following is not None:
            gates(following)
        if i > 0:
            reduce_far(pending.pop(0))
        reduce_near(z)
        pending.append(z)
    weight_grad(hidden, routed, wd_ref, grad_down)
    reduce_far(pending.pop(0))
    pick(0, 0)
    pick(0, 1)
    reduce_far(pending.pop(0))
    weight_grad(d_gate, x_ref, wg_ref, grad_gate)
    while taken[0] < rounds:
        mixer_round(1)
    mixer_finish()
    weight_grad(d_up, x_ref, wu_ref, grad_up)
    loads["w"].wait()
    for z in early:
        pick(z, 0)
    share_out(0)
    project(0, 0)
    for z in early:
        pick(z, 1)
    share_out(1)
    project(0, 1)
    pair_up(0)
    settle(1, 0)
    project(1, 0)
    settle(1, 1)
    project(1, 1)
    pair_up(1)
    share_on(0)
    project(2, 0)
    hand_over(0)
    hand_over(1)
    share_on(1)
    project(2, 1)
    pair_up(2)
    settle(3, 0)
    project(3, 0)
    settle(3, 1)
    project(3, 1)
    back_states()
    taken[0] = 0
    mixer_send(-1, 0)
    pair_up(3)
    back_inner()
    mixer_round(-1)
    mixer_round(-1)
    hand_over(2)
    hand_over(3)
    mixer_round(-1)
    store(gq_ref, grad_q)
    back_finish()
    store(gk_ref, grad_k)
    store(gv_ref, grad_v)
    store(gg_ref, grad_g)
    project_sum()
    store(proj_ref, grad_proj)
    for copy in stored:
        copy.wait()
    for copy in sent:
        copy.wait_send()
    for group in (given, crossed, beside, relayed, halves, over, returned, paired_off):
        for copy in group.values():
            copy.wait_send()
    for away, copy in handed:

        @pl.when(away != 0)
        def _():
            copy.wait_send()


def expert_stage(
    d_out, route_expert, route_weight, rows_in, gate_t, up_t, down, q, k, v, g, w_out, cap, scale
):
    n = lax.axis_size("sp")
    tokens, model = d_out.shape
    quarter = model // 4
    units = down.shape[0]
    slots = n * cap
    channels, width = q.shape[1], v.shape[1]
    blocks = tokens // BLK
    rounds = len(distances(n))
    share = model // n
    turns = n // 8
    bf16, f32 = jnp.bfloat16, jnp.float32
    weight_shape = jax.ShapeDtypeStruct((units, model), bf16)
    out_shape = (
        weight_shape,
        weight_shape,
        weight_shape,
        jax.ShapeDtypeStruct((share, width), f32),
        jax.ShapeDtypeStruct((tokens, channels), bf16),
        jax.ShapeDtypeStruct((tokens, channels), bf16),
        jax.ShapeDtypeStruct((tokens, width), bf16),
        jax.ShapeDtypeStruct((tokens, channels), f32),
    )
    anywhere = pl.BlockSpec(memory_space=pl.ANY)
    local = pl.BlockSpec(memory_space=pltpu.VMEM)
    dma = pltpu.SemaphoreType.DMA
    return pl.pallas_call(
        functools.partial(expert_kernel, n, cap, scale),
        out_shape=out_shape,
        in_specs=[anywhere, local, local] + [anywhere] * 4 + [local] * 4 + [anywhere],
        out_specs=(anywhere,) * 8,
        scratch_shapes=[pltpu.VMEM(a.shape, a.dtype) for a in out_shape]
        + [
            pltpu.VMEM((4, tokens, quarter), bf16),
            pltpu.VMEM((tokens, width), bf16),
            pltpu.VMEM((blocks, width, channels), bf16),
            pltpu.VMEM((tokens, model), bf16),
            pltpu.VMEM((slots, model), bf16),
            pltpu.VMEM((slots, model), bf16),
            pltpu.VMEM((slots, tokens), bf16),
            pltpu.VMEM((slots - 4 * cap, quarter), bf16),
            pltpu.VMEM((3 * cap, model // 2), bf16),
            pltpu.VMEM((2, 2 * cap, units), f32),
            pltpu.VMEM((2, 2 * cap, units), f32),
            pltpu.VMEM((slots, units), bf16),
            pltpu.VMEM((slots, units), bf16),
            pltpu.VMEM((slots, units), bf16),
            pltpu.VMEM((slots, model), bf16),
            pltpu.VMEM((2, slots, quarter), bf16),
            pltpu.VMEM((slots, quarter), bf16),
            pltpu.VMEM((slots, quarter), bf16),
            pltpu.VMEM((slots, quarter), bf16),
            pltpu.VMEM((slots, quarter), bf16),
            pltpu.VMEM((tokens, quarter), f32),
            pltpu.VMEM((units, slots), bf16),
            pltpu.VMEM((tokens, channels), f32),
            pltpu.VMEM((blocks, width, channels), f32),
            pltpu.VMEM((blocks, channels), f32),
            pltpu.VMEM((tokens, width), f32),
            pltpu.VMEM((tokens, channels), bf16),
            pltpu.VMEM((tokens, channels), bf16),
            pltpu.VMEM((tokens, channels), bf16),
            pltpu.VMEM((tokens, BLK), bf16),
            pltpu.VMEM((tokens, width), f32),
            pltpu.VMEM((tokens, width), bf16),
            pltpu.VMEM((tokens, channels), f32),
            pltpu.VMEM((4, turns, 2, share, width), bf16),
            pltpu.VMEM((4, turns, share, width), bf16),
            pltpu.VMEM((share, width), f32),
            pltpu.VMEM((n // 2, share, width), bf16),
            pltpu.VMEM((model, width), bf16),
            pltpu.VMEM((width, channels), f32),
            pltpu.VMEM((8, channels), f32),
            pltpu.VMEM((width, channels), f32),
            pltpu.VMEM((8, channels), f32),
            pltpu.VMEM((2 * rounds, width + 16, channels), bf16),
            pltpu.VMEM((2 * rounds, width + 16, channels), bf16),
            dma((5 + n,)),
            dma((8,)),
            dma((n,)),
            dma((n,)),
            dma((n,)),
            dma((n,)),
            dma((n,)),
            dma((n,)),
            dma((n,)),
            dma((n,)),
            dma((n // 2, 2)),
            dma((n // 2, 2)),
            dma((n // 2, 2)),
            dma((n // 2, 2)),
            dma((n, 2)),
            dma((n, 2)),
            dma((2 * rounds,)),
            dma((2 * rounds,)),
            dma((4, 2)),
            dma((4, 2)),
            dma((4, turns)),
            dma((4, turns)),
            dma((4, turns)),
            dma((n // 2,)),
        ],
        compiler_params=pltpu.CompilerParams(
            collective_id=5, has_side_effects=True, vmem_limit_bytes=60 * 1024 * 1024
        ),
        cost_estimate=pl.CostEstimate(
            flops=60_000_000_000, bytes_accessed=30_000_000, transcendentals=0
        ),
        name="expert_stage",
    )(d_out, route_expert.T, route_weight.T, rows_in, gate_t, up_t, down, q, k, v, g, w_out)


def store_kernel(pieces, count, *refs):
    sources, targets, held = refs[:count], refs[count : 2 * count], refs[2 * count : 3 * count]
    isem, osem = refs[3 * count :]
    cuts = []
    for i in range(count):
        parts = pieces if i < 3 else 1
        rows = sources[i].shape[0] // parts
        cuts += [(i, pl.ds(p * rows, rows)) for p in range(parts)]
    reads = [
        pltpu.make_async_copy(sources[i].at[cut, :], held[i].at[cut, :], isem.at[at])
        for at, (i, cut) in enumerate(cuts)
    ]
    writes = [
        pltpu.make_async_copy(held[i].at[cut, :], targets[i].at[cut, :], osem.at[at])
        for at, (i, cut) in enumerate(cuts)
    ]
    for read in reads:
        read.start()
    for read, write in zip(reads, writes):
        read.wait()
        write.start()
    for write in writes:
        write.wait()


def store_out(arrays):
    count = len(arrays)
    pieces = 4 if arrays[0].shape[0] % 64 == 0 else 1
    total = 3 * pieces + count - 3
    anywhere = pl.BlockSpec(memory_space=pl.ANY)
    return pl.pallas_call(
        functools.partial(store_kernel, pieces, count),
        out_shape=tuple(jax.ShapeDtypeStruct(a.shape, a.dtype) for a in arrays),
        in_specs=[anywhere] * count,
        out_specs=(anywhere,) * count,
        scratch_shapes=[pltpu.VMEM(a.shape, a.dtype) for a in arrays]
        + [pltpu.SemaphoreType.DMA((total,)), pltpu.SemaphoreType.DMA((total,))],
        compiler_params=pltpu.CompilerParams(vmem_limit_bytes=60 * 1024 * 1024),
        name="store_out",
    )(*arrays)


def fused_local(
    d_out,
    route_expert,
    route_weight,
    expert_inputs,
    w_gate,
    w_up,
    w_down,
    w_out,
    queries,
    keys,
    values,
    log_decay,
):
    experts = lax.axis_size("sp")
    capacity = expert_inputs.shape[1] // experts
    scale_q = queries.shape[2] ** (-0.5)
    q, k, v, g = queries[:, 0], keys[:, 0], values[:, 0], log_decay[:, 0]
    results = expert_stage(
        d_out,
        route_expert,
        route_weight,
        expert_inputs[0],
        w_gate[0].T,
        w_up[0].T,
        w_down[0],
        q,
        k,
        v,
        g,
        w_out,
        capacity,
        scale_q,
    )
    grad_gate, grad_up, grad_down, grad_proj, grad_q, grad_k, grad_v, grad_g = store_out(results)
    return (
        grad_gate.T[None],
        grad_up.T[None],
        grad_down[None],
        grad_proj,
        grad_q[:, None],
        grad_k[:, None],
        grad_v[:, None],
        grad_g[:, None],
    )


def choose(*arrays):
    n, tp = lax.axis_size("sp"), lax.axis_size("tp")
    tokens, model = arrays[0].shape
    capacity = arrays[3].shape[1] // n
    power = n & (n - 1) == 0 and n % 8 == 0
    if tp == 4 and power and capacity % 16 == 0 and n * capacity <= 1536 and model % 512 == 0:
        return fused_local(*arrays)
    return local(*arrays)


def solution(mesh):
    return jax.shard_map(
        choose,
        mesh=mesh,
        in_specs=(
            P("sp", None),
            P("sp", None),
            P("sp", None),
            P("sp", None, None),
            P("sp", None, "tp"),
            P("sp", None, "tp"),
            P("sp", "tp", None),
            P(None, "tp"),
            P("sp", "tp", None),
            P("sp", "tp", None),
            P("sp", "tp", None),
            P("sp", "tp", None),
        ),
        out_specs=(
            P("sp", None, "tp"),
            P("sp", None, "tp"),
            P("sp", "tp", None),
            P("sp", "tp"),
            P("sp", "tp", None),
            P("sp", "tp", None),
            P("sp", "tp", None),
            P("sp", "tp", None),
        ),
        check_vma=False,
    )
```
